32 devices in a mesh: grp: 2 (over y), fs: 4 (over z), tp: 4 (over x, core).
Axes of the slice: x: 2, y: 2, z: 4, core: 2. Of those that a mesh axis runs over, the one named last changes fastest.
Arguments:
- tokens: bfloat16 [3072, 2048], P(('grp', 'fs'), 'tp'), parts along dimension 0, may hold values from -6 to 6
- mix_gain: float32 [2048], replicated, may hold values from 0.1 to 1.9
- w_signal: bfloat16 [2048, 1024], P('fs', 'tp'), may hold values from -0.125 to 0.125
- w_outer_gate: bfloat16 [2048, 1024], P('fs', 'tp'), may hold values from -0.125 to 0.125
- w_inner_gate: bfloat16 [2048, 1024], P('fs', 'tp'), may hold values from -0.125 to 0.125
- mix_taps: float32 [3, 1024], P(None, 'tp'), may hold values from -3 to 3
- w_mix_out: bfloat16 [1024, 2048], P('tp', 'fs'), may hold values from -0.1875 to 0.1875
- ffn_gain: float32 [2048], replicated, may hold values from 0.1 to 1.9
- w_gate: bfloat16 [2048, 5120], P('fs', 'tp'), may hold values from -0.125 to 0.125
- w_value: bfloat16 [2048, 5120], P('fs', 'tp'), may hold values from -0.125 to 0.125
- up_taps: float32 [2, 3, 5120], P(None, None, 'tp'), may hold values from -3 to 3
- up_bias: float32 [2, 5120], P(None, 'tp'), may hold values from -3 to 3
- w_down: bfloat16 [5120, 2048], P('tp', 'fs'), may hold values from -0.078125 to 0.078125
Outputs:
- layer_out: bfloat16 [3072, 2048], P(('grp', 'fs'), 'tp'), parts along dimension 0
The draws below stay inside these ranges and needn't reach their ends.
There are 2 independent parts, one for each index of `grp`. The reference program is written for one: setup_inputs(seed, part) draws one part's arguments, and reference() takes and returns one part's arrays. A program takes and returns all parts, laid end to end along the dimension named above; an argument that names none is the same for every part. Nothing has to cross between parts.
All inputs are finite; a program needn't handle non-finite values.
Results may differ from the reference program's by a relative error of at most 0.022.
Values may be sent and summed in bfloat16 or wider, within the bound.
A program may use at most 64 MiB of HBM per device.

```python
import jax
import jax.numpy as jnp
from jax import lax

D = 2048
DC = 1024
FF = 5120
TAPS = 3
LEN = 192
TOKENS = 1536
N_TP = 4


def block_levels(stream_key, extent, split, least, high):
    level, own = 1.0, jax.random.fold_in(stream_key, 6)
    for dim, blocks in split:
        steps = jnp.exp(jax.random.uniform(jax.random.fold_in(own, dim), (blocks,), jnp.float32, least / len(split), high / len(split)))
        level = level * jnp.repeat(steps, extent[dim] // blocks).reshape([-1 if axis == dim else 1 for axis in range(len(extent))])
    return level


def centred(rng, dims, deviation, bound, shards=(), dtype=jnp.bfloat16):
    drawn = jax.random.normal(rng, dims, jnp.float32) * deviation
    if len(shards) > 0:
        drawn = block_levels(rng, dims, shards, -0.22, 0.18) * drawn
    return jnp.clip(drawn, min=-bound, max=bound).astype(dtype)


def setup_inputs(seed: int = 0, part: int = 0) -> dict:
    key_list = jax.random.split(jax.random.key(seed), 14)
    part_splits = jax.random.split(jax.random.fold_in(key_list[13], part), 14)
    return {
        "tokens": centred(part_splits[0], (TOKENS, D), 1.0, 6.0, ((0, 4), (1, 4))),
        "mix_gain": jnp.clip(1.0 + 0.18 * jax.random.normal(key_list[1], (D,), jnp.float32), 0.1, 1.9),
        "w_signal": centred(key_list[2], (D, DC), D ** -0.5, 0.125, ((0, 4), (1, 4))),
        "w_outer_gate": centred(key_list[3], (D, DC), D ** -0.5, 0.125, ((0, 4), (1, 4))),
        "w_inner_gate": centred(key_list[4], (D, DC), D ** -0.5, 0.125, ((0, 4), (1, 4))),
        "mix_taps": centred(key_list[5], (TAPS, DC), 0.577, 3.0, ((1, 4),), jnp.float32),
        "w_mix_out": centred(key_list[6], (DC, D), DC ** -0.5, 0.1875, ((0, 4), (1, 4))),
        "ffn_gain": jnp.clip(1.0 + 0.18 * jax.random.normal(key_list[7], (D,), jnp.float32), 0.1, 1.9),
        "w_gate": centred(key_list[8], (D, FF), D ** -0.5, 0.125, ((0, 4), (1, 4))),
        "w_value": centred(key_list[9], (D, FF), D ** -0.5, 0.125, ((0, 4), (1, 4))),
        "up_taps": centred(key_list[10], (2, TAPS, FF), 0.577, 3.0, ((2, 4),), jnp.float32),
        "up_bias": centred(key_list[11], (2, FF), 0.5, 3.0, ((1, 4),), jnp.float32),
        "w_down": centred(key_list[12], (FF, D), FF ** -0.5, 0.078125, ((0, 4), (1, 4))),
    }


def conv_positions(values, taps):
    width = values.shape[1]
    blocks = values.reshape(-1, LEN, width)
    padded = jnp.pad(blocks, ((0, 0), (2, 0), (0, 0)))
    result = padded[:, 0:LEN] * taps[0] + padded[:, 1:LEN + 1] * taps[1] + padded[:, 2:LEN + 2] * taps[2]
    return result.reshape(-1, width)

def rms_norm(stream, gain):
    values = stream.astype(jnp.float32)
    scale = lax.rsqrt(lax.optimization_barrier(jnp.mean(values * values, axis=-1, keepdims=True)) + 1e-06)
    return (values * scale * gain).astype(jnp.bfloat16)

def block_partials(left, right, blocks):
    width = left.shape[1] // blocks
    total = jnp.zeros((left.shape[0], right.shape[1]), jnp.float32)
    for index in range(blocks):
        part = jnp.dot(left[:, index * width:(index + 1) * width], right[index * width:(index + 1) * width], preferred_element_type=jnp.float32)
        part = lax.optimization_barrier(part.astype(jnp.bfloat16))
        total = total + part.astype(jnp.float32)
    return total

def reference(tokens, mix_gain, w_signal, w_outer_gate, w_inner_gate, mix_taps, w_mix_out, ffn_gain, w_gate, w_value, up_taps, up_bias, w_down):
    normed = rms_norm(tokens, mix_gain)
    signal = jnp.dot(normed, w_signal, preferred_element_type=jnp.float32).astype(jnp.bfloat16)
    outer = jnp.dot(normed, w_outer_gate, preferred_element_type=jnp.float32).astype(jnp.bfloat16)
    inner = jnp.dot(normed, w_inner_gate, preferred_element_type=jnp.float32).astype(jnp.bfloat16)
    product = inner.astype(jnp.float32) * signal.astype(jnp.float32)
    mixed = (outer.astype(jnp.float32) * conv_positions(product, mix_taps)).astype(jnp.bfloat16)
    mix_sum = block_partials(mixed, w_mix_out, N_TP)
    resid = (tokens.astype(jnp.float32) + mix_sum).astype(jnp.bfloat16)
    normed_ffn = rms_norm(resid, ffn_gain)
    gate = jnp.dot(normed_ffn, w_gate, preferred_element_type=jnp.float32).astype(jnp.bfloat16)
    value = jnp.dot(normed_ffn, w_value, preferred_element_type=jnp.float32).astype(jnp.bfloat16)
    gate_conv = conv_positions(gate.astype(jnp.float32), up_taps[0]) + up_bias[0]
    value_conv = conv_positions(value.astype(jnp.float32), up_taps[1]) + up_bias[1]
    hidden = (jax.nn.silu(gate_conv) * value_conv).astype(jnp.bfloat16)
    ffn_sum = block_partials(hidden, w_down, N_TP)
    return (resid.astype(jnp.float32) + ffn_sum).astype(jnp.bfloat16)
```

```python
import functools

import jax
import jax.numpy as jnp
from jax import lax
from jax.experimental import pallas as pl
from jax.experimental.pallas import tpu as pltpu
from jax.sharding import PartitionSpec as P

SEQS_DEV = 2


def conv_positions(values, taps):
    width = values.shape[1]
    blocks = values.reshape(SEQS_DEV, -1, width)
    length = blocks.shape[1]
    padded = jnp.pad(blocks, ((0, 0), (2, 0), (0, 0)))
    result = (
        padded[:, 0:length] * taps[0]
        + padded[:, 1 : length + 1] * taps[1]
        + padded[:, 2 : length + 2] * taps[2]
    )
    return result.reshape(-1, width)


def rms_norm(stream, gain):
    values = stream.astype(jnp.float32)
    scale = lax.rsqrt(jnp.mean(values * values, axis=-1, keepdims=True) + 1e-06)
    return (values * scale * gain).astype(jnp.bfloat16)


def on_device(
    tokens,
    mix_gain,
    w_signal,
    w_outer_gate,
    w_inner_gate,
    mix_taps,
    w_mix_out,
    ffn_gain,
    w_gate,
    w_value,
    up_taps,
    up_bias,
    w_down,
):
    whole = lax.all_gather(tokens, "tp", axis=1, tiled=True)
    normed = rms_norm(whole, mix_gain)
    pieces = (
        lax.all_gather(w_signal, "fs", axis=0, tiled=True),
        lax.all_gather(w_outer_gate, "fs", axis=0, tiled=True),
        lax.all_gather(w_inner_gate, "fs", axis=0, tiled=True),
    )
    columns = normed
    signal, outer, inner = tuple(
        (jnp.dot(columns, piece, preferred_element_type=jnp.float32) for piece in pieces)
    )
    signal = signal.astype(jnp.bfloat16).astype(jnp.float32)
    outer = outer.astype(jnp.bfloat16).astype(jnp.float32)
    inner = inner.astype(jnp.bfloat16).astype(jnp.float32)
    mixed = (outer * conv_positions(inner * signal, mix_taps)).astype(jnp.bfloat16)
    mix_terms = jnp.dot(
        mixed,
        lax.all_gather(w_mix_out, "fs", axis=1, tiled=True),
        preferred_element_type=jnp.float32,
    )
    mix_sum = lax.psum_scatter(
        mix_terms.astype(jnp.bfloat16), "tp", scatter_dimension=1, tiled=True
    ).astype(jnp.float32)
    resid = (tokens.astype(jnp.float32) + mix_sum).astype(jnp.bfloat16)
    whole_ffn = lax.all_gather(resid, "tp", axis=1, tiled=True)
    normed_ffn = rms_norm(whole_ffn, ffn_gain)
    pieces = (
        lax.all_gather(w_gate, "fs", axis=0, tiled=True),
        lax.all_gather(w_value, "fs", axis=0, tiled=True),
    )
    columns = normed_ffn
    gate = jnp.dot(columns, pieces[0], preferred_element_type=jnp.float32)
    value = jnp.dot(columns, pieces[1], preferred_element_type=jnp.float32)
    gate = gate.astype(jnp.bfloat16).astype(jnp.float32)
    value = value.astype(jnp.bfloat16).astype(jnp.float32)
    gate_conv = conv_positions(gate, up_taps[0]) + up_bias[0]
    value_conv = conv_positions(value, up_taps[1]) + up_bias[1]
    hidden = (jax.nn.silu(gate_conv) * value_conv).astype(jnp.bfloat16)
    ffn_terms = jnp.dot(
        hidden, lax.all_gather(w_down, "fs", axis=1, tiled=True), preferred_element_type=jnp.float32
    )
    ffn_sum = lax.psum_scatter(
        ffn_terms.astype(jnp.bfloat16), "tp", scatter_dimension=1, tiled=True
    ).astype(jnp.float32)
    return (resid.astype(jnp.float32) + ffn_sum).astype(jnp.bfloat16)


MESH = pl.DeviceIdType.MESH
UP, DOWN = 0, 1
LANES = 128


def shifted(values, by, length):
    rolled = pltpu.roll(values, by, 0)
    position = lax.rem(lax.broadcasted_iota(jnp.int32, values.shape, 0), length)
    return jnp.where(position < by, 0.0, rolled)


def conv_rows(values, taps, length):
    return (
        shifted(values, 2, length) * taps[0:1]
        + shifted(values, 1, length) * taps[1:2]
        + values * taps[2:3]
    )


def layer_kernel(
    n_fs,
    n_tp,
    tokens,
    mix_gain,
    w_signal,
    w_outer_gate,
    w_inner_gate,
    mix_taps,
    w_mix_out,
    ffn_gain,
    w_gate,
    w_value,
    up_taps,
    up_bias,
    w_down,
    out,
    mix_in,
    mix_out,
    ffn_in,
    ffn_out,
    tok,
    res,
    normed,
    hidden,
    part_mix,
    mix_core,
    mix_x_sum,
    mix_x_got,
    mix_z_sum,
    mix_z_got,
    part_ffn,
    got_core,
    sum_x,
    got_x,
    sum_z,
    got_z,
    z_send,
    z_recv,
    y_send,
    y_recv,
    load_sem,
    all_send,
    all_recv,
    mix_core_send,
    mix_core_recv,
    mix_x_send,
    mix_x_recv,
    core_send,
    core_recv,
    x_send,
    x_recv,
    pair_send,
    pair_recv,
):
    g, j, k = lax.axis_index("grp"), lax.axis_index("fs"), lax.axis_index("tp")
    rows, own_cols = tokens.shape
    length = rows // SEQS_DEV
    shard, chans = w_signal.shape
    half, unit_chans = shard // 2, chans // 2
    units = w_gate.shape[1] // 2
    n_in, n_out = units // LANES, shard // LANES
    n_x = n_tp // 2
    x, c = k // 2, lax.rem(k, 2)
    core = k + 1 - 2 * c
    p = lax.rem(j, 2)
    pair = j + 1 - 2 * p
    inward = jnp.where(j < n_fs // 2, 1, n_fs - 1)
    at_end = (j == 0) | (j == n_fs - 1)

    MINE, THEIRS = 0, 1

    def held_rows(o, h=None):
        side = p if o == MINE else 1 - p
        if h is None:
            return pl.ds(pl.multiple_of(side * rows, rows), rows)
        return pl.ds(pl.multiple_of(side * rows + h * length, length), length)

    def in_half(h):
        return slice(h * length, (h + 1) * length)

    mix = ("mix", 0)
    order = [mix, *(("in", t) for t in range(n_in)), *(("out", u) for u in range(n_out))]

    def other(d):
        return lax.rem(j + inward * d, n_fs)

    def sources(stage, q, side):
        kind, i = stage
        at_rows = pl.ds(pl.multiple_of(side * half, half), half)
        if kind == "mix":
            lanes = pl.ds(pl.multiple_of(q * unit_chans, unit_chans), unit_chans)
            tall = unit_chans // 2
            at = pl.ds(pl.multiple_of((q * 2 + side) * tall, tall), tall)
            refs = [ref.at[at_rows, lanes] for ref in (w_signal, w_outer_gate, w_inner_gate)]
            return [*refs, w_mix_out.at[at, :]]
        if kind == "in":
            lanes = pl.ds(pl.multiple_of(q * units + i * LANES, LANES), LANES)
            return [w_gate.at[at_rows, lanes], w_value.at[at_rows, lanes]]
        tall = units // 2
        at = pl.ds(pl.multiple_of((q * 2 + side) * tall, tall), tall)
        return [w_down.at[at, pl.ds(i * LANES, LANES)]]

    def places(stage, source, side, whole):
        kind, i = stage
        at_rows = pl.ds(pl.multiple_of((source * 2 + side) * half, half), half)
        if kind == "mix":
            tall = unit_chans // 2
            at = pl.ds(pl.multiple_of(side * tall, tall), tall)
            outs = mix_out.at[source, at, :]
            if whole:
                return [mix_in.at[at_rows, :], outs]
            lanes = [pl.ds(b * unit_chans, unit_chans) for b in range(3)]
            return [*(mix_in.at[at_rows, lane] for lane in lanes), outs]
        if kind == "in":
            if whole:
                return [ffn_in.at[i, at_rows, :]]
            return [ffn_in.at[i, at_rows, pl.ds(b * LANES, LANES)] for b in (0, 1)]
        tall = units // 2
        at = pl.ds(pl.multiple_of(side * tall, tall), tall)
        lanes = pl.ds(pl.multiple_of(source * LANES, LANES), LANES)
        return [ffn_out.at[i, at, lanes]]

    def slot(stage, i, wide):
        kind, at = stage
        if kind == "mix":
            return i
        if kind == "in":
            return (4 + 2 * at + i) if wide else 2 + at
        return 4 + 2 * n_in + at if wide else 2 + n_in + at

    def z_sends(s, d):
        to = other(d)
        return [
            pltpu.make_async_remote_copy(
                src_ref=src,
                dst_ref=dst,
                send_sem=z_send.at[slot(s, i, True), to],
                recv_sem=z_recv.at[slot(s, i, True), j],
                device_id={"fs": to},
                device_id_type=MESH,
            )
            for i, (src, dst) in enumerate(
                zip(sources(s, lax.rem(to, 2), g), places(s, j, g, False))
            )
        ]

    def z_takes(s, d):
        source = other(d)
        return [
            pltpu.make_async_remote_copy(
                src_ref=dst,
                dst_ref=dst,
                send_sem=z_send.at[slot(s, i, True), source],
                recv_sem=z_recv.at[slot(s, i, True), source],
                device_id={"fs": source},
                device_id_type=MESH,
            )
            for i, dst in enumerate(places(s, source, g, False))
        ]

    def y_copies(s, d, side):
        source = other(d)
        return [
            pltpu.make_async_remote_copy(
                src_ref=view,
                dst_ref=view,
                send_sem=y_send.at[slot(s, i, False), source],
                recv_sem=y_recv.at[slot(s, i, False), source],
                device_id={"grp": 1 - g},
                device_id_type=MESH,
            )
            for i, view in enumerate(places(s, source, side, True))
        ]

    def start(copies):
        for copy in copies:
            copy.start()

    def wait_recv(copies):
        for copy in copies:
            copy.wait_recv()

    def wait_send(copies):
        for copy in copies:
            copy.wait_send()

    def send(s, ds):
        for d in ds:
            start(z_sends(s, d))

    def relay(s, d):
        wait_recv(z_takes(s, d))
        start(y_copies(s, d, g))

    def relay_all(s):
        for d in range(1, n_fs):
            relay(s, d)

    def arrived(s):
        for d in range(1, n_fs):
            wait_recv(y_copies(s, d, 1 - g))

    def to_tp(src, dst, send_sem, recv_sem, to):
        return pltpu.make_async_remote_copy(
            src_ref=src,
            dst_ref=dst,
            send_sem=send_sem,
            recv_sem=recv_sem,
            device_id={"tp": to},
            device_id_type=MESH,
        )

    def all_copies(buffer, i, at, kind):
        copies = []
        for dx in range(n_x):
            there = lax.rem(x + dx, n_x)
            if kind == "over":
                if dx:
                    view = buffer.at[k, at]
                    sems = all_send.at[i, 0, dx], all_recv.at[i, 0, dx]
                    copies.append(to_tp(view, view, *sems, there * 2 + c))
            else:
                back = lax.rem(x + n_x - dx, n_x) * 2
                seen = back + c if kind == "pass" else back + 1 - c
                view = buffer.at[seen, at]
                sems = all_send.at[i, 1, dx], all_recv.at[i, 1, dx]
                copies.append(to_tp(view, view, *sems, core))
        return copies

    def all_begin(buffer, i, at):
        start(all_copies(buffer, i, at, "over"))
        all_copies(buffer, i, at, "pass")[0].start()

    def all_middle(buffer, i, at):
        passed = all_copies(buffer, i, at, "pass")
        for dx in range(1, n_x):
            view = buffer.at[lax.rem(x + n_x - dx, n_x) * 2 + c, at]
            to_tp(view, view, all_send.at[i, 0, dx], all_recv.at[i, 0, dx], core).wait_recv()
            passed[dx].start()

    def all_end(buffer, i, at):
        wait_recv(all_copies(buffer, i, at, "take"))

    def to_pair(i, src, dst):
        return pltpu.make_async_remote_copy(
            src_ref=src,
            dst_ref=dst,
            send_sem=pair_send.at[i],
            recv_sem=pair_recv.at[i],
            device_id={"fs": pair},
            device_id_type=MESH,
        )

    halves = range(SEQS_DEV)
    mine, theirs = held_rows(MINE), held_rows(THEIRS)

    def tok_swap(at):
        return to_pair(0, tok.at[k, at], tok.at[k, at])

    def res_swap(o, h):
        view = res.at[k, held_rows(o, h)]
        return to_pair(1 + h, view, view)

    def mix_swap(h):
        return to_pair(1 + SEQS_DEV + h, mix_z_sum.at[h], mix_z_got.at[h])

    def back(u):
        return to_pair(1 + 2 * SEQS_DEV + u, sum_z.at[u], got_z.at[u])

    barrier = pltpu.get_barrier_semaphore()
    for d in range(1, n_fs):
        to = lax.rem(j + d, n_fs)
        pl.semaphore_signal(barrier, inc=1, device_id={"fs": to}, device_id_type=MESH)
    pl.semaphore_signal(barrier, inc=1, device_id={"grp": 1 - g}, device_id_type=MESH)
    for d in range(1, n_tp):
        to = lax.rem(k + d, n_tp)
        pl.semaphore_signal(barrier, inc=1, device_id={"tp": to}, device_id_type=MESH)

    loads = [pltpu.make_async_copy(tokens, tok.at[k, mine], load_sem.at[0])]
    own_rows = pl.ds(pl.multiple_of(j * shard, shard), shard)
    own_lanes = pl.ds(pl.multiple_of(j * LANES, LANES), LANES)
    at_chans = pl.ds(pl.multiple_of(p * unit_chans, unit_chans), unit_chans)
    at_units = pl.ds(pl.multiple_of(p * units, units), units)

    def load(src, dst):
        loads.append(pltpu.make_async_copy(src, dst, load_sem.at[len(loads)]))

    for i, ref in enumerate((w_signal, w_outer_gate, w_inner_gate)):
        lanes = pl.ds(i * unit_chans, unit_chans)
        load(ref.at[:, at_chans], mix_in.at[own_rows, lanes])
    load(w_mix_out.at[at_chans, :], mix_out.at[j])
    for t in range(n_in):
        lanes = pl.ds(pl.multiple_of(p * units + t * LANES, LANES), LANES)
        for i, ref in enumerate((w_gate, w_value)):
            load(ref.at[:, lanes], ffn_in.at[t, own_rows, pl.ds(i * LANES, LANES)])
    for u in range(n_out):
        load(w_down.at[at_units, pl.ds(u * LANES, LANES)], ffn_out.at[u, :, own_lanes])
    start(loads)
    loads[0].wait()
    pl.semaphore_wait(barrier, n_fs - 1 + 1 + n_tp - 1)

    tok_swap(mine).start()
    all_begin(tok, 0, mine)
    send(mix, (*range(2, n_fs - 1), n_fs - 1, 1))
    for copy in loads[1:]:
        copy.wait()

    def norm(buffer, at, gain):
        count = at.size
        squares = jnp.zeros((count, 1), jnp.float32)
        for b in range(n_tp):
            values = buffer[b, at, :].astype(jnp.float32)
            squares = squares + jnp.sum(values * values, axis=-1, keepdims=True)
        scale = lax.rsqrt(squares / (n_tp * own_cols) + 1e-06)
        for b in range(n_tp):
            cut = slice(b * own_cols, (b + 1) * own_cols)
            values = buffer[b, at, :].astype(jnp.float32)
            normed[at, cut] = (values * scale * gain[:, cut]).astype(jnp.bfloat16)

    all_middle(tok, 0, mine)
    tok_swap(theirs).wait_recv()
    all_begin(tok, 1, theirs)
    relay(mix, 1)
    all_end(tok, 0, mine)
    norm(tok, mine, mix_gain)
    relay(mix, 2)
    all_middle(tok, 1, theirs)
    for d in range(3, n_fs):
        relay(mix, d)

    eager, late = range(1, n_fs - 1), (n_fs - 1,)

    @pl.when(jnp.logical_not(at_end))
    def _():
        for s in order[1:]:
            send(s, eager)
        for s in order[1:3]:
            send(s, late)

    @pl.when(at_end)
    def _():
        for s in order[1:3]:
            send(s, (*eager, *late))

    all_end(tok, 1, theirs)
    norm(tok, theirs, mix_gain)
    arrived(mix)

    taps = mix_taps[:, at_chans]

    def mix_core_copy(o, dx):
        there = lax.rem(x + dx, n_x)
        return to_tp(
            part_mix.at[o, there * 2 + 1 - c],
            mix_core.at[o, there],
            mix_core_send.at[o, dx],
            mix_core_recv.at[o, dx],
            core,
        )

    def mix_x_copy(o, h, dx):
        to = lax.rem(x + dx, n_x) * 2 + c
        return to_tp(
            mix_x_sum.at[o, h, dx],
            mix_x_got.at[o, h, dx],
            mix_x_send.at[o, h, dx],
            mix_x_recv.at[o, h, dx],
            to,
        )

    def mix_chip_sum(o, h, dx):
        there = lax.rem(x + dx, n_x)
        cut = in_half(h)
        near = part_mix[o, there * 2 + c, cut, :].astype(jnp.float32)
        return near + mix_core[o, there, cut, :].astype(jnp.float32)

    def mix_place_sum(o, h):
        value = mix_chip_sum(o, h, 0)
        for dx in range(1, n_x):
            value = value + mix_x_got[o, h, dx].astype(jnp.float32)
        return value

    for o, at in ((THEIRS, theirs), (MINE, mine)):
        both = jnp.dot(normed[at, :], mix_in[...], preferred_element_type=jnp.float32)
        both = both.astype(jnp.bfloat16).astype(jnp.float32)
        gated = both[:, 2 * unit_chans :] * both[:, :unit_chans]
        conv = conv_rows(gated, taps, length)
        mixed = (both[:, unit_chans : 2 * unit_chans] * conv).astype(jnp.bfloat16)
        for b in range(n_fs):
            terms = jnp.dot(mixed, mix_out[b], preferred_element_type=jnp.float32)
            part_mix[o, b] = terms.astype(jnp.bfloat16)
        for dx in (*range(1, n_x), 0):
            mix_core_copy(o, dx).start()

    for o in (THEIRS, MINE):
        for dx in range(1, n_x):
            mix_core_copy(o, dx).wait_recv()
            for h in halves:
                mix_x_sum[o, h, dx] = mix_chip_sum(o, h, dx).astype(jnp.bfloat16)
                mix_x_copy(o, h, dx).start()
        mix_core_copy(o, 0).wait_recv()
    relay_all(order[1])
    for h in halves:
        for dx in range(1, n_x):
            mix_x_copy(THEIRS, h, dx).wait_recv()
        mix_z_sum[h] = mix_place_sum(THEIRS, h).astype(jnp.bfloat16)
        mix_swap(h).start()

    def late_sends(stages):
        @pl.when(jnp.logical_not(at_end))
        def _():
            for s in stages:
                send(s, late)

        @pl.when(at_end)
        def _():
            for s in stages:
                send(s, (*eager, *late))

    late_sends(order[3:4])
    relay_all(order[2])
    for h in halves:
        for dx in range(1, n_x):
            mix_x_copy(MINE, h, dx).wait_recv()
        mix_swap(h).wait_recv()
        mixer = mix_place_sum(MINE, h) + mix_z_got[h].astype(jnp.float32)
        at = held_rows(MINE, h)
        res[k, at, :] = (tok[k, at, :].astype(jnp.float32) + mixer).astype(jnp.bfloat16)
        res_swap(MINE, h).start()
        all_begin(res, 2 + h, at)
    late_sends(order[4:])

    relay_all(order[3])
    for h in halves:
        all_middle(res, 2 + h, held_rows(MINE, h))
    for h in halves:
        res_swap(THEIRS, h).wait_recv()
        all_begin(res, 2 + SEQS_DEV + h, held_rows(THEIRS, h))
    for h in halves:
        all_end(res, 2 + h, held_rows(MINE, h))
        norm(res, held_rows(MINE, h), ffn_gain)
    for h in halves:
        all_middle(res, 2 + SEQS_DEV + h, held_rows(THEIRS, h))
    relay_all(order[4])
    for h in halves:
        all_end(res, 2 + SEQS_DEV + h, held_rows(THEIRS, h))
        norm(res, held_rows(THEIRS, h), ffn_gain)

    def feed(t):
        arrived(("in", t))
        cut = pl.ds(pl.multiple_of(p * units + t * LANES, LANES), LANES)
        both = jnp.dot(normed[...], ffn_in[t], preferred_element_type=jnp.float32)
        both = both.astype(jnp.bfloat16).astype(jnp.float32)
        gate = conv_rows(both[:, :LANES], up_taps[0, :, cut], length) + up_bias[0:1, cut]
        value = conv_rows(both[:, LANES:], up_taps[1, :, cut], length) + up_bias[1:2, cut]
        unit = (gate / (1.0 + jnp.exp(-gate)) * value).astype(jnp.bfloat16)
        hidden[:, pl.ds(pl.multiple_of(t * LANES, LANES), LANES)] = unit

    beside = {2: 5, 3: 6, 4: 7}

    @pl.loop(0, n_in)
    def _(t):
        for at, index in beside.items():

            @pl.when(t == at)
            def _():
                relay_all(order[index])

        feed(t)

    def core_copy(u, dx):
        there = lax.rem(x + dx, n_x)
        return to_tp(
            part_ffn.at[u, :, there * 2 + 1 - c],
            got_core.at[u, :, there],
            core_send.at[u, dx],
            core_recv.at[u, dx],
            core,
        )

    def x_copy(u, dx):
        to = lax.rem(x + dx, n_x) * 2 + c
        return to_tp(sum_x.at[u, dx], got_x.at[u, dx], x_send.at[u, dx], x_recv.at[u, dx], to)

    def chip_sum(u, o, dx):
        there = lax.rem(x + dx, n_x)
        mine_there = part_ffn[u, o, there * 2 + c].astype(jnp.float32)
        return mine_there + got_core[u, o, there].astype(jnp.float32)

    def place_sum(u, o):
        value = chip_sum(u, o, 0)
        for dx in range(1, n_x):
            value = value + got_x[u, dx, o].astype(jnp.float32)
        return value

    def down(u):
        arrived(("out", u))
        for o, at in enumerate((theirs, mine)):
            terms = jnp.dot(hidden[at, :], ffn_out[u], preferred_element_type=jnp.float32)
            for b in range(n_tp):
                part_ffn[u, o, b] = terms[:, b * LANES : (b + 1) * LANES].astype(jnp.bfloat16)
        for dx in (*range(1, n_x), 0):
            core_copy(u, dx).start()

    def over_x(u):
        for dx in range(1, n_x):
            core_copy(u, dx).wait_recv()
            for o in (0, 1):
                sum_x[u, dx, o] = chip_sum(u, o, dx).astype(jnp.bfloat16)
            x_copy(u, dx).start()

    def over_z(u):
        core_copy(u, 0).wait_recv()
        for dx in range(1, n_x):
            x_copy(u, dx).wait_recv()
        sum_z[u] = place_sum(u, 0).astype(jnp.bfloat16)
        back(u).start()

    for u in range(n_out):
        if 8 + u < len(order):
            relay_all(order[8 + u])
        down(u)
        if u >= 1:
            over_x(u - 1)
        if u >= 2:
            over_z(u - 2)
    over_x(n_out - 1)
    for u in range(max(n_out - 2, 0), n_out):
        over_z(u)
    for u in range(n_out):
        cut = slice(u * LANES, (u + 1) * LANES)
        value = res[k, mine, cut].astype(jnp.float32) + place_sum(u, 1)
        back(u).wait_recv()
        out[:, cut] = (value + got_z[u].astype(jnp.float32)).astype(jnp.bfloat16)

    tok_swap(mine).wait_send()
    gathers = [(tok, 0, mine), (tok, 1, theirs)]
    for h in halves:
        gathers.append((res, 2 + h, held_rows(MINE, h)))
        gathers.append((res, 2 + SEQS_DEV + h, held_rows(THEIRS, h)))
        res_swap(MINE, h).wait_send()
        mix_swap(h).wait_send()
    for gather in gathers:
        wait_send(all_copies(*gather, "over"))
        wait_send(all_copies(*gather, "pass"))
    for o in (MINE, THEIRS):
        for dx in range(n_x):
            mix_core_copy(o, dx).wait_send()
        for dx in range(1, n_x):
            for h in halves:
                mix_x_copy(o, h, dx).wait_send()
    for u in range(n_out):
        for dx in range(n_x):
            core_copy(u, dx).wait_send()
        for dx in range(1, n_x):
            x_copy(u, dx).wait_send()
        back(u).wait_send()

    for s in order:
        for d in range(1, n_fs):
            wait_send(z_sends(s, d))
            wait_send(y_copies(s, d, g))


def fused(n_fs, n_tp, *args):
    tokens, w_signal, w_gate = args[0], args[2], args[8]
    rows, cols = tokens.shape
    shard, chans = w_signal.shape
    units = w_gate.shape[1] // 2
    n_in, n_out = units // LANES, shard // LANES
    width = n_fs * shard
    args = list(args)
    args[1], args[7] = args[1].reshape(1, -1), args[7].reshape(1, -1)
    in_vmem = {1, 5, 7, 10, 11}
    n_x = n_tp // 2
    length = rows // SEQS_DEV
    dma = pltpu.SemaphoreType.DMA

    def held(*shape):
        return pltpu.VMEM(shape, jnp.bfloat16)

    return pl.pallas_call(
        functools.partial(layer_kernel, n_fs, n_tp),
        out_shape=jax.ShapeDtypeStruct((rows, cols), jnp.bfloat16),
        in_specs=[
            pl.BlockSpec(memory_space=pltpu.VMEM if i in in_vmem else pl.ANY)
            for i in range(len(args))
        ],
        out_specs=pl.BlockSpec(memory_space=pltpu.VMEM),
        scratch_shapes=[
            held(width, 3 * (chans // 2)),
            held(n_fs, chans // 2, shard),
            held(n_in, width, 2 * LANES),
            held(n_out, units, n_fs * LANES),
            held(n_tp, 2 * rows, cols),
            held(n_tp, 2 * rows, cols),
            held(2 * rows, width),
            held(2 * rows, units),
            held(2, n_tp, rows, cols),
            held(2, n_x, rows, cols),
            held(2, SEQS_DEV, n_x, length, cols),
            held(2, SEQS_DEV, n_x, length, cols),
            held(SEQS_DEV, length, cols),
            held(SEQS_DEV, length, cols),
            held(n_out, 2, n_tp, rows, LANES),
            held(n_out, 2, n_x, rows, LANES),
            held(n_out, n_x, 2, rows, LANES),
            held(n_out, n_x, 2, rows, LANES),
            held(n_out, rows, LANES),
            held(n_out, rows, LANES),
            dma((4 + 2 * n_in + n_out, n_fs)),
            dma((4 + 2 * n_in + n_out, n_fs)),
            dma((2 + n_in + n_out, n_fs)),
            dma((2 + n_in + n_out, n_fs)),
            dma((5 + 2 * n_in + n_out,)),
            dma((2 + 2 * SEQS_DEV, 2, n_x)),
            dma((2 + 2 * SEQS_DEV, 2, n_x)),
            dma((2, n_x)),
            dma((2, n_x)),
            dma((2, SEQS_DEV, n_x)),
            dma((2, SEQS_DEV, n_x)),
            dma((n_out, n_x)),
            dma((n_out, n_x)),
            dma((n_out, n_x)),
            dma((n_out, n_x)),
            dma((1 + 2 * SEQS_DEV + n_out,)),
            dma((1 + 2 * SEQS_DEV + n_out,)),
        ],
        compiler_params=pltpu.CompilerParams(
            collective_id=0, has_side_effects=True, vmem_limit_bytes=62 * 1024 * 1024
        ),
    )(*args)


def solution(mesh):
    n_fs, n_tp = mesh.shape["fs"], mesh.shape["tp"]
    body = functools.partial(fused, n_fs, n_tp)
    if n_fs > 8 or n_fs != n_tp or n_fs % 2 or mesh.shape["grp"] != 2:
        body = on_device
    placed = (
        P(("grp", "fs"), "tp"),
        P(),
        P("fs", "tp"),
        P("fs", "tp"),
        P("fs", "tp"),
        P(None, "tp"),
        P("tp", "fs"),
        P(),
        P("fs", "tp"),
        P("fs", "tp"),
        P(None, None, "tp"),
        P(None, "tp"),
        P("tp", "fs"),
    )
    return jax.shard_map(
        body, mesh=mesh, in_specs=placed, out_specs=P(("grp", "fs"), "tp"), check_vma=False
    )
```

```python
import functools

import jax
import jax.numpy as jnp
from jax import lax
from jax.experimental import pallas as pl
from jax.experimental.pallas import tpu as pltpu
from jax.sharding import PartitionSpec as P

SEQS_DEV = 2


def conv_positions(values, taps):
    width = values.shape[1]
    blocks = values.reshape(SEQS_DEV, -1, width)
    length = blocks.shape[1]
    padded = jnp.pad(blocks, ((0, 0), (2, 0), (0, 0)))
    result = (
        padded[:, 0:length] * taps[0]
        + padded[:, 1 : length + 1] * taps[1]
        + padded[:, 2 : length + 2] * taps[2]
    )
    return result.reshape(-1, width)


def rms_norm(stream, gain):
    values = stream.astype(jnp.float32)
    scale = lax.rsqrt(jnp.mean(values * values, axis=-1, keepdims=True) + 1e-06)
    return (values * scale * gain).astype(jnp.bfloat16)


def on_device(
    tokens,
    mix_gain,
    w_signal,
    w_outer_gate,
    w_inner_gate,
    mix_taps,
    w_mix_out,
    ffn_gain,
    w_gate,
    w_value,
    up_taps,
    up_bias,
    w_down,
):
    whole = lax.all_gather(tokens, "tp", axis=1, tiled=True)
    normed = rms_norm(whole, mix_gain)
    pieces = (
        lax.all_gather(w_signal, "fs", axis=0, tiled=True),
        lax.all_gather(w_outer_gate, "fs", axis=0, tiled=True),
        lax.all_gather(w_inner_gate, "fs", axis=0, tiled=True),
    )
    columns = normed
    signal, outer, inner = tuple(
        (jnp.dot(columns, piece, preferred_element_type=jnp.float32) for piece in pieces)
    )
    signal = signal.astype(jnp.bfloat16).astype(jnp.float32)
    outer = outer.astype(jnp.bfloat16).astype(jnp.float32)
    inner = inner.astype(jnp.bfloat16).astype(jnp.float32)
    mixed = (outer * conv_positions(inner * signal, mix_taps)).astype(jnp.bfloat16)
    mix_terms = jnp.dot(
        mixed,
        lax.all_gather(w_mix_out, "fs", axis=1, tiled=True),
        preferred_element_type=jnp.float32,
    )
    mix_sum = lax.psum_scatter(
        mix_terms.astype(jnp.bfloat16), "tp", scatter_dimension=1, tiled=True
    ).astype(jnp.float32)
    resid = (tokens.astype(jnp.float32) + mix_sum).astype(jnp.bfloat16)
    whole_ffn = lax.all_gather(resid, "tp", axis=1, tiled=True)
    normed_ffn = rms_norm(whole_ffn, ffn_gain)
    pieces = (
        lax.all_gather(w_gate, "fs", axis=0, tiled=True),
        lax.all_gather(w_value, "fs", axis=0, tiled=True),
    )
    columns = normed_ffn
    gate = jnp.dot(columns, pieces[0], preferred_element_type=jnp.float32)
    value = jnp.dot(columns, pieces[1], preferred_element_type=jnp.float32)
    gate = gate.astype(jnp.bfloat16).astype(jnp.float32)
    value = value.astype(jnp.bfloat16).astype(jnp.float32)
    gate_conv = conv_positions(gate, up_taps[0]) + up_bias[0]
    value_conv = conv_positions(value, up_taps[1]) + up_bias[1]
    hidden = (jax.nn.silu(gate_conv) * value_conv).astype(jnp.bfloat16)
    ffn_terms = jnp.dot(
        hidden, lax.all_gather(w_down, "fs", axis=1, tiled=True), preferred_element_type=jnp.float32
    )
    ffn_sum = lax.psum_scatter(
        ffn_terms.astype(jnp.bfloat16), "tp", scatter_dimension=1, tiled=True
    ).astype(jnp.float32)
    return (resid.astype(jnp.float32) + ffn_sum).astype(jnp.bfloat16)


MESH = pl.DeviceIdType.MESH
UP, DOWN = 0, 1
LANES = 128


def shifted(values, by, length):
    rolled = pltpu.roll(values, by, 0)
    position = lax.rem(lax.broadcasted_iota(jnp.int32, values.shape, 0), length)
    return jnp.where(position < by, 0.0, rolled)


def conv_rows(values, taps, length):
    return (
        shifted(values, 2, length) * taps[0]
        + shifted(values, 1, length) * taps[1]
        + values * taps[2]
    )


def layer_kernel(
    n_fs,
    n_tp,
    tokens,
    mix_gain,
    w_signal,
    w_outer_gate,
    w_inner_gate,
    mix_taps,
    w_mix_out,
    ffn_gain,
    w_gate,
    w_value,
    up_taps,
    up_bias,
    w_down,
    out,
    mix_in,
    mix_out,
    ffn_in,
    ffn_out,
    tok,
    res,
    normed,
    hidden,
    part_mix,
    mix_core,
    mix_x_sum,
    mix_x_got,
    mix_z_sum,
    mix_z_got,
    part_ffn,
    got_core,
    sum_x,
    got_x,
    sum_z,
    got_z,
    z_send,
    z_recv,
    f_send,
    y_send,
    y_recv,
    load_sem,
    all_send,
    all_recv,
    mix_core_send,
    mix_core_recv,
    mix_x_send,
    mix_x_recv,
    core_send,
    core_recv,
    x_send,
    x_recv,
    pair_send,
    pair_recv,
):
    g, j, k = lax.axis_index("grp"), lax.axis_index("fs"), lax.axis_index("tp")
    rows, own_cols = tokens.shape
    length = rows // SEQS_DEV
    shard, chans = w_signal.shape
    half, unit_chans = shard // 2, chans // 2
    units = w_gate.shape[1] // 2
    n_in, n_out = units // LANES, shard // LANES
    n_x = n_tp // 2
    x, c = k // 2, lax.rem(k, 2)
    core = k + 1 - 2 * c
    p = lax.rem(j, 2)
    pair = j + 1 - 2 * p
    inward = jnp.where(j < n_fs // 2, 1, n_fs - 1)
    at_end = (j == 0) | (j == n_fs - 1)

    MINE, THEIRS = 0, 1

    def held_rows(o, h=None):
        side = p if o == MINE else 1 - p
        if h is None:
            return pl.ds(pl.multiple_of(side * rows, rows), rows)
        return pl.ds(pl.multiple_of(side * rows + h * length, length), length)

    def in_half(h):
        return slice(h * length, (h + 1) * length)

    mix = ("mix", 0)
    order = [mix, *(("in", t) for t in range(n_in)), *(("out", u) for u in range(n_out))]

    def other(d):
        return lax.rem(j + inward * d, n_fs)

    def sources(stage, q, side):
        kind, i = stage
        at_rows = pl.ds(pl.multiple_of(side * half, half), half)
        if kind == "mix":
            lanes = pl.ds(pl.multiple_of(q * unit_chans, unit_chans), unit_chans)
            tall = unit_chans // 2
            at = pl.ds(pl.multiple_of((q * 2 + side) * tall, tall), tall)
            refs = [ref.at[at_rows, lanes] for ref in (w_signal, w_outer_gate, w_inner_gate)]
            return [*refs, w_mix_out.at[at, :]]
        if kind == "in":
            lanes = pl.ds(pl.multiple_of(q * units + i * LANES, LANES), LANES)
            return [w_gate.at[at_rows, lanes], w_value.at[at_rows, lanes]]
        tall = units // 2
        at = pl.ds(pl.multiple_of((q * 2 + side) * tall, tall), tall)
        return [w_down.at[at, pl.ds(i * LANES, LANES)]]

    def places(stage, source, side, whole):
        kind, i = stage
        at_rows = pl.ds(pl.multiple_of((source * 2 + side) * half, half), half)
        if kind == "mix":
            tall = unit_chans // 2
            at = pl.ds(pl.multiple_of(side * tall, tall), tall)
            outs = mix_out.at[source, at, :]
            if whole:
                return [mix_in.at[at_rows, :], outs]
            lanes = [pl.ds(b * unit_chans, unit_chans) for b in range(3)]
            return [*(mix_in.at[at_rows, lane] for lane in lanes), outs]
        if kind == "in":
            if whole:
                return [ffn_in.at[i, at_rows, :]]
            return [ffn_in.at[i, at_rows, pl.ds(b * LANES, LANES)] for b in (0, 1)]
        tall = units // 2
        at = pl.ds(pl.multiple_of(side * tall, tall), tall)
        lanes = pl.ds(pl.multiple_of(source * LANES, LANES), LANES)
        return [ffn_out.at[i, at, lanes]]

    def slot(stage, i):
        kind, at = stage
        if kind == "mix":
            return i
        return 2 + at if kind == "in" else 2 + n_in + at

    def group(stage, i):
        kind, _ = stage
        return i if kind == "mix" else {"in": 2, "out": 3}[kind]

    def to_fs(src, dst, send_sem, recv_sem, to):
        return pltpu.make_async_remote_copy(
            src_ref=src,
            dst_ref=dst,
            send_sem=send_sem,
            recv_sem=recv_sem,
            device_id={"fs": to},
            device_id_type=MESH,
        )

    def z_sends(s, d):
        to = other(d)
        pairs = zip(sources(s, lax.rem(to, 2), g), places(s, j, g, False))
        copies = []
        for i, (src, dst) in enumerate(pairs):
            wide = i // 3 if s[0] == "mix" else 0
            sems = z_send.at[group(s, wide)], z_recv.at[slot(s, wide), j]
            copies.append(to_fs(src, dst, *sems, to))
        return copies

    def z_takes(s, d):
        source = other(d)
        return [
            to_fs(view, view, z_send.at[group(s, i)], z_recv.at[slot(s, i), source], source)
            for i, view in enumerate(places(s, source, g, True))
        ]

    def z_forwards(s):
        source = other(n_fs - 1)
        return [
            to_fs(view, view, f_send.at[group(s, i)], z_recv.at[slot(s, i), source], other(n_fs - 2))
            for i, view in enumerate(places(s, source, g, True))
        ]

    def to_y(src, dst, send_sem, recv_sem):
        return pltpu.make_async_remote_copy(
            src_ref=src,
            dst_ref=dst,
            send_sem=send_sem,
            recv_sem=recv_sem,
            device_id={"grp": 1 - g},
            device_id_type=MESH,
        )

    def y_copies(s, d):
        return [
            to_y(view, view, y_send.at[group(s, i)], y_recv.at[slot(s, i)])
            for i, view in enumerate(places(s, other(d), g, True))
        ]

    n_from = n_fs - 1

    def sums(stage):
        kind, i = stage
        if kind == "mix":
            some = mix_out.at[pl.ds(0, n_from), pl.ds(0, unit_chans // 2), :]
            return [mix_in.at[pl.ds(0, n_from * half), :], some]
        if kind == "in":
            return [ffn_in.at[i, pl.ds(0, n_from * half), :]]
        return [ffn_out.at[i, pl.ds(0, units // 2), pl.ds(0, n_from * LANES)]]

    def all_sums(count):
        return [
            mix_in.at[pl.ds(0, count * half), :],
            mix_out.at[pl.ds(0, count), pl.ds(0, unit_chans // 2), :],
            ffn_in.at[:, pl.ds(0, count * half), :],
            ffn_out.at[:, pl.ds(0, units // 2), pl.ds(0, count * LANES)],
        ]

    def start(copies):
        for copy in copies:
            copy.start()

    def wait_recv(copies):
        for copy in copies:
            copy.wait_recv()

    def wait_send(copies):
        for copy in copies:
            copy.wait_send()

    def send(s, ds):
        for d in ds:
            start(z_sends(s, d))

    straight, last = range(1, n_fs - 1), n_fs - 1

    def relay(s, d):
        wait_recv(z_takes(s, d))
        start(y_copies(s, d))

    def relay_all(s, following=()):
        relay(s, 1)

        @pl.when(at_end)
        def _():
            for d in range(2, n_fs):
                relay(s, d)

        @pl.when(jnp.logical_not(at_end))
        def _():
            relay(s, last)
            start(z_forwards(s))
            for later in following:
                send(later, straight)
            for d in range(2, n_fs - 1):
                relay(s, d)

    def arrived(s):
        for i, view in enumerate(sums(s)):
            to_y(view, view, y_send.at[group(s, i)], y_recv.at[slot(s, i)]).wait_recv()

    def to_tp(src, dst, send_sem, recv_sem, to):
        return pltpu.make_async_remote_copy(
            src_ref=src,
            dst_ref=dst,
            send_sem=send_sem,
            recv_sem=recv_sem,
            device_id={"tp": to},
            device_id_type=MESH,
        )

    def all_copies(buffer, i, at, kind):
        sent = all_send.at[0 if i < 2 else 1]
        copies = []
        for dx in range(n_x):
            there = lax.rem(x + dx, n_x)
            if kind == "over":
                if dx:
                    view = buffer.at[k, at]
                    copies.append(to_tp(view, view, sent, all_recv.at[i, dx - 1], there * 2 + c))
            else:
                back = lax.rem(x + n_x - dx, n_x) * 2
                seen = back + c if kind == "pass" else back + 1 - c
                view = buffer.at[seen, at]
                copies.append(to_tp(view, view, sent, all_recv.at[i, n_x - 1 + dx], core))
        return copies

    def all_begin(buffer, i, at):
        start(all_copies(buffer, i, at, "over"))
        all_copies(buffer, i, at, "pass")[0].start()

    def all_middle(buffer, i, at):
        passed = all_copies(buffer, i, at, "pass")
        for dx in range(1, n_x):
            view = buffer.at[lax.rem(x + n_x - dx, n_x) * 2 + c, at]
            sent = all_send.at[0 if i < 2 else 1]
            to_tp(view, view, sent, all_recv.at[i, dx - 1], core).wait_recv()
            passed[dx].start()

    def all_end(buffer, i, at):
        wait_recv(all_copies(buffer, i, at, "take"))

    def to_pair(i, src, dst):
        return pltpu.make_async_remote_copy(
            src_ref=src,
            dst_ref=dst,
            send_sem=pair_send.at[0],
            recv_sem=pair_recv.at[i],
            device_id={"fs": pair},
            device_id_type=MESH,
        )

    halves = range(SEQS_DEV)
    mine, theirs = held_rows(MINE), held_rows(THEIRS)

    def tok_swap(at):
        return to_pair(0, tok.at[k, at], tok.at[k, at])

    def res_swap(o, h):
        view = res.at[k, held_rows(o, h)]
        return to_pair(1 + h, view, view)

    def mix_swap(h):
        return to_pair(1 + SEQS_DEV + h, mix_z_sum.at[h], mix_z_got.at[h])

    def back(u):
        return to_pair(1 + 2 * SEQS_DEV + u, sum_z.at[u], got_z.at[u])

    barrier = pltpu.get_barrier_semaphore()
    for d in range(1, n_fs):
        to = lax.rem(j + d, n_fs)
        pl.semaphore_signal(barrier, inc=1, device_id={"fs": to}, device_id_type=MESH)
    pl.semaphore_signal(barrier, inc=1, device_id={"grp": 1 - g}, device_id_type=MESH)
    for d in range(1, n_tp):
        to = lax.rem(k + d, n_tp)
        pl.semaphore_signal(barrier, inc=1, device_id={"tp": to}, device_id_type=MESH)

    first = pltpu.make_async_copy(tokens, tok.at[k, mine], load_sem.at[4])
    own_rows = pl.ds(pl.multiple_of(j * shard, shard), shard)
    own_lanes = pl.ds(pl.multiple_of(j * LANES, LANES), LANES)
    at_chans = pl.ds(pl.multiple_of(p * unit_chans, unit_chans), unit_chans)
    at_units = pl.ds(pl.multiple_of(p * units, units), units)

    def load(i, src, dst):
        pltpu.make_async_copy(src, dst, load_sem.at[i]).start()

    first.start()
    for i, ref in enumerate((w_signal, w_outer_gate, w_inner_gate)):
        load(0, ref.at[:, at_chans], mix_in.at[own_rows, pl.ds(i * unit_chans, unit_chans)])
    load(1, w_mix_out.at[at_chans, :], mix_out.at[j])
    for t in range(n_in):
        lanes = pl.ds(pl.multiple_of(p * units + t * LANES, LANES), LANES)
        for i, ref in enumerate((w_gate, w_value)):
            load(2, ref.at[:, lanes], ffn_in.at[t, own_rows, pl.ds(i * LANES, LANES)])
    for u in range(n_out):
        load(3, w_down.at[at_units, pl.ds(u * LANES, LANES)], ffn_out.at[u, :, own_lanes])
    loaded = [
        mix_in.at[own_rows, :],
        mix_out.at[j],
        ffn_in.at[:, own_rows, :],
        ffn_out.at[:, :, own_lanes],
    ]
    with jax.named_scope("barrier"):
        first.wait()
        pl.semaphore_wait(barrier, n_fs - 1 + 1 + n_tp - 1)

    send(mix, (1,))

    @pl.when(at_end)
    def _():
        tok_swap(mine).start()
        all_begin(tok, 0, mine)
        send(mix, range(2, n_fs - 1))

    @pl.when(jnp.logical_not(at_end))
    def _():
        send(mix, (last,))
        tok_swap(mine).start()
        all_begin(tok, 0, mine)
        send(mix, range(2, n_fs - 1))

    with jax.named_scope("loads"):
        for i, view in enumerate(loaded):
            pltpu.make_async_copy(view, view, load_sem.at[i]).wait()

    def norm(buffer, at, gain):
        count = at.size
        squares = jnp.zeros((count, 1), jnp.float32)
        for b in range(n_tp):
            values = buffer[b, at, :].astype(jnp.float32)
            squares = squares + jnp.sum(values * values, axis=-1, keepdims=True)
        scale = lax.rsqrt(squares / (n_tp * own_cols) + 1e-06)
        for b in range(n_tp):
            cut = slice(b * own_cols, (b + 1) * own_cols)
            values = buffer[b, at, :].astype(jnp.float32)
            normed[at, cut] = (values * scale * gain[:, cut]).astype(jnp.bfloat16)

    with jax.named_scope("tok_mid"):
        all_middle(tok, 0, mine)
    with jax.named_scope("relay_mix1"):
        relay(mix, 1)

    @pl.when(at_end)
    def _():
        with jax.named_scope("relay_mix2"):
            relay(mix, 2)

    @pl.when(jnp.logical_not(at_end))
    def _():
        with jax.named_scope("relay_mix2"):
            relay(mix, last)
            start(z_forwards(mix))

    with jax.named_scope("norm_mine"):
        all_end(tok, 0, mine)
        norm(tok, mine, mix_gain)
    with jax.named_scope("tok_swap"):
        tok_swap(theirs).wait_recv()
        all_begin(tok, 1, theirs)

    @pl.when(at_end)
    def _():
        with jax.named_scope("relay_mix3"):
            relay(mix, last)
        for s in order[1:4]:
            send(s, straight)

    @pl.when(jnp.logical_not(at_end))
    def _():
        with jax.named_scope("relay_mix3"):
            relay(mix, 2)
        for s in order[1:3]:
            send(s, straight)
        for s in order[1:4]:
            send(s, (last,))

    with jax.named_scope("tok_theirs"):
        all_middle(tok, 1, theirs)
    with jax.named_scope("norm_theirs"):
        all_end(tok, 1, theirs)
        norm(tok, theirs, mix_gain)
    with jax.named_scope("arrived_mix"):
        arrived(mix)
    taps = [mix_taps[i : i + 1, at_chans] for i in range(3)]

    def mix_core_copy(o, dx):
        there = lax.rem(x + dx, n_x)
        return to_tp(
            part_mix.at[o, there * 2 + 1 - c],
            mix_core.at[o, there],
            mix_core_send.at[0],
            mix_core_recv.at[o, dx],
            core,
        )

    def mix_x_copy(o, h, dx):
        to = lax.rem(x + dx, n_x) * 2 + c
        return to_tp(
            mix_x_sum.at[o, h, dx - 1],
            mix_x_got.at[o, h, dx - 1],
            mix_x_send.at[0],
            mix_x_recv.at[o, h, dx - 1],
            to,
        )

    def mix_chip_sum(o, h, dx):
        there = lax.rem(x + dx, n_x)
        cut = in_half(h)
        near = part_mix[o, there * 2 + c, cut, :].astype(jnp.float32)
        return near + mix_core[o, there, cut, :].astype(jnp.float32)

    def mix_place_sum(o, h):
        value = mix_chip_sum(o, h, 0)
        for dx in range(1, n_x):
            value = value + mix_x_got[o, h, dx - 1].astype(jnp.float32)
        return value

    with jax.named_scope("mixer"):
        for o, at in ((THEIRS, theirs), (MINE, mine)):
            both = jnp.dot(normed[at, :], mix_in[...], preferred_element_type=jnp.float32)
            both = both.astype(jnp.bfloat16).astype(jnp.float32)
            gated = both[:, 2 * unit_chans :] * both[:, :unit_chans]
            conv = conv_rows(gated, taps, length)
            mixed = (both[:, unit_chans : 2 * unit_chans] * conv).astype(jnp.bfloat16)
            for b in range(n_fs):
                terms = jnp.dot(mixed, mix_out[b], preferred_element_type=jnp.float32)
                part_mix[o, b] = terms.astype(jnp.bfloat16)
            for dx in (*range(1, n_x), 0):
                mix_core_copy(o, dx).start()

    with jax.named_scope("mix_core"):
        for o in (THEIRS, MINE):
            for dx in range(1, n_x):
                mix_core_copy(o, dx).wait_recv()
                for h in halves:
                    mix_x_sum[o, h, dx - 1] = mix_chip_sum(o, h, dx).astype(jnp.bfloat16)
                    mix_x_copy(o, h, dx).start()
            mix_core_copy(o, 0).wait_recv()
    with jax.named_scope("relay_in0"):
        relay_all(order[1], order[3:4])
    with jax.named_scope("mix_x_theirs"):
        for h in halves:
            for dx in range(1, n_x):
                mix_x_copy(THEIRS, h, dx).wait_recv()
            mix_z_sum[h] = mix_place_sum(THEIRS, h).astype(jnp.bfloat16)
            mix_swap(h).start()

    with jax.named_scope("relay_in1"):
        relay_all(order[2], order[4:5])
    with jax.named_scope("mix_mine"):
        for h in halves:
            for dx in range(1, n_x):
                mix_x_copy(MINE, h, dx).wait_recv()
            mix_swap(h).wait_recv()
            mixer = mix_place_sum(MINE, h) + mix_z_got[h].astype(jnp.float32)
            at = held_rows(MINE, h)
            res[k, at, :] = (tok[k, at, :].astype(jnp.float32) + mixer).astype(jnp.bfloat16)
            res_swap(MINE, h).start()
            all_begin(res, 2 + h, at)

    @pl.when(at_end)
    def _():
        for s in order[4:]:
            send(s, straight)

    @pl.when(jnp.logical_not(at_end))
    def _():
        for s in order[4:]:
            send(s, (last,))


    with jax.named_scope("relay_in2"):
        relay_all(order[3], order[5:6])
    with jax.named_scope("res_mid"):
        for h in halves:
            all_middle(res, 2 + h, held_rows(MINE, h))
    with jax.named_scope("res_swap"):
        for h in halves:
            res_swap(THEIRS, h).wait_recv()
            all_begin(res, 2 + SEQS_DEV + h, held_rows(THEIRS, h))
    with jax.named_scope("res_norm"):
        for h in halves:
            all_end(res, 2 + h, held_rows(MINE, h))
            norm(res, held_rows(MINE, h), ffn_gain)
    with jax.named_scope("res_mid2"):
        for h in halves:
            all_middle(res, 2 + SEQS_DEV + h, held_rows(THEIRS, h))
    with jax.named_scope("relay_in3"):
        relay_all(order[4], order[6:7])
    with jax.named_scope("res_norm2"):
        for h in halves:
            all_end(res, 2 + SEQS_DEV + h, held_rows(THEIRS, h))
            norm(res, held_rows(THEIRS, h), ffn_gain)

    def feed(t):
        with jax.named_scope("in_wait"):
            arrived(("in", t))
        cut = pl.ds(pl.multiple_of(p * units + t * LANES, LANES), LANES)
        both = jnp.dot(normed[...], ffn_in[t], preferred_element_type=jnp.float32)
        both = both.astype(jnp.bfloat16).astype(jnp.float32)
        gate_taps, value_taps = ([up_taps[i, b : b + 1, cut] for i in range(3)] for b in (0, 1))
        gate = conv_rows(both[:, :LANES], gate_taps, length) + up_bias[0:1, cut]
        value = conv_rows(both[:, LANES:], value_taps, length) + up_bias[1:2, cut]
        unit = (gate / (1.0 + jnp.exp(-gate)) * value).astype(jnp.bfloat16)
        hidden[:, pl.ds(pl.multiple_of(t * LANES, LANES), LANES)] = unit

    beside = {2: 5, 3: 6, 4: 7}

    @pl.loop(0, n_in)
    def _(t):
        for at, index in beside.items():

            @pl.when(t == at)
            def _():
                with jax.named_scope("relay_out"):
                    relay_all(order[index], order[index + 2 : index + 3])

        feed(t)

    def core_copy(u, dx):
        there = lax.rem(x + dx, n_x)
        return to_tp(
            part_ffn.at[u, :, there * 2 + 1 - c],
            got_core.at[u, :, there],
            core_send.at[0],
            core_recv.at[u, dx],
            core,
        )

    def x_copy(u, dx):
        to = lax.rem(x + dx, n_x) * 2 + c
        sems = x_send.at[0], x_recv.at[u, dx - 1]
        return to_tp(sum_x.at[u, dx - 1], got_x.at[u, dx - 1], *sems, to)

    def chip_sum(u, o, dx):
        there = lax.rem(x + dx, n_x)
        mine_there = part_ffn[u, o, there * 2 + c].astype(jnp.float32)
        return mine_there + got_core[u, o, there].astype(jnp.float32)

    def place_sum(u, o):
        value = chip_sum(u, o, 0)
        for dx in range(1, n_x):
            value = value + got_x[u, dx - 1, o].astype(jnp.float32)
        return value

    def down(u):
        with jax.named_scope("out_wait"):
            arrived(("out", u))
        for o, at in enumerate((theirs, mine)):
            terms = jnp.dot(hidden[at, :], ffn_out[u], preferred_element_type=jnp.float32)
            for b in range(n_tp):
                part_ffn[u, o, b] = terms[:, b * LANES : (b + 1) * LANES].astype(jnp.bfloat16)
        for dx in (*range(1, n_x), 0):
            core_copy(u, dx).start()

    def over_x(u):
        for dx in range(1, n_x):
            core_copy(u, dx).wait_recv()
            for o in (0, 1):
                sum_x[u, dx - 1, o] = chip_sum(u, o, dx).astype(jnp.bfloat16)
            x_copy(u, dx).start()

    def over_z(u):
        core_copy(u, 0).wait_recv()
        for dx in range(1, n_x):
            x_copy(u, dx).wait_recv()
        sum_z[u] = place_sum(u, 0).astype(jnp.bfloat16)
        back(u).start()

    for u in range(n_out):
        if 8 + u < len(order):
            with jax.named_scope("relay_out2"):
                relay_all(order[8 + u], order[10 + u : 11 + u])
        with jax.named_scope("down"):
            down(u)
        if u >= 1:
            with jax.named_scope("over_x"):
                over_x(u - 1)
        if u >= 2:
            with jax.named_scope("over_z"):
                over_z(u - 2)
    with jax.named_scope("over_x_last"):
        over_x(n_out - 1)
    for u in range(max(n_out - 2, 0), n_out):
        with jax.named_scope("over_z_last"):
            over_z(u)
    with jax.named_scope("final"):
        for u in range(n_out):
            cut = slice(u * LANES, (u + 1) * LANES)
            value = res[k, mine, cut].astype(jnp.float32) + place_sum(u, 1)
            back(u).wait_recv()
            out[:, cut] = (value + got_z[u].astype(jnp.float32)).astype(jnp.bfloat16)

    with jax.named_scope("drain"):
        for i, view in enumerate(all_sums(n_from)):
            to_y(view, view, y_send.at[i], y_recv.at[0]).wait_send()

        @pl.when(at_end)
        def _():
            for i, view in enumerate(all_sums(n_from - 1)):
                to_fs(view, view, z_send.at[i], z_recv.at[0, 0], pair).wait_send()

        @pl.when(jnp.logical_not(at_end))
        def _():
            for i, view in enumerate(all_sums(n_from)):
                to_fs(view, view, z_send.at[i], z_recv.at[0, 0], pair).wait_send()
            for i, view in enumerate(all_sums(1)):
                to_fs(view, view, f_send.at[i], z_recv.at[0, 0], pair).wait_send()

        for i, buffer in enumerate((tok, res)):
            view = buffer.at[pl.ds(0, n_tp - 1)]
            to_tp(view, view, all_send.at[i], all_recv.at[0, 0], core).wait_send()
        view = part_mix.at[:, pl.ds(0, n_x)]
        to_tp(view, view, mix_core_send.at[0], all_recv.at[0, 0], core).wait_send()
        to_tp(mix_x_sum, mix_x_sum, mix_x_send.at[0], all_recv.at[0, 0], core).wait_send()
        view = part_ffn.at[:, :, pl.ds(0, n_x)]
        to_tp(view, view, core_send.at[0], all_recv.at[0, 0], core).wait_send()
        to_tp(sum_x, sum_x, x_send.at[0], all_recv.at[0, 0], core).wait_send()
        view = tok.at[pl.ds(0, 2)]
        to_pair(0, view, view).wait_send()


def fused(n_fs, n_tp, *args):
    tokens, w_signal, w_gate = args[0], args[2], args[8]
    rows, cols = tokens.shape
    shard, chans = w_signal.shape
    units = w_gate.shape[1] // 2
    n_in, n_out = units // LANES, shard // LANES
    width = n_fs * shard
    args = list(args)
    args[1], args[7] = args[1].reshape(1, -1), args[7].reshape(1, -1)
    args[10] = args[10].transpose(1, 0, 2)
    in_vmem = {1, 5, 7, 10, 11}
    n_x = n_tp // 2
    length = rows // SEQS_DEV
    dma = pltpu.SemaphoreType.DMA

    def held(*shape):
        return pltpu.VMEM(shape, jnp.bfloat16)

    return pl.pallas_call(
        functools.partial(layer_kernel, n_fs, n_tp),
        out_shape=jax.ShapeDtypeStruct((rows, cols), jnp.bfloat16),
        in_specs=[
            pl.BlockSpec(memory_space=pltpu.VMEM if i in in_vmem else pl.ANY)
            for i in range(len(args))
        ],
        out_specs=pl.BlockSpec(memory_space=pltpu.VMEM),
        scratch_shapes=[
            held(width, 3 * (chans // 2)),
            held(n_fs, chans // 2, shard),
            held(n_in, width, 2 * LANES),
            held(n_out, units, n_fs * LANES),
            held(n_tp, 2 * rows, cols),
            held(n_tp, 2 * rows, cols),
            held(2 * rows, width),
            held(2 * rows, units),
            held(2, n_tp, rows, cols),
            held(2, n_x, rows, cols),
            held(2, SEQS_DEV, n_x - 1, length, cols),
            held(2, SEQS_DEV, n_x - 1, length, cols),
            held(SEQS_DEV, length, cols),
            held(SEQS_DEV, length, cols),
            held(n_out, 2, n_tp, rows, LANES),
            held(n_out, 2, n_x, rows, LANES),
            held(n_out, n_x - 1, 2, rows, LANES),
            held(n_out, n_x - 1, 2, rows, LANES),
            held(n_out, rows, LANES),
            held(n_out, rows, LANES),
            dma((4,)),
            dma((2 + n_in + n_out, n_fs)),
            dma((4,)),
            dma((4,)),
            dma((2 + n_in + n_out,)),
            dma((5,)),
            dma((2,)),
            dma((2 + 2 * SEQS_DEV, 2 * n_x - 1)),
            dma((1,)),
            dma((2, n_x)),
            dma((1,)),
            dma((2, SEQS_DEV, n_x - 1)),
            dma((1,)),
            dma((n_out, n_x)),
            dma((1,)),
            dma((n_out, n_x - 1)),
            dma((1,)),
            dma((1 + 2 * SEQS_DEV + n_out,)),
        ],
        compiler_params=pltpu.CompilerParams(
            collective_id=0, has_side_effects=True, vmem_limit_bytes=62 * 1024 * 1024
        ),
    )(*args)


def solution(mesh):
    n_fs, n_tp = mesh.shape["fs"], mesh.shape["tp"]
    body = functools.partial(fused, n_fs, n_tp)
    if n_fs != 4 or n_tp != 4 or mesh.shape["grp"] != 2:
        body = on_device
    placed = (
        P(("grp", "fs"), "tp"),
        P(),
        P("fs", "tp"),
        P("fs", "tp"),
        P("fs", "tp"),
        P(None, "tp"),
        P("tp", "fs"),
        P(),
        P("fs", "tp"),
        P("fs", "tp"),
        P(None, None, "tp"),
        P(None, "tp"),
        P("tp", "fs"),
    )
    return jax.shard_map(
        body, mesh=mesh, in_specs=placed, out_specs=P(("grp", "fs"), "tp"), check_vma=False
    )
```

```python
import functools

import jax
import jax.numpy as jnp
from jax import lax
from jax.experimental import pallas as pl
from jax.experimental.pallas import tpu as pltpu
from jax.sharding import PartitionSpec as P

SEQS_DEV = 2


def conv_positions(values, taps):
    width = values.shape[1]
    blocks = values.reshape(SEQS_DEV, -1, width)
    length = blocks.shape[1]
    padded = jnp.pad(blocks, ((0, 0), (2, 0), (0, 0)))
    result = (
        padded[:, 0:length] * taps[0]
        + padded[:, 1 : length + 1] * taps[1]
        + padded[:, 2 : length + 2] * taps[2]
    )
    return result.reshape(-1, width)


def rms_norm(stream, gain):
    values = stream.astype(jnp.float32)
    scale = lax.rsqrt(jnp.mean(values * values, axis=-1, keepdims=True) + 1e-06)
    return (values * scale * gain).astype(jnp.bfloat16)


def on_device(
    tokens,
    mix_gain,
    w_signal,
    w_outer_gate,
    w_inner_gate,
    mix_taps,
    w_mix_out,
    ffn_gain,
    w_gate,
    w_value,
    up_taps,
    up_bias,
    w_down,
):
    whole = lax.all_gather(tokens, "tp", axis=1, tiled=True)
    normed = rms_norm(whole, mix_gain)
    pieces = (
        lax.all_gather(w_signal, "fs", axis=0, tiled=True),
        lax.all_gather(w_outer_gate, "fs", axis=0, tiled=True),
        lax.all_gather(w_inner_gate, "fs", axis=0, tiled=True),
    )
    columns = normed
    signal, outer, inner = tuple(
        (jnp.dot(columns, piece, preferred_element_type=jnp.float32) for piece in pieces)
    )
    signal = signal.astype(jnp.bfloat16).astype(jnp.float32)
    outer = outer.astype(jnp.bfloat16).astype(jnp.float32)
    inner = inner.astype(jnp.bfloat16).astype(jnp.float32)
    mixed = (outer * conv_positions(inner * signal, mix_taps)).astype(jnp.bfloat16)
    mix_terms = jnp.dot(
        mixed,
        lax.all_gather(w_mix_out, "fs", axis=1, tiled=True),
        preferred_element_type=jnp.float32,
    )
    mix_sum = lax.psum_scatter(
        mix_terms.astype(jnp.bfloat16), "tp", scatter_dimension=1, tiled=True
    ).astype(jnp.float32)
    resid = (tokens.astype(jnp.float32) + mix_sum).astype(jnp.bfloat16)
    whole_ffn = lax.all_gather(resid, "tp", axis=1, tiled=True)
    normed_ffn = rms_norm(whole_ffn, ffn_gain)
    pieces = (
        lax.all_gather(w_gate, "fs", axis=0, tiled=True),
        lax.all_gather(w_value, "fs", axis=0, tiled=True),
    )
    columns = normed_ffn
    gate = jnp.dot(columns, pieces[0], preferred_element_type=jnp.float32)
    value = jnp.dot(columns, pieces[1], preferred_element_type=jnp.float32)
    gate = gate.astype(jnp.bfloat16).astype(jnp.float32)
    value = value.astype(jnp.bfloat16).astype(jnp.float32)
    gate_conv = conv_positions(gate, up_taps[0]) + up_bias[0]
    value_conv = conv_positions(value, up_taps[1]) + up_bias[1]
    hidden = (jax.nn.silu(gate_conv) * value_conv).astype(jnp.bfloat16)
    ffn_terms = jnp.dot(
        hidden, lax.all_gather(w_down, "fs", axis=1, tiled=True), preferred_element_type=jnp.float32
    )
    ffn_sum = lax.psum_scatter(
        ffn_terms.astype(jnp.bfloat16), "tp", scatter_dimension=1, tiled=True
    ).astype(jnp.float32)
    return (resid.astype(jnp.float32) + ffn_sum).astype(jnp.bfloat16)


MESH = pl.DeviceIdType.MESH
UP, DOWN = 0, 1
LANES = 128


def shifted(values, by, length):
    rolled = pltpu.roll(values, by, 0)
    position = lax.rem(lax.broadcasted_iota(jnp.int32, values.shape, 0), length)
    return jnp.where(position < by, 0.0, rolled)


def conv_rows(values, taps, length):
    return (
        shifted(values, 2, length) * taps[0]
        + shifted(values, 1, length) * taps[1]
        + values * taps[2]
    )


END, INNER = 0, 1


def tiles_of(n_tiles, role):
    at_end = 2 * n_tiles // 5
    return at_end if role == END else n_tiles - at_end


def layer_kernel(
    n_fs,
    n_tp,
    tokens,
    mix_gain,
    w_signal,
    w_outer_gate,
    w_inner_gate,
    mix_taps,
    w_mix_out,
    ffn_gain,
    w_gate,
    w_value,
    up_taps,
    up_bias,
    w_down,
    out,
    mix_in,
    mix_out,
    ffn_in,
    ffn_out,
    tok,
    res,
    normed,
    hidden,
    part_mix,
    mix_core,
    mix_x_sum,
    mix_x_got,
    mix_z_sum,
    mix_z_got,
    part_ffn,
    got_core,
    sum_x,
    got_x,
    sum_z,
    got_z,
    z_send,
    z_recv,
    f_send,
    y_send,
    y_recv,
    load_sem,
    all_send,
    all_recv,
    mix_core_send,
    mix_core_recv,
    mix_x_send,
    mix_x_recv,
    core_send,
    core_recv,
    x_send,
    x_recv,
    pair_send,
    pair_recv,
):
    g, j, k = lax.axis_index("grp"), lax.axis_index("fs"), lax.axis_index("tp")
    rows, own_cols = tokens.shape
    length = rows // SEQS_DEV
    shard, chans = w_signal.shape
    half, unit_chans = shard // 2, chans // 2
    n_tiles, n_out = w_gate.shape[1] // LANES, shard // LANES
    tiles = {END: tiles_of(n_tiles, END), INNER: tiles_of(n_tiles, INNER)}
    base = {END: 0, INNER: tiles[END]}
    n_x = n_tp // 2
    x, c = k // 2, lax.rem(k, 2)
    core = k + 1 - 2 * c
    p = lax.rem(j, 2)
    pair = j + 1 - 2 * p
    inward = jnp.where(j < n_fs // 2, 1, n_fs - 1)
    at_end = (j == 0) | (j == n_fs - 1)

    MINE, THEIRS = 0, 1

    def held_rows(o, h=None):
        side = p if o == MINE else 1 - p
        if h is None:
            return pl.ds(pl.multiple_of(side * rows, rows), rows)
        return pl.ds(pl.multiple_of(side * rows + h * length, length), length)

    def in_half(h):
        return slice(h * length, (h + 1) * length)

    mix = ("mix", 0)
    n_in = tiles[INNER]
    ins = [("in", t) for t in range(n_in)]
    outs = [("out", u) for u in range(n_out)]

    def by_role(body):
        pl.when(at_end)(functools.partial(body, END))
        pl.when(jnp.logical_not(at_end))(functools.partial(body, INNER))


    def other(d):
        return lax.rem(j + inward * d, n_fs)

    def sources(stage, role, side):
        kind, i = stage
        at_rows = pl.ds(pl.multiple_of(side * half, half), half)
        if kind == "mix":
            lanes = pl.ds(role * unit_chans, unit_chans)
            tall = unit_chans // 2
            at = pl.ds(pl.multiple_of(role * unit_chans + side * tall, tall), tall)
            refs = [ref.at[at_rows, lanes] for ref in (w_signal, w_outer_gate, w_inner_gate)]
            return [*refs, w_mix_out.at[at, :]]
        if kind == "in":
            lanes = pl.ds((base[role] + i) * LANES, LANES)
            return [w_gate.at[at_rows, lanes], w_value.at[at_rows, lanes]]
        tall = tiles[role] * LANES // 2
        at = pl.ds(pl.multiple_of(base[role] * LANES + side * tall, LANES), tall)
        return [w_down.at[at, pl.ds(i * LANES, LANES)]]

    def places(stage, role, source, side, whole):
        kind, i = stage
        at_rows = pl.ds(pl.multiple_of((source * 2 + side) * half, half), half)
        if kind == "mix":
            tall = unit_chans // 2
            at = pl.ds(pl.multiple_of(side * tall, tall), tall)
            outs = mix_out.at[source, at, :]
            if whole:
                return [mix_in.at[at_rows, :], outs]
            lanes = [pl.ds(b * unit_chans, unit_chans) for b in range(3)]
            return [*(mix_in.at[at_rows, lane] for lane in lanes), outs]
        if kind == "in":
            if whole:
                return [ffn_in.at[i, at_rows, :]]
            return [ffn_in.at[i, at_rows, pl.ds(b * LANES, LANES)] for b in (0, 1)]
        tall = tiles[role] * LANES // 2
        at = pl.ds(pl.multiple_of(side * tall, LANES), tall)
        lanes = pl.ds(pl.multiple_of(source * LANES, LANES), LANES)
        return [ffn_out.at[i, at, lanes]]

    def slot(stage, i):
        kind, at = stage
        if kind == "mix":
            return i
        return 2 + at if kind == "in" else 2 + n_in + at

    def group(stage, i):
        kind, _ = stage
        return i if kind == "mix" else {"in": 2, "out": 3}[kind]

    def to_fs(src, dst, send_sem, recv_sem, to):
        return pltpu.make_async_remote_copy(
            src_ref=src,
            dst_ref=dst,
            send_sem=send_sem,
            recv_sem=recv_sem,
            device_id={"fs": to},
            device_id_type=MESH,
        )

    def role_of(role, d):
        return INNER if d < n_fs - 1 - role else END

    def z_sends(s, role, d):
        to = other(d)
        there = role_of(role, d)
        pairs = zip(sources(s, there, g), places(s, there, j, g, False))
        copies = []
        for i, (src, dst) in enumerate(pairs):
            wide = i // 3 if s[0] == "mix" else 0
            sems = z_send.at[group(s, wide), d - 1], z_recv.at[slot(s, wide), j]
            copies.append(to_fs(src, dst, *sems, to))
        return copies

    def z_takes(s, role, d):
        source = other(d)
        return [
            to_fs(view, view, z_send.at[group(s, i), 0], z_recv.at[slot(s, i), source], source)
            for i, view in enumerate(places(s, role, source, g, True))
        ]

    def z_forwards(s):
        source = other(last)
        return [
            to_fs(view, view, f_send.at[group(s, i)], z_recv.at[slot(s, i), source], other(1))
            for i, view in enumerate(places(s, INNER, source, g, True))
        ]

    def to_y(src, dst, send_sem, recv_sem):
        return pltpu.make_async_remote_copy(
            src_ref=src,
            dst_ref=dst,
            send_sem=send_sem,
            recv_sem=recv_sem,
            device_id={"grp": 1 - g},
            device_id_type=MESH,
        )

    def y_copies(s, role, d):
        return [
            to_y(view, view, y_send.at[group(s, i)], y_recv.at[slot(s, i)])
            for i, view in enumerate(places(s, role, other(d), g, True))
        ]

    n_from = n_fs - 1

    def sums(stage, role, count):
        kind, i = stage
        if kind == "mix":
            some = mix_out.at[pl.ds(0, count), pl.ds(0, unit_chans // 2), :]
            return [mix_in.at[pl.ds(0, count * half), :], some]
        if kind == "in":
            return [ffn_in.at[i, pl.ds(0, count * half), :]]
        return [ffn_out.at[i, pl.ds(0, tiles[role] * LANES // 2), pl.ds(0, count * LANES)]]

    def all_sums(role, count):
        return [
            *sums(mix, role, count),
            *sums(("in", pl.ds(0, tiles[role])), role, count),
            *sums(("out", pl.ds(0, n_out)), role, count),
        ]

    def start(copies):
        for copy in copies:
            copy.start()

    def wait_recv(copies):
        for copy in copies:
            copy.wait_recv()

    def wait_send(copies):
        for copy in copies:
            copy.wait_send()

    def send(s, role, ds):
        for d in ds:
            if s[0] != "in" or s[1] < tiles[role_of(role, d)]:
                start(z_sends(s, role, d))

    last = n_fs - 1

    def relay(s, role, d):
        wait_recv(z_takes(s, role, d))
        start(y_copies(s, role, d))

    def ahead(s):
        relay(s, INNER, last)
        start(z_forwards(s))

    def relay_all(s, role):
        if s[0] == "in" and s[1] >= tiles[role]:
            return
        for d in (1, 2, last) if role == END else (1, 2):
            relay(s, role, d)

    def relay_both(s):
        by_role(lambda role: relay_all(s, role))

    def arrived(s, role):
        for i, view in enumerate(sums(s, role, n_from)):
            to_y(view, view, y_send.at[group(s, i)], y_recv.at[slot(s, i)]).wait_recv()

    def to_tp(src, dst, send_sem, recv_sem, to):
        return pltpu.make_async_remote_copy(
            src_ref=src,
            dst_ref=dst,
            send_sem=send_sem,
            recv_sem=recv_sem,
            device_id={"tp": to},
            device_id_type=MESH,
        )

    def all_copies(buffer, i, at, kind):
        sent = all_send.at[0 if i <= SEQS_DEV else 1]
        copies = []
        for dx in range(n_x):
            there = lax.rem(x + dx, n_x)
            if kind == "over":
                if dx:
                    view = buffer.at[k, at]
                    copies.append(to_tp(view, view, sent, all_recv.at[i, dx - 1], there * 2 + c))
            else:
                back = lax.rem(x + n_x - dx, n_x) * 2
                seen = back + c if kind == "pass" else back + 1 - c
                view = buffer.at[seen, at]
                copies.append(to_tp(view, view, sent, all_recv.at[i, n_x - 1 + dx], core))
        return copies

    def all_begin(buffer, i, at):
        start(all_copies(buffer, i, at, "over"))
        all_copies(buffer, i, at, "pass")[0].start()

    def all_middle(buffer, i, at):
        passed = all_copies(buffer, i, at, "pass")
        for dx in range(1, n_x):
            view = buffer.at[lax.rem(x + n_x - dx, n_x) * 2 + c, at]
            sent = all_send.at[0 if i <= SEQS_DEV else 1]
            to_tp(view, view, sent, all_recv.at[i, dx - 1], core).wait_recv()
            passed[dx].start()

    def all_end(buffer, i, at):
        wait_recv(all_copies(buffer, i, at, "take"))

    def to_pair(i, src, dst):
        return pltpu.make_async_remote_copy(
            src_ref=src,
            dst_ref=dst,
            send_sem=pair_send.at[0],
            recv_sem=pair_recv.at[i],
            device_id={"fs": pair},
            device_id_type=MESH,
        )

    halves = range(SEQS_DEV)
    mine, theirs = held_rows(MINE), held_rows(THEIRS)

    def tok_swap(o, h):
        view = tok.at[k, held_rows(o, h)]
        return to_pair(h, view, view)

    def res_swap(o, h):
        view = res.at[k, held_rows(o, h)]
        return to_pair(SEQS_DEV + h, view, view)

    def mix_swap(h):
        return to_pair(2 * SEQS_DEV + h, mix_z_sum.at[h], mix_z_got.at[h])

    def back(u):
        return to_pair(3 * SEQS_DEV + u, sum_z.at[u], got_z.at[u])

    barrier = pltpu.get_barrier_semaphore()
    for d in range(1, n_fs):
        to = lax.rem(j + d, n_fs)
        pl.semaphore_signal(barrier, inc=1, device_id={"fs": to}, device_id_type=MESH)
    pl.semaphore_signal(barrier, inc=1, device_id={"grp": 1 - g}, device_id_type=MESH)
    for d in range(1, n_tp):
        to = lax.rem(k + d, n_tp)
        pl.semaphore_signal(barrier, inc=1, device_id={"tp": to}, device_id_type=MESH)

    first = pltpu.make_async_copy(tokens, tok.at[k, mine], load_sem.at[4])
    own_rows = pl.ds(pl.multiple_of(j * shard, shard), shard)
    own_lanes = pl.ds(pl.multiple_of(j * LANES, LANES), LANES)
    inner_role = jnp.where(at_end, END, INNER)
    at_chans = pl.ds(pl.multiple_of(inner_role * unit_chans, unit_chans), unit_chans)

    def load(i, src, dst):
        pltpu.make_async_copy(src, dst, load_sem.at[i]).start()

    first.start()
    for i, ref in enumerate((w_signal, w_outer_gate, w_inner_gate)):
        load(0, ref.at[:, at_chans], mix_in.at[own_rows, pl.ds(i * unit_chans, unit_chans)])
    load(1, w_mix_out.at[at_chans, :], mix_out.at[j])
    def load_ffn(role):
        for t in range(tiles[role]):
            for i, src in enumerate((w_gate, w_value)):
                lanes = pl.ds((base[role] + t) * LANES, LANES)
                load(2, src.at[:, lanes], ffn_in.at[t, own_rows, pl.ds(i * LANES, LANES)])
        tall = tiles[role] * LANES
        for u in range(n_out):
            src = w_down.at[pl.ds(base[role] * LANES, tall), pl.ds(u * LANES, LANES)]
            load(3, src, ffn_out.at[u, pl.ds(0, tall), own_lanes])

    def wait_loads(role):
        views = [
            mix_in.at[own_rows, :],
            mix_out.at[j],
            ffn_in.at[pl.ds(0, tiles[role]), own_rows, :],
            ffn_out.at[:, pl.ds(0, tiles[role] * LANES), own_lanes],
        ]
        for i, view in enumerate(views):
            pltpu.make_async_copy(view, view, load_sem.at[i]).wait()

    with jax.named_scope("barrier"):
        first.wait()
        pl.semaphore_wait(barrier, n_fs - 1 + 1 + n_tp - 1)

    def begin(role):
        send(mix, role, (1, last) if role == END else (last, 1))
        tok_swap(MINE, 0).start()
        all_begin(tok, 0, mine)
        if role == INNER:
            send(mix, role, (2,))
        for h in halves[1:]:
            tok_swap(MINE, h).start()
        if role == END:
            for s in ins:
                send(s, role, (1,))
            for s in ins[:2]:
                send(s, role, (last,))
        load_ffn(role)

    by_role(begin)
    with jax.named_scope("loads"):
        by_role(wait_loads)

    def norm(buffer, at, gain):
        count = at.size
        squares = jnp.zeros((count, 1), jnp.float32)
        for b in range(n_tp):
            values = buffer[b, at, :].astype(jnp.float32)
            squares = squares + jnp.sum(values * values, axis=-1, keepdims=True)
        scale = lax.rsqrt(squares / (n_tp * own_cols) + 1e-06)
        for b in range(n_tp):
            cut = slice(b * own_cols, (b + 1) * own_cols)
            values = buffer[b, at, :].astype(jnp.float32)
            normed[at, cut] = (values * scale * gain[:, cut]).astype(jnp.bfloat16)

    with jax.named_scope("tok_mid"):
        all_middle(tok, 0, mine)
    def take_tok(h):
        with jax.named_scope("tok_swap"):
            tok_swap(THEIRS, h).wait_recv()
            all_begin(tok, 1 + h, held_rows(THEIRS, h))

    def pass_tok(h):
        with jax.named_scope("tok_theirs"):
            all_middle(tok, 1 + h, held_rows(THEIRS, h))

    def early(role):
        if role == END:
            with jax.named_scope("relay_mix"):
                relay(mix, role, 1)
            take_tok(0)
            with jax.named_scope("norm_mine"):
                all_end(tok, 0, mine)
                norm(tok, mine, mix_gain)
            with jax.named_scope("relay_mix"):
                relay(mix, role, 2)
            pass_tok(0)
            for h in halves[1:]:
                take_tok(h)
            with jax.named_scope("relay_mix"):
                relay(mix, role, last)
            for h in halves[1:]:
                pass_tok(h)
            return
        with jax.named_scope("relay_mix"):
            relay(mix, role, 1)
        with jax.named_scope("relay_mix"):
            ahead(mix)
        send(ins[0], role, (1, 2))
        take_tok(0)
        with jax.named_scope("norm_mine"):
            all_end(tok, 0, mine)
            norm(tok, mine, mix_gain)
        for h in halves[1:]:
            take_tok(h)
        pass_tok(0)
        with jax.named_scope("relay_mix"):
            relay(mix, role, 2)
        for s in ins[:3]:
            send(s, role, (last,))
        with jax.named_scope("ahead0"):
            ahead(ins[0])
            send(ins[1], role, (1, 2))
        for h in halves[1:]:
            pass_tok(h)

    by_role(early)
    with jax.named_scope("norm_theirs"):
        for h in halves:
            all_end(tok, 1 + h, held_rows(THEIRS, h))
        norm(tok, theirs, mix_gain)
    with jax.named_scope("arrived_mix"):
        arrived(mix, INNER)

    taps = [mix_taps[i : i + 1, at_chans] for i in range(3)]

    def mix_core_copy(o, dx):
        there = lax.rem(x + dx, n_x)
        return to_tp(
            part_mix.at[o, there * 2 + 1 - c],
            mix_core.at[o, there],
            mix_core_send.at[0],
            mix_core_recv.at[o, dx],
            core,
        )

    def mix_x_copy(o, h, dx):
        to = lax.rem(x + dx, n_x) * 2 + c
        return to_tp(
            mix_x_sum.at[o, h, dx - 1],
            mix_x_got.at[o, h, dx - 1],
            mix_x_send.at[0],
            mix_x_recv.at[o, h, dx - 1],
            to,
        )

    def mix_chip_sum(o, h, dx):
        there = lax.rem(x + dx, n_x)
        cut = in_half(h)
        near = part_mix[o, there * 2 + c, cut, :].astype(jnp.float32)
        return near + mix_core[o, there, cut, :].astype(jnp.float32)

    def mix_place_sum(o, h):
        value = mix_chip_sum(o, h, 0)
        for dx in range(1, n_x):
            value = value + mix_x_got[o, h, dx - 1].astype(jnp.float32)
        return value

    with jax.named_scope("mixer"):
        for o, at in ((THEIRS, theirs), (MINE, mine)):
            both = jnp.dot(normed[at, :], mix_in[...], preferred_element_type=jnp.float32)
            both = both.astype(jnp.bfloat16).astype(jnp.float32)
            gated = both[:, 2 * unit_chans :] * both[:, :unit_chans]
            conv = conv_rows(gated, taps, length)
            mixed = (both[:, unit_chans : 2 * unit_chans] * conv).astype(jnp.bfloat16)
            for b in range(n_fs):
                terms = jnp.dot(mixed, mix_out[b], preferred_element_type=jnp.float32)
                part_mix[o, b] = terms.astype(jnp.bfloat16)
            for dx in (*range(1, n_x), 0):
                mix_core_copy(o, dx).start()

    with jax.named_scope("mix_core"):
        for o in (THEIRS, MINE):
            for dx in range(1, n_x):
                mix_core_copy(o, dx).wait_recv()
                for h in halves:
                    mix_x_sum[o, h, dx - 1] = mix_chip_sum(o, h, dx).astype(jnp.bfloat16)
                    mix_x_copy(o, h, dx).start()
            mix_core_copy(o, 0).wait_recv()
    def between(role):
        if role == INNER:
            with jax.named_scope("ahead1"):
                for at in (1, 2):
                    ahead(ins[at])
                    send(ins[at + 1], role, (1, 2))
        with jax.named_scope("relay_in0"):
            relay_all(ins[0], role)

    by_role(between)

    with jax.named_scope("mix_x_theirs"):
        for h in halves:
            for dx in range(1, n_x):
                mix_x_copy(THEIRS, h, dx).wait_recv()
            mix_z_sum[h] = mix_place_sum(THEIRS, h).astype(jnp.bfloat16)
            mix_swap(h).start()

    def second(role):
        if role == END:
            send(ins[2], role, (last,))
            for s in outs[:2]:
                send(s, role, (1,))
        else:
            with jax.named_scope("ahead3"):
                for at in range(3, n_in):
                    ahead(ins[at])
                    if at + 1 < n_in:
                        send(ins[at + 1], role, (1, 2))
        with jax.named_scope("relay_in1"):
            relay_all(ins[1], role)

    by_role(second)
    with jax.named_scope("mix_mine"):
        for h in halves:
            for dx in range(1, n_x):
                mix_x_copy(MINE, h, dx).wait_recv()
            mix_swap(h).wait_recv()
            mixer = mix_place_sum(MINE, h) + mix_z_got[h].astype(jnp.float32)
            at = held_rows(MINE, h)
            res[k, at, :] = (tok[k, at, :].astype(jnp.float32) + mixer).astype(jnp.bfloat16)
            res_swap(MINE, h).start()
            all_begin(res, 1 + SEQS_DEV + h, at)

    def third(role):
        for s in outs[2:] if role == END else ():
            send(s, role, (1,))
        for s in ins[3:]:
            send(s, role, (last,))
        for s in outs:
            send(s, role, (2, last) if role == END else (1, 2, last))
        with jax.named_scope("relay_in2"):
            relay_all(ins[2], role)

    by_role(third)
    with jax.named_scope("res_mid"):
        for h in halves:
            all_middle(res, 1 + SEQS_DEV + h, held_rows(MINE, h))
    @pl.when(jnp.logical_not(at_end))
    def _():
        with jax.named_scope("relay_in3"):
            relay_all(ins[3], INNER)

    with jax.named_scope("res_swap"):
        for h in halves:
            res_swap(THEIRS, h).wait_recv()
            all_begin(res, 1 + 2 * SEQS_DEV + h, held_rows(THEIRS, h))
    @pl.when(at_end)
    def _():
        with jax.named_scope("relay_in3"):
            relay_all(ins[3], END)

    @pl.when(jnp.logical_not(at_end))
    def _():
        for s in outs[:2]:
            relay(s, INNER, last)

    with jax.named_scope("res_norm"):
        for h in halves:
            all_end(res, 1 + SEQS_DEV + h, held_rows(MINE, h))
            norm(res, held_rows(MINE, h), ffn_gain)
    with jax.named_scope("res_mid2"):
        for h in halves:
            all_middle(res, 1 + 2 * SEQS_DEV + h, held_rows(THEIRS, h))
    with jax.named_scope("res_norm2"):
        for h in halves:
            all_end(res, 1 + 2 * SEQS_DEV + h, held_rows(THEIRS, h))
            norm(res, held_rows(THEIRS, h), ffn_gain)

    first_tile = jnp.where(at_end, base[END], base[INNER])

    def feed(t):
        with jax.named_scope("in_wait"):
            arrived(("in", t), INNER)
        cut = pl.ds(pl.multiple_of((first_tile + t) * LANES, LANES), LANES)
        both = jnp.dot(normed[...], ffn_in[t], preferred_element_type=jnp.float32)
        both = both.astype(jnp.bfloat16).astype(jnp.float32)
        gate_taps, value_taps = ([up_taps[i, b : b + 1, cut] for i in range(3)] for b in (0, 1))
        gate = conv_rows(both[:, :LANES], gate_taps, length) + up_bias[0:1, cut]
        value = conv_rows(both[:, LANES:], value_taps, length) + up_bias[1:2, cut]
        unit = (gate / (1.0 + jnp.exp(-gate)) * value).astype(jnp.bfloat16)
        hidden[:, pl.ds(pl.multiple_of(t * LANES, LANES), LANES)] = unit

    beside = {
        (INNER, 1): (ins[4],),
        (INNER, 2): outs[2:],
        (INNER, 3): (ins[5],),
        (INNER, 5): (outs[0],),
        (END, 2): (outs[0],),
        (END, 3): (outs[1],),
    }

    @pl.loop(0, jnp.where(at_end, tiles[END], tiles[INNER]))
    def _(t):
        for (role, at), stages in beside.items():
            here = at_end if role == END else jnp.logical_not(at_end)

            @pl.when(here & (t == at))
            def _():
                with jax.named_scope("relay_beside"):
                    for stage in stages:
                        if len(stages) > 1:
                            relay(stage, role, last)
                        else:
                            relay_all(stage, role)

        feed(t)

    def core_copy(u, o, dx):
        there = lax.rem(x + dx, n_x)
        return to_tp(
            part_ffn.at[u, o, there * 2 + 1 - c],
            got_core.at[u, o, there],
            core_send.at[0],
            core_recv.at[u, o, dx],
            core,
        )

    def x_copy(u, o, dx):
        to = lax.rem(x + dx, n_x) * 2 + c
        sems = x_send.at[0], x_recv.at[u, o, dx - 1]
        return to_tp(sum_x.at[u, o, dx - 1], got_x.at[u, o, dx - 1], *sems, to)

    def chip_sum(u, o, dx):
        there = lax.rem(x + dx, n_x)
        mine_there = part_ffn[u, o, there * 2 + c].astype(jnp.float32)
        return mine_there + got_core[u, o, there].astype(jnp.float32)

    def place_sum(u, o):
        value = chip_sum(u, o, 0)
        for dx in range(1, n_x):
            value = value + got_x[u, o, dx - 1].astype(jnp.float32)
        return value

    def down(u, role):
        with jax.named_scope("out_wait"):
            arrived(("out", u), role)
        deep = pl.ds(0, tiles[role] * LANES)
        for o, at in ((THEIRS, theirs), (MINE, mine)):
            left, right = hidden[at, deep], ffn_out[u, deep, :]
            terms = jnp.dot(left, right, preferred_element_type=jnp.float32)
            for b in range(n_tp):
                part_ffn[u, o, b] = terms[:, b * LANES : (b + 1) * LANES].astype(jnp.bfloat16)
            for dx in (*range(1, n_x), 0):
                core_copy(u, o, dx).start()

    def over_x(u):
        for o in (THEIRS, MINE):
            for dx in range(1, n_x):
                core_copy(u, o, dx).wait_recv()
                sum_x[u, o, dx - 1] = chip_sum(u, o, dx).astype(jnp.bfloat16)
                x_copy(u, o, dx).start()

    def over_z(u):
        core_copy(u, THEIRS, 0).wait_recv()
        for dx in range(1, n_x):
            x_copy(u, THEIRS, dx).wait_recv()
        sum_z[u] = place_sum(u, THEIRS).astype(jnp.bfloat16)
        back(u).start()

    for u in range(n_out):
        def step(role):
            at = u + 1 + (role == END)
            if at < n_out:
                with jax.named_scope("relay_out"):
                    relay_all(outs[at], role)
            with jax.named_scope("down"):
                down(u, role)

        by_role(step)
        with jax.named_scope("over_x"):
            over_x(u)
        if u >= 1:
            with jax.named_scope("over_z"):
                over_z(u - 1)
    with jax.named_scope("over_z_last"):
        over_z(n_out - 1)
    with jax.named_scope("final"):
        for u in range(n_out):
            cut = slice(u * LANES, (u + 1) * LANES)
            core_copy(u, MINE, 0).wait_recv()
            for dx in range(1, n_x):
                x_copy(u, MINE, dx).wait_recv()
            value = res[k, mine, cut].astype(jnp.float32) + place_sum(u, MINE)
            back(u).wait_recv()
            out[:, cut] = (value + got_z[u].astype(jnp.float32)).astype(jnp.bfloat16)

    with jax.named_scope("drain"):
        def drain(role):
            for i, view in enumerate(all_sums(role, n_from)):
                to_y(view, view, y_send.at[i], y_recv.at[0]).wait_send()
            for d in range(1, n_fs):
                for i, view in enumerate(all_sums(role_of(role, d), 1)):
                    if (role, d) != (END, 2) or i == 3:
                        to_fs(view, view, z_send.at[i, d - 1], z_recv.at[0, 0], pair).wait_send()
            if role == INNER:
                for i, view in enumerate(all_sums(role, 1)[:3]):
                    to_fs(view, view, f_send.at[i], z_recv.at[0, 0], pair).wait_send()

        by_role(drain)
        for i, buffer in enumerate((tok, res)):
            view = buffer.at[pl.ds(0, n_tp - 1)]
            to_tp(view, view, all_send.at[i], all_recv.at[0, 0], core).wait_send()
        view = part_mix.at[:, pl.ds(0, n_x)]
        to_tp(view, view, mix_core_send.at[0], all_recv.at[0, 0], core).wait_send()
        to_tp(mix_x_sum, mix_x_sum, mix_x_send.at[0], all_recv.at[0, 0], core).wait_send()
        view = part_ffn.at[:, :, pl.ds(0, n_x)]
        to_tp(view, view, core_send.at[0], all_recv.at[0, 0], core).wait_send()
        to_tp(sum_x, sum_x, x_send.at[0], all_recv.at[0, 0], core).wait_send()
        view = tok.at[pl.ds(0, 2)]
        to_pair(0, view, view).wait_send()


def fused(n_fs, n_tp, *args):
    tokens, w_signal, w_gate = args[0], args[2], args[8]
    rows, cols = tokens.shape
    shard, chans = w_signal.shape
    n_in, n_out = tiles_of(w_gate.shape[1] // LANES, INNER), shard // LANES
    units = n_in * LANES
    width = n_fs * shard
    args = list(args)
    args[1], args[7] = args[1].reshape(1, -1), args[7].reshape(1, -1)
    args[10] = args[10].transpose(1, 0, 2)
    in_vmem = {1, 5, 7, 10, 11}
    n_x = n_tp // 2
    length = rows // SEQS_DEV
    dma = pltpu.SemaphoreType.DMA

    def held(*shape):
        return pltpu.VMEM(shape, jnp.bfloat16)

    return pl.pallas_call(
        functools.partial(layer_kernel, n_fs, n_tp),
        out_shape=jax.ShapeDtypeStruct((rows, cols), jnp.bfloat16),
        in_specs=[
            pl.BlockSpec(memory_space=pltpu.VMEM if i in in_vmem else pl.ANY)
            for i in range(len(args))
        ],
        out_specs=pl.BlockSpec(memory_space=pltpu.VMEM),
        scratch_shapes=[
            held(width, 3 * (chans // 2)),
            held(n_fs, chans // 2, shard),
            held(n_in, width, 2 * LANES),
            held(n_out, units, n_fs * LANES),
            held(n_tp, 2 * rows, cols),
            held(n_tp, 2 * rows, cols),
            held(2 * rows, width),
            held(2 * rows, units),
            held(2, n_tp, rows, cols),
            held(2, n_x, rows, cols),
            held(2, SEQS_DEV, n_x - 1, length, cols),
            held(2, SEQS_DEV, n_x - 1, length, cols),
            held(SEQS_DEV, length, cols),
            held(SEQS_DEV, length, cols),
            held(n_out, 2, n_tp, rows, LANES),
            held(n_out, 2, n_x, rows, LANES),
            held(n_out, 2, n_x - 1, rows, LANES),
            held(n_out, 2, n_x - 1, rows, LANES),
            held(n_out, rows, LANES),
            held(n_out, rows, LANES),
            dma((4, n_fs - 1)),
            dma((2 + n_in + n_out, n_fs)),
            dma((4,)),
            dma((4,)),
            dma((2 + n_in + n_out,)),
            dma((5,)),
            dma((2,)),
            dma((1 + 3 * SEQS_DEV, 2 * n_x - 1)),
            dma((1,)),
            dma((2, n_x)),
            dma((1,)),
            dma((2, SEQS_DEV, n_x - 1)),
            dma((1,)),
            dma((n_out, 2, n_x)),
            dma((1,)),
            dma((n_out, 2, n_x - 1)),
            dma((1,)),
            dma((3 * SEQS_DEV + n_out,)),
        ],
        compiler_params=pltpu.CompilerParams(
            collective_id=0, has_side_effects=True, vmem_limit_bytes=62 * 1024 * 1024
        ),
    )(*args)


def solution(mesh):
    n_fs, n_tp = mesh.shape["fs"], mesh.shape["tp"]
    body = functools.partial(fused, n_fs, n_tp)
    if n_fs != 4 or n_tp != 4 or mesh.shape["grp"] != 2:
        body = on_device
    placed = (
        P(("grp", "fs"), "tp"),
        P(),
        P("fs", "tp"),
        P("fs", "tp"),
        P("fs", "tp"),
        P(None, "tp"),
        P("tp", "fs"),
        P(),
        P("fs", "tp"),
        P("fs", "tp"),
        P(None, None, "tp"),
        P(None, "tp"),
        P("tp", "fs"),
    )
    return jax.shard_map(
        body, mesh=mesh, in_specs=placed, out_specs=P(("grp", "fs"), "tp"), check_vma=False
    )
```

```python
import functools

import jax
import jax.numpy as jnp
from jax import lax
from jax.experimental import pallas as pl
from jax.experimental.pallas import tpu as pltpu
from jax.sharding import PartitionSpec as P

SEQS_DEV = 2


def conv_positions(values, taps):
    width = values.shape[1]
    blocks = values.reshape(SEQS_DEV, -1, width)
    length = blocks.shape[1]
    padded = jnp.pad(blocks, ((0, 0), (2, 0), (0, 0)))
    result = (
        padded[:, 0:length] * taps[0]
        + padded[:, 1 : length + 1] * taps[1]
        + padded[:, 2 : length + 2] * taps[2]
    )
    return result.reshape(-1, width)


def rms_norm(stream, gain):
    values = stream.astype(jnp.float32)
    scale = lax.rsqrt(jnp.mean(values * values, axis=-1, keepdims=True) + 1e-06)
    return (values * scale * gain).astype(jnp.bfloat16)


def on_device(
    tokens,
    mix_gain,
    w_signal,
    w_outer_gate,
    w_inner_gate,
    mix_taps,
    w_mix_out,
    ffn_gain,
    w_gate,
    w_value,
    up_taps,
    up_bias,
    w_down,
):
    whole = lax.all_gather(tokens, "tp", axis=1, tiled=True)
    normed = rms_norm(whole, mix_gain)
    pieces = (
        lax.all_gather(w_signal, "fs", axis=0, tiled=True),
        lax.all_gather(w_outer_gate, "fs", axis=0, tiled=True),
        lax.all_gather(w_inner_gate, "fs", axis=0, tiled=True),
    )
    columns = normed
    signal, outer, inner = tuple(
        (jnp.dot(columns, piece, preferred_element_type=jnp.float32) for piece in pieces)
    )
    signal = signal.astype(jnp.bfloat16).astype(jnp.float32)
    outer = outer.astype(jnp.bfloat16).astype(jnp.float32)
    inner = inner.astype(jnp.bfloat16).astype(jnp.float32)
    mixed = (outer * conv_positions(inner * signal, mix_taps)).astype(jnp.bfloat16)
    mix_terms = jnp.dot(
        mixed,
        lax.all_gather(w_mix_out, "fs", axis=1, tiled=True),
        preferred_element_type=jnp.float32,
    )
    mix_sum = lax.psum_scatter(
        mix_terms.astype(jnp.bfloat16), "tp", scatter_dimension=1, tiled=True
    ).astype(jnp.float32)
    resid = (tokens.astype(jnp.float32) + mix_sum).astype(jnp.bfloat16)
    whole_ffn = lax.all_gather(resid, "tp", axis=1, tiled=True)
    normed_ffn = rms_norm(whole_ffn, ffn_gain)
    pieces = (
        lax.all_gather(w_gate, "fs", axis=0, tiled=True),
        lax.all_gather(w_value, "fs", axis=0, tiled=True),
    )
    columns = normed_ffn
    gate = jnp.dot(columns, pieces[0], preferred_element_type=jnp.float32)
    value = jnp.dot(columns, pieces[1], preferred_element_type=jnp.float32)
    gate = gate.astype(jnp.bfloat16).astype(jnp.float32)
    value = value.astype(jnp.bfloat16).astype(jnp.float32)
    gate_conv = conv_positions(gate, up_taps[0]) + up_bias[0]
    value_conv = conv_positions(value, up_taps[1]) + up_bias[1]
    hidden = (jax.nn.silu(gate_conv) * value_conv).astype(jnp.bfloat16)
    ffn_terms = jnp.dot(
        hidden, lax.all_gather(w_down, "fs", axis=1, tiled=True), preferred_element_type=jnp.float32
    )
    ffn_sum = lax.psum_scatter(
        ffn_terms.astype(jnp.bfloat16), "tp", scatter_dimension=1, tiled=True
    ).astype(jnp.float32)
    return (resid.astype(jnp.float32) + ffn_sum).astype(jnp.bfloat16)


MESH = pl.DeviceIdType.MESH
UP, DOWN = 0, 1
LANES = 128


def shifted(values, by, length):
    rolled = pltpu.roll(values, by, 0)
    position = lax.rem(lax.broadcasted_iota(jnp.int32, values.shape, 0), length)
    return jnp.where(position < by, 0.0, rolled)


def conv_rows(values, taps, length):
    return (
        shifted(values, 2, length) * taps[0]
        + shifted(values, 1, length) * taps[1]
        + values * taps[2]
    )


END, INNER = 0, 1


def tiles_of(n_tiles, role):
    at_end = 2 * n_tiles // 5
    return at_end if role == END else n_tiles - at_end


def layer_kernel(
    n_fs,
    n_tp,
    tokens,
    mix_gain,
    w_signal,
    w_outer_gate,
    w_inner_gate,
    mix_taps,
    w_mix_out,
    ffn_gain,
    w_gate,
    w_value,
    up_taps,
    up_bias,
    w_down,
    out,
    mix_in,
    mix_out,
    ffn_in,
    ffn_out,
    tok,
    res,
    normed,
    hidden,
    part_mix,
    mix_core,
    mix_x_sum,
    mix_x_got,
    mix_z_sum,
    mix_z_got,
    part_ffn,
    got_core,
    sum_x,
    got_x,
    sum_z,
    got_z,
    done,
    z_send,
    z_recv,
    f_send,
    y_send,
    y_recv,
    load_sem,
    all_send,
    all_recv,
    mix_core_send,
    mix_core_recv,
    mix_x_send,
    mix_x_recv,
    core_send,
    core_recv,
    x_send,
    x_recv,
    pair_send,
    pair_recv,
):
    g, j, k = lax.axis_index("grp"), lax.axis_index("fs"), lax.axis_index("tp")
    rows, own_cols = tokens.shape
    length = rows // SEQS_DEV
    shard, chans = w_signal.shape
    half, unit_chans = shard // 2, chans // 2
    n_tiles, n_out = w_gate.shape[1] // LANES, shard // LANES
    tiles = {END: tiles_of(n_tiles, END), INNER: tiles_of(n_tiles, INNER)}
    base = {END: 0, INNER: tiles[END]}
    n_x = n_tp // 2
    x, c = k // 2, lax.rem(k, 2)
    core = k + 1 - 2 * c
    p = lax.rem(j, 2)
    pair = j + 1 - 2 * p
    inward = jnp.where(j < n_fs // 2, 1, n_fs - 1)
    at_end = (j == 0) | (j == n_fs - 1)

    MINE, THEIRS = 0, 1

    def held_rows(o, h=None):
        side = p if o == MINE else 1 - p
        if h is None:
            return pl.ds(pl.multiple_of(side * rows, rows), rows)
        return pl.ds(pl.multiple_of(side * rows + h * length, length), length)

    def in_half(h):
        return slice(h * length, (h + 1) * length)

    mix = ("mix", 0)
    n_in = tiles[INNER]
    ins = [("in", t) for t in range(n_in)]
    outs = [("out", u) for u in range(n_out)]

    def by_role(body):
        pl.when(at_end)(functools.partial(body, END))
        pl.when(jnp.logical_not(at_end))(functools.partial(body, INNER))


    def other(d):
        return lax.rem(j + inward * d, n_fs)

    def sources(stage, role, side):
        kind, i = stage
        at_rows = pl.ds(pl.multiple_of(side * half, half), half)
        if kind == "mix":
            lanes = pl.ds(role * unit_chans, unit_chans)
            tall = unit_chans // 2
            at = pl.ds(pl.multiple_of(role * unit_chans + side * tall, tall), tall)
            refs = [ref.at[at_rows, lanes] for ref in (w_signal, w_outer_gate, w_inner_gate)]
            return [*refs, w_mix_out.at[at, :]]
        if kind == "in":
            lanes = pl.ds((base[role] + i) * LANES, LANES)
            return [w_gate.at[at_rows, lanes], w_value.at[at_rows, lanes]]
        tall = tiles[role] * LANES // 2
        at = pl.ds(pl.multiple_of(base[role] * LANES + side * tall, LANES), tall)
        return [w_down.at[at, pl.ds(i * LANES, LANES)]]

    def places(stage, role, source, side, whole):
        kind, i = stage
        at_rows = pl.ds(pl.multiple_of((source * 2 + side) * half, half), half)
        if kind == "mix":
            tall = unit_chans // 2
            at = pl.ds(pl.multiple_of(side * tall, tall), tall)
            outs = mix_out.at[source, at, :]
            if whole:
                return [mix_in.at[at_rows, :], outs]
            lanes = [pl.ds(b * unit_chans, unit_chans) for b in range(3)]
            return [*(mix_in.at[at_rows, lane] for lane in lanes), outs]
        if kind == "in":
            if whole:
                return [ffn_in.at[i, at_rows, :]]
            return [ffn_in.at[i, at_rows, pl.ds(b * LANES, LANES)] for b in (0, 1)]
        tall = tiles[role] * LANES // 2
        at = pl.ds(pl.multiple_of(side * tall, LANES), tall)
        lanes = pl.ds(pl.multiple_of(source * LANES, LANES), LANES)
        return [ffn_out.at[i, at, lanes]]

    def slot(stage, i):
        kind, at = stage
        if kind == "mix":
            return i
        return 2 + at if kind == "in" else 2 + n_in + at

    def group(stage, i):
        kind, _ = stage
        return i if kind == "mix" else {"in": 2, "out": 3}[kind]

    def to_fs(src, dst, send_sem, recv_sem, to):
        return pltpu.make_async_remote_copy(
            src_ref=src,
            dst_ref=dst,
            send_sem=send_sem,
            recv_sem=recv_sem,
            device_id={"fs": to},
            device_id_type=MESH,
        )

    def role_of(role, d):
        return INNER if d < n_fs - 1 - role else END

    def z_sends(s, role, d):
        to = other(d)
        there = role_of(role, d)
        pairs = zip(sources(s, there, g), places(s, there, j, g, False))
        copies = []
        for i, (src, dst) in enumerate(pairs):
            wide = i // 3 if s[0] == "mix" else 0
            sems = z_send.at[group(s, wide), d - 1], z_recv.at[slot(s, wide), j]
            copies.append(to_fs(src, dst, *sems, to))
        return copies

    def z_takes(s, role, d):
        source = other(d)
        return [
            to_fs(view, view, z_send.at[group(s, i), 0], z_recv.at[slot(s, i), source], source)
            for i, view in enumerate(places(s, role, source, g, True))
        ]

    def z_forwards(s):
        source = other(last)
        return [
            to_fs(view, view, f_send.at[group(s, i)], z_recv.at[slot(s, i), source], other(1))
            for i, view in enumerate(places(s, INNER, source, g, True))
        ]

    def to_y(src, dst, send_sem, recv_sem):
        return pltpu.make_async_remote_copy(
            src_ref=src,
            dst_ref=dst,
            send_sem=send_sem,
            recv_sem=recv_sem,
            device_id={"grp": 1 - g},
            device_id_type=MESH,
        )

    def y_copies(s, role, d):
        return [
            to_y(view, view, y_send.at[group(s, i)], y_recv.at[slot(s, i)])
            for i, view in enumerate(places(s, role, other(d), g, True))
        ]

    n_from = n_fs - 1

    def sums(stage, role, count):
        kind, i = stage
        if kind == "mix":
            some = mix_out.at[pl.ds(0, count), pl.ds(0, unit_chans // 2), :]
            return [mix_in.at[pl.ds(0, count * half), :], some]
        if kind == "in":
            return [ffn_in.at[i, pl.ds(0, count * half), :]]
        return [ffn_out.at[i, pl.ds(0, tiles[role] * LANES // 2), pl.ds(0, count * LANES)]]

    def all_sums(role, count):
        return [
            *sums(mix, role, count),
            *sums(("in", pl.ds(0, tiles[role])), role, count),
            *sums(("out", pl.ds(0, n_out)), role, count),
        ]

    def start(copies):
        for copy in copies:
            copy.start()

    def wait_recv(copies):
        for copy in copies:
            copy.wait_recv()

    def wait_send(copies):
        for copy in copies:
            copy.wait_send()

    def send(s, role, ds):
        for d in ds:
            if s[0] != "in" or s[1] < tiles[role_of(role, d)]:
                start(z_sends(s, role, d))

    last = n_fs - 1

    def relay(s, role, d):
        wait_recv(z_takes(s, role, d))
        start(y_copies(s, role, d))

    def ahead(s):
        relay(s, INNER, last)
        start(z_forwards(s))

    def relay_all(s, role):
        if s[0] == "in" and s[1] >= tiles[role]:
            return
        for d in (1, 2, last) if role == END else (1, 2):
            relay(s, role, d)

    def relay_both(s):
        by_role(lambda role: relay_all(s, role))

    def arrived(s, role):
        for i, view in enumerate(sums(s, role, n_from)):
            to_y(view, view, y_send.at[group(s, i)], y_recv.at[slot(s, i)]).wait_recv()

    def to_tp(src, dst, send_sem, recv_sem, to):
        return pltpu.make_async_remote_copy(
            src_ref=src,
            dst_ref=dst,
            send_sem=send_sem,
            recv_sem=recv_sem,
            device_id={"tp": to},
            device_id_type=MESH,
        )

    def all_copies(buffer, i, at, kind):
        sent = all_send.at[0 if i <= SEQS_DEV else 1]
        copies = []
        for dx in range(n_x):
            there = lax.rem(x + dx, n_x)
            if kind == "over":
                if dx:
                    view = buffer.at[k, at]
                    copies.append(to_tp(view, view, sent, all_recv.at[i, dx - 1], there * 2 + c))
            else:
                back = lax.rem(x + n_x - dx, n_x) * 2
                seen = back + c if kind == "pass" else back + 1 - c
                view = buffer.at[seen, at]
                copies.append(to_tp(view, view, sent, all_recv.at[i, n_x - 1 + dx], core))
        return copies

    def all_begin(buffer, i, at):
        start(all_copies(buffer, i, at, "over"))
        all_copies(buffer, i, at, "pass")[0].start()

    def all_middle(buffer, i, at):
        passed = all_copies(buffer, i, at, "pass")
        for dx in range(1, n_x):
            view = buffer.at[lax.rem(x + n_x - dx, n_x) * 2 + c, at]
            sent = all_send.at[0 if i <= SEQS_DEV else 1]
            to_tp(view, view, sent, all_recv.at[i, dx - 1], core).wait_recv()
            passed[dx].start()

    def all_end(buffer, i, at):
        wait_recv(all_copies(buffer, i, at, "take"))

    def to_pair(i, src, dst):
        return pltpu.make_async_remote_copy(
            src_ref=src,
            dst_ref=dst,
            send_sem=pair_send.at[0],
            recv_sem=pair_recv.at[i],
            device_id={"fs": pair},
            device_id_type=MESH,
        )

    halves = range(SEQS_DEV)
    mine, theirs = held_rows(MINE), held_rows(THEIRS)

    def tok_swap(o, h):
        view = tok.at[k, held_rows(o, h)]
        return to_pair(h, view, view)

    def res_swap(o, h):
        view = res.at[k, held_rows(o, h)]
        return to_pair(SEQS_DEV + h, view, view)

    def mix_swap(h):
        return to_pair(2 * SEQS_DEV + h, mix_z_sum.at[h], mix_z_got.at[h])

    def back(u):
        return to_pair(3 * SEQS_DEV + u, sum_z.at[u], got_z.at[u])

    barrier = pltpu.get_barrier_semaphore()
    for d in range(1, n_fs):
        to = lax.rem(j + d, n_fs)
        pl.semaphore_signal(barrier, inc=1, device_id={"fs": to}, device_id_type=MESH)
    pl.semaphore_signal(barrier, inc=1, device_id={"grp": 1 - g}, device_id_type=MESH)
    for d in range(1, n_tp):
        to = lax.rem(k + d, n_tp)
        pl.semaphore_signal(barrier, inc=1, device_id={"tp": to}, device_id_type=MESH)
    for dx in range(1, n_x):
        far = {"tp": lax.rem(x + dx, n_x) * 2 + c, "fs": pair}
        pl.semaphore_signal(barrier, inc=1, device_id=far, device_id_type=MESH)

    first = pltpu.make_async_copy(tokens, tok.at[k, mine], load_sem.at[4])
    own_rows = pl.ds(pl.multiple_of(j * shard, shard), shard)
    own_lanes = pl.ds(pl.multiple_of(j * LANES, LANES), LANES)
    inner_role = jnp.where(at_end, END, INNER)
    at_chans = pl.ds(pl.multiple_of(inner_role * unit_chans, unit_chans), unit_chans)

    def load(i, src, dst):
        pltpu.make_async_copy(src, dst, load_sem.at[i]).start()

    first.start()
    for i, ref in enumerate((w_signal, w_outer_gate, w_inner_gate)):
        load(0, ref.at[:, at_chans], mix_in.at[own_rows, pl.ds(i * unit_chans, unit_chans)])
    load(1, w_mix_out.at[at_chans, :], mix_out.at[j])
    def load_ffn(role):
        for t in range(tiles[role]):
            for i, src in enumerate((w_gate, w_value)):
                lanes = pl.ds((base[role] + t) * LANES, LANES)
                load(2, src.at[:, lanes], ffn_in.at[t, own_rows, pl.ds(i * LANES, LANES)])
        tall = tiles[role] * LANES
        for u in range(n_out):
            src = w_down.at[pl.ds(base[role] * LANES, tall), pl.ds(u * LANES, LANES)]
            load(3, src, ffn_out.at[u, pl.ds(0, tall), own_lanes])

    def wait_loads(role):
        views = [
            mix_in.at[own_rows, :],
            mix_out.at[j],
            ffn_in.at[pl.ds(0, tiles[role]), own_rows, :],
            ffn_out.at[:, pl.ds(0, tiles[role] * LANES), own_lanes],
        ]
        for i, view in enumerate(views):
            pltpu.make_async_copy(view, view, load_sem.at[i]).wait()

    with jax.named_scope("barrier"):
        first.wait()
        pl.semaphore_wait(barrier, n_fs - 1 + 1 + n_tp - 1 + n_x - 1)

    def begin(role):
        send(mix, role, (1, last) if role == END else (last, 1))
        tok_swap(MINE, 0).start()
        all_begin(tok, 0, mine)
        if role == INNER:
            send(mix, role, (2,))
        for h in halves[1:]:
            tok_swap(MINE, h).start()
        if role == END:
            for s in ins:
                send(s, role, (1,))
            for s in ins[:2]:
                send(s, role, (last,))
        load_ffn(role)

    by_role(begin)
    with jax.named_scope("loads"):
        by_role(wait_loads)

    def norm(buffer, at, gain):
        count = at.size
        squares = jnp.zeros((count, 1), jnp.float32)
        for b in range(n_tp):
            values = buffer[b, at, :].astype(jnp.float32)
            squares = squares + jnp.sum(values * values, axis=-1, keepdims=True)
        scale = lax.rsqrt(squares / (n_tp * own_cols) + 1e-06)
        for b in range(n_tp):
            cut = slice(b * own_cols, (b + 1) * own_cols)
            values = buffer[b, at, :].astype(jnp.float32)
            normed[at, cut] = (values * scale * gain[:, cut]).astype(jnp.bfloat16)

    with jax.named_scope("tok_mid"):
        all_middle(tok, 0, mine)
    def take_tok(h):
        with jax.named_scope("tok_swap"):
            tok_swap(THEIRS, h).wait_recv()
            all_begin(tok, 1 + h, held_rows(THEIRS, h))

    def pass_tok(h):
        with jax.named_scope("tok_theirs"):
            all_middle(tok, 1 + h, held_rows(THEIRS, h))

    def early(role):
        if role == END:
            with jax.named_scope("relay_mix"):
                relay(mix, role, 1)
            take_tok(0)
            with jax.named_scope("norm_mine"):
                all_end(tok, 0, mine)
                norm(tok, mine, mix_gain)
            with jax.named_scope("relay_mix"):
                relay(mix, role, 2)
            pass_tok(0)
            for h in halves[1:]:
                take_tok(h)
            with jax.named_scope("relay_mix"):
                relay(mix, role, last)
            for h in halves[1:]:
                pass_tok(h)
            return
        with jax.named_scope("relay_mix"):
            relay(mix, role, 1)
        with jax.named_scope("relay_mix"):
            ahead(mix)
        send(ins[0], role, (1, 2))
        take_tok(0)
        with jax.named_scope("norm_mine"):
            all_end(tok, 0, mine)
            norm(tok, mine, mix_gain)
        for h in halves[1:]:
            take_tok(h)
        pass_tok(0)
        with jax.named_scope("relay_mix"):
            relay(mix, role, 2)
        for s in ins[:3]:
            send(s, role, (last,))
        with jax.named_scope("ahead0"):
            ahead(ins[0])
            send(ins[1], role, (1, 2))
        for h in halves[1:]:
            pass_tok(h)

    by_role(early)
    with jax.named_scope("norm_theirs"):
        for h in halves:
            all_end(tok, 1 + h, held_rows(THEIRS, h))
        norm(tok, theirs, mix_gain)
    with jax.named_scope("arrived_mix"):
        arrived(mix, INNER)

    taps = [mix_taps[i : i + 1, at_chans] for i in range(3)]

    def mix_core_copy(o, dx):
        there = lax.rem(x + dx, n_x)
        return to_tp(
            part_mix.at[o, there * 2 + 1 - c],
            mix_core.at[o, there],
            mix_core_send.at[0],
            mix_core_recv.at[o, dx],
            core,
        )

    def mix_x_copy(o, h, dx):
        to = lax.rem(x + dx, n_x) * 2 + c
        return to_tp(
            mix_x_sum.at[o, h, dx - 1],
            mix_x_got.at[o, h, dx - 1],
            mix_x_send.at[0],
            mix_x_recv.at[o, h, dx - 1],
            to,
        )

    def mix_chip_sum(o, h, dx):
        there = lax.rem(x + dx, n_x)
        cut = in_half(h)
        near = part_mix[o, there * 2 + c, cut, :].astype(jnp.float32)
        return near + mix_core[o, there, cut, :].astype(jnp.float32)

    def mix_place_sum(o, h):
        value = mix_chip_sum(o, h, 0)
        for dx in range(1, n_x):
            value = value + mix_x_got[o, h, dx - 1].astype(jnp.float32)
        return value

    with jax.named_scope("mixer"):
        for o, at in ((THEIRS, theirs), (MINE, mine)):
            both = jnp.dot(normed[at, :], mix_in[...], preferred_element_type=jnp.float32)
            both = both.astype(jnp.bfloat16).astype(jnp.float32)
            gated = both[:, 2 * unit_chans :] * both[:, :unit_chans]
            conv = conv_rows(gated, taps, length)
            mixed = (both[:, unit_chans : 2 * unit_chans] * conv).astype(jnp.bfloat16)
            for b in range(n_fs):
                terms = jnp.dot(mixed, mix_out[b], preferred_element_type=jnp.float32)
                part_mix[o, b] = terms.astype(jnp.bfloat16)
            for dx in (*range(1, n_x), 0):
                mix_core_copy(o, dx).start()

    with jax.named_scope("mix_core"):
        for o in (THEIRS, MINE):
            for dx in range(1, n_x):
                mix_core_copy(o, dx).wait_recv()
                for h in halves:
                    mix_x_sum[o, h, dx - 1] = mix_chip_sum(o, h, dx).astype(jnp.bfloat16)
                    mix_x_copy(o, h, dx).start()
            mix_core_copy(o, 0).wait_recv()
    def between(role):
        if role == INNER:
            with jax.named_scope("ahead1"):
                for at in (1, 2):
                    ahead(ins[at])
                    send(ins[at + 1], role, (1, 2))
        with jax.named_scope("relay_in0"):
            relay_all(ins[0], role)

    by_role(between)

    with jax.named_scope("mix_x_theirs"):
        for h in halves:
            for dx in range(1, n_x):
                mix_x_copy(THEIRS, h, dx).wait_recv()
            mix_z_sum[h] = mix_place_sum(THEIRS, h).astype(jnp.bfloat16)
            mix_swap(h).start()

    def second(role):
        if role == END:
            send(ins[2], role, (last,))
            for s in outs[:2]:
                send(s, role, (1,))
        else:
            with jax.named_scope("ahead3"):
                for at in range(3, n_in):
                    ahead(ins[at])
                    if at + 1 < n_in:
                        send(ins[at + 1], role, (1, 2))
        with jax.named_scope("relay_in1"):
            relay_all(ins[1], role)

    by_role(second)
    with jax.named_scope("mix_mine"):
        for h in halves:
            for dx in range(1, n_x):
                mix_x_copy(MINE, h, dx).wait_recv()
            mix_swap(h).wait_recv()
            mixer = mix_place_sum(MINE, h) + mix_z_got[h].astype(jnp.float32)
            at = held_rows(MINE, h)
            res[k, at, :] = (tok[k, at, :].astype(jnp.float32) + mixer).astype(jnp.bfloat16)
            res_swap(MINE, h).start()
            all_begin(res, 1 + SEQS_DEV + h, at)

    def third(role):
        for s in ins[3:]:
            send(s, role, (last,))
        for s in outs[2:] if role == END else ():
            send(s, role, (1,))
        for s in outs if role == INNER else ():
            send(s, role, (1, 2, last))
        with jax.named_scope("relay_in2"):
            relay_all(ins[2], role)

    by_role(third)
    with jax.named_scope("res_mid"):
        for h in halves:
            all_middle(res, 1 + SEQS_DEV + h, held_rows(MINE, h))
    @pl.when(jnp.logical_not(at_end))
    def _():
        with jax.named_scope("relay_in3"):
            relay_all(ins[3], INNER)

    with jax.named_scope("res_swap"):
        for h in halves:
            res_swap(THEIRS, h).wait_recv()
            all_begin(res, 1 + 2 * SEQS_DEV + h, held_rows(THEIRS, h))
    @pl.when(at_end)
    def _():
        with jax.named_scope("relay_in3"):
            relay_all(ins[3], END)

    @pl.when(jnp.logical_not(at_end))
    def _():
        for s in outs[:2]:
            relay(s, INNER, last)

    with jax.named_scope("res_norm"):
        for h in halves:
            all_end(res, 1 + SEQS_DEV + h, held_rows(MINE, h))
            norm(res, held_rows(MINE, h), ffn_gain)
    def fourth(role):
        if role == INNER:
            with jax.named_scope("relay_in4"):
                relay_all(ins[4], INNER)

    by_role(fourth)
    with jax.named_scope("res_mid2"):
        for h in halves:
            all_middle(res, 1 + 2 * SEQS_DEV + h, held_rows(THEIRS, h))
    with jax.named_scope("res_norm2"):
        for h in halves:
            all_end(res, 1 + 2 * SEQS_DEV + h, held_rows(THEIRS, h))
            norm(res, held_rows(THEIRS, h), ffn_gain)

    first_tile = jnp.where(at_end, base[END], base[INNER])

    def feed(t):
        with jax.named_scope("in_wait"):
            arrived(("in", t), INNER)
        cut = pl.ds(pl.multiple_of((first_tile + t) * LANES, LANES), LANES)
        both = jnp.dot(normed[...], ffn_in[t], preferred_element_type=jnp.float32)
        both = both.astype(jnp.bfloat16).astype(jnp.float32)
        gate_taps, value_taps = ([up_taps[i, b : b + 1, cut] for i in range(3)] for b in (0, 1))
        gate = conv_rows(both[:, :LANES], gate_taps, length) + up_bias[0:1, cut]
        value = conv_rows(both[:, LANES:], value_taps, length) + up_bias[1:2, cut]
        unit = (gate / (1.0 + jnp.exp(-gate)) * value).astype(jnp.bfloat16)
        hidden[:, pl.ds(pl.multiple_of(t * LANES, LANES), LANES)] = unit

    paced = {0: outs[:1], 2: outs[1:2], 3: outs[2:3]}
    beside = {
        (INNER, 2): [(ins[5], 1), (ins[5], 2)],
        (INNER, 3): [(outs[2], last), (outs[3], last)],
        (INNER, 4): [(outs[0], 2), (outs[0], 1)],
        (END, 1): [(stage, 1) for stage in outs],
        (END, 3): [(outs[0], last), (outs[0], 2)],
    }
    after = {
        (INNER, 0): [(outs[1], 2), (outs[1], 1)],
        (INNER, 1): [(outs[2], 2), (outs[2], 1)],
        (INNER, 2): [(outs[3], 2), (outs[3], 1)],
        (END, 0): [(outs[1], last), (outs[1], 2)],
        (END, 1): [(outs[2], last), (outs[2], 2)],
        (END, 2): [(outs[3], last), (outs[3], 2)],
    }

    @pl.loop(0, jnp.where(at_end, tiles[END], tiles[INNER]))
    def _(t):
        for at, stages in paced.items():

            @pl.when(at_end & (t == at))
            def _():
                for stage in stages:
                    send(stage, END, (2, last))

        for (role, at), relays in beside.items():
            here = at_end if role == END else jnp.logical_not(at_end)

            @pl.when(here & (t == at))
            def _():
                for stage, d in relays:
                    with jax.named_scope("relay_beside"):
                        relay(stage, role, d)

        feed(t)

    @pl.when(at_end)
    def _():
        for stage in outs[3:]:
            send(stage, END, (2, last))

    def core_copy(u, o, dx):
        there = lax.rem(x + dx, n_x)
        return to_tp(
            part_ffn.at[u, o, there * 2 + 1 - c],
            got_core.at[u, o, there],
            core_send.at[0],
            core_recv.at[u, o, dx],
            core,
        )

    def x_copy(u, o, dx):
        to = lax.rem(x + dx, n_x) * 2 + c
        straight = u == n_out - 1 and o == THEIRS
        return pltpu.make_async_remote_copy(
            src_ref=sum_x.at[u, o, dx - 1],
            dst_ref=got_x.at[u, o, dx - 1],
            send_sem=x_send.at[0],
            recv_sem=x_recv.at[u, o, dx - 1],
            device_id={"tp": to, "fs": pair} if straight else {"tp": to},
            device_id_type=MESH,
        )

    def chip_sum(u, o, dx):
        there = lax.rem(x + dx, n_x)
        mine_there = part_ffn[u, o, there * 2 + c].astype(jnp.float32)
        return mine_there + got_core[u, o, there].astype(jnp.float32)

    def place_sum(u, o):
        value = chip_sum(u, o, 0)
        for dx in range(1, n_x):
            value = value + got_x[u, o, dx - 1].astype(jnp.float32)
        return value

    def down(u, role):
        with jax.named_scope("out_wait"):
            arrived(("out", u), role)
        deep = pl.ds(0, tiles[role] * LANES)
        for o, at in ((THEIRS, theirs), (MINE, mine)):
            left, right = hidden[at, deep], ffn_out[u, deep, :]
            terms = jnp.dot(left, right, preferred_element_type=jnp.float32)
            for b in range(n_tp):
                part_ffn[u, o, b] = terms[:, b * LANES : (b + 1) * LANES].astype(jnp.bfloat16)
            for dx in (*range(1, n_x), 0):
                core_copy(u, o, dx).start()

    def over_x(u):
        for o in (THEIRS, MINE):
            for dx in range(1, n_x):
                core_copy(u, o, dx).wait_recv()
                sum_x[u, o, dx - 1] = chip_sum(u, o, dx).astype(jnp.bfloat16)
                x_copy(u, o, dx).start()

    def over_z(u):
        core_copy(u, THEIRS, 0).wait_recv()
        if u == n_out - 1:
            value = chip_sum(u, THEIRS, 0)
        else:
            for dx in range(1, n_x):
                x_copy(u, THEIRS, dx).wait_recv()
            value = place_sum(u, THEIRS)
        sum_z[u] = value.astype(jnp.bfloat16)
        back(u).start()

    for u in range(n_out):
        if u >= 2:
            with jax.named_scope("over_z"):
                over_z(u - 2)

        def step(role):
            for stage, d in after.get((role, u), ()):
                with jax.named_scope("relay_out"):
                    relay(stage, role, d)
            with jax.named_scope("down"):
                down(u, role)

        by_role(step)
        with jax.named_scope("over_x"):
            over_x(u)
    for u in (n_out - 1, *range(max(n_out - 2, 0), n_out - 1)):
        with jax.named_scope("over_z_last"):
            over_z(u)
    def result(u):
        cut = pl.ds(u * LANES, LANES)
        return pltpu.make_async_copy(done.at[u], out.at[:, cut], load_sem.at[u])

    with jax.named_scope("final"):
        for u in range(n_out):
            cut = slice(u * LANES, (u + 1) * LANES)
            core_copy(u, MINE, 0).wait_recv()
            for dx in range(1, n_x):
                x_copy(u, MINE, dx).wait_recv()
            value = res[k, mine, cut].astype(jnp.float32) + place_sum(u, MINE)
            back(u).wait_recv()
            value = value + got_z[u].astype(jnp.float32)
            for dx in range(1, n_x) if u == n_out - 1 else ():
                x_copy(u, THEIRS, dx).wait_recv()
                value = value + got_x[u, THEIRS, dx - 1].astype(jnp.float32)
            done[u] = value.astype(jnp.bfloat16)
            result(u).start()

    with jax.named_scope("drain"):
        for u in range(n_out):
            result(u).wait()
        def drain(role):
            for i, view in enumerate(all_sums(role, n_from)):
                to_y(view, view, y_send.at[i], y_recv.at[0]).wait_send()
            for d in range(1, n_fs):
                for i, view in enumerate(all_sums(role_of(role, d), 1)):
                    if (role, d) != (END, 2) or i == 3:
                        to_fs(view, view, z_send.at[i, d - 1], z_recv.at[0, 0], pair).wait_send()
            if role == INNER:
                for i, view in enumerate(all_sums(role, 1)[:3]):
                    to_fs(view, view, f_send.at[i], z_recv.at[0, 0], pair).wait_send()

        by_role(drain)
        for i, buffer in enumerate((tok, res)):
            view = buffer.at[pl.ds(0, n_tp - 1)]
            to_tp(view, view, all_send.at[i], all_recv.at[0, 0], core).wait_send()
        view = part_mix.at[:, pl.ds(0, n_x)]
        to_tp(view, view, mix_core_send.at[0], all_recv.at[0, 0], core).wait_send()
        to_tp(mix_x_sum, mix_x_sum, mix_x_send.at[0], all_recv.at[0, 0], core).wait_send()
        view = part_ffn.at[:, :, pl.ds(0, n_x)]
        to_tp(view, view, core_send.at[0], all_recv.at[0, 0], core).wait_send()
        to_tp(sum_x, sum_x, x_send.at[0], all_recv.at[0, 0], core).wait_send()
        view = tok.at[pl.ds(0, 2)]
        to_pair(0, view, view).wait_send()


def fused(n_fs, n_tp, *args):
    tokens, w_signal, w_gate = args[0], args[2], args[8]
    rows, cols = tokens.shape
    shard, chans = w_signal.shape
    n_in, n_out = tiles_of(w_gate.shape[1] // LANES, INNER), shard // LANES
    units = n_in * LANES
    width = n_fs * shard
    args = list(args)
    args[1], args[7] = args[1].reshape(1, -1), args[7].reshape(1, -1)
    args[10] = args[10].transpose(1, 0, 2)
    in_vmem = {1, 5, 7, 10, 11}
    n_x = n_tp // 2
    length = rows // SEQS_DEV
    dma = pltpu.SemaphoreType.DMA

    def held(*shape):
        return pltpu.VMEM(shape, jnp.bfloat16)

    return pl.pallas_call(
        functools.partial(layer_kernel, n_fs, n_tp),
        out_shape=jax.ShapeDtypeStruct((rows, cols), jnp.bfloat16),
        in_specs=[
            pl.BlockSpec(memory_space=pltpu.VMEM if i in in_vmem else pl.ANY)
            for i in range(len(args))
        ],
        out_specs=pl.BlockSpec(memory_space=pl.ANY),
        scratch_shapes=[
            held(width, 3 * (chans // 2)),
            held(n_fs, chans // 2, shard),
            held(n_in, width, 2 * LANES),
            held(n_out, units, n_fs * LANES),
            held(n_tp, 2 * rows, cols),
            held(n_tp, 2 * rows, cols),
            held(2 * rows, width),
            held(2 * rows, units),
            held(2, n_tp, rows, cols),
            held(2, n_x, rows, cols),
            held(2, SEQS_DEV, n_x - 1, length, cols),
            held(2, SEQS_DEV, n_x - 1, length, cols),
            held(SEQS_DEV, length, cols),
            held(SEQS_DEV, length, cols),
            held(n_out, 2, n_tp, rows, LANES),
            held(n_out, 2, n_x, rows, LANES),
            held(n_out, 2, n_x - 1, rows, LANES),
            held(n_out, 2, n_x - 1, rows, LANES),
            held(n_out, rows, LANES),
            held(n_out, rows, LANES),
            held(n_out, rows, LANES),
            dma((4, n_fs - 1)),
            dma((2 + n_in + n_out, n_fs)),
            dma((4,)),
            dma((4,)),
            dma((2 + n_in + n_out,)),
            dma((5,)),
            dma((2,)),
            dma((1 + 3 * SEQS_DEV, 2 * n_x - 1)),
            dma((1,)),
            dma((2, n_x)),
            dma((1,)),
            dma((2, SEQS_DEV, n_x - 1)),
            dma((1,)),
            dma((n_out, 2, n_x)),
            dma((1,)),
            dma((n_out, 2, n_x - 1)),
            dma((1,)),
            dma((3 * SEQS_DEV + n_out,)),
        ],
        compiler_params=pltpu.CompilerParams(
            collective_id=0, has_side_effects=True, vmem_limit_bytes=62 * 1024 * 1024
        ),
    )(*args)


def solution(mesh):
    n_fs, n_tp = mesh.shape["fs"], mesh.shape["tp"]
    body = functools.partial(fused, n_fs, n_tp)
    if n_fs != 4 or n_tp != 4 or mesh.shape["grp"] != 2:
        body = on_device
    placed = (
        P(("grp", "fs"), "tp"),
        P(),
        P("fs", "tp"),
        P("fs", "tp"),
        P("fs", "tp"),
        P(None, "tp"),
        P("tp", "fs"),
        P(),
        P("fs", "tp"),
        P("fs", "tp"),
        P(None, None, "tp"),
        P(None, "tp"),
        P("tp", "fs"),
    )
    return jax.shard_map(
        body, mesh=mesh, in_specs=placed, out_specs=P(("grp", "fs"), "tp"), check_vma=False
    )
```

```python
import functools

import jax
import jax.numpy as jnp
from jax import lax
from jax.experimental import pallas as pl
from jax.experimental.pallas import tpu as pltpu
from jax.sharding import PartitionSpec as P

SEQS_DEV = 2


def conv_positions(values, taps):
    width = values.shape[1]
    blocks = values.reshape(SEQS_DEV, -1, width)
    length = blocks.shape[1]
    padded = jnp.pad(blocks, ((0, 0), (2, 0), (0, 0)))
    result = (
        padded[:, 0:length] * taps[0]
        + padded[:, 1 : length + 1] * taps[1]
        + padded[:, 2 : length + 2] * taps[2]
    )
    return result.reshape(-1, width)


def rms_norm(stream, gain):
    values = stream.astype(jnp.float32)
    scale = lax.rsqrt(jnp.mean(values * values, axis=-1, keepdims=True) + 1e-06)
    return (values * scale * gain).astype(jnp.bfloat16)


def on_device(
    tokens,
    mix_gain,
    w_signal,
    w_outer_gate,
    w_inner_gate,
    mix_taps,
    w_mix_out,
    ffn_gain,
    w_gate,
    w_value,
    up_taps,
    up_bias,
    w_down,
):
    whole = lax.all_gather(tokens, "tp", axis=1, tiled=True)
    normed = rms_norm(whole, mix_gain)
    pieces = (
        lax.all_gather(w_signal, "fs", axis=0, tiled=True),
        lax.all_gather(w_outer_gate, "fs", axis=0, tiled=True),
        lax.all_gather(w_inner_gate, "fs", axis=0, tiled=True),
    )
    columns = normed
    signal, outer, inner = tuple(
        (jnp.dot(columns, piece, preferred_element_type=jnp.float32) for piece in pieces)
    )
    signal = signal.astype(jnp.bfloat16).astype(jnp.float32)
    outer = outer.astype(jnp.bfloat16).astype(jnp.float32)
    inner = inner.astype(jnp.bfloat16).astype(jnp.float32)
    mixed = (outer * conv_positions(inner * signal, mix_taps)).astype(jnp.bfloat16)
    mix_terms = jnp.dot(
        mixed,
        lax.all_gather(w_mix_out, "fs", axis=1, tiled=True),
        preferred_element_type=jnp.float32,
    )
    mix_sum = lax.psum_scatter(
        mix_terms.astype(jnp.bfloat16), "tp", scatter_dimension=1, tiled=True
    ).astype(jnp.float32)
    resid = (tokens.astype(jnp.float32) + mix_sum).astype(jnp.bfloat16)
    whole_ffn = lax.all_gather(resid, "tp", axis=1, tiled=True)
    normed_ffn = rms_norm(whole_ffn, ffn_gain)
    pieces = (
        lax.all_gather(w_gate, "fs", axis=0, tiled=True),
        lax.all_gather(w_value, "fs", axis=0, tiled=True),
    )
    columns = normed_ffn
    gate = jnp.dot(columns, pieces[0], preferred_element_type=jnp.float32)
    value = jnp.dot(columns, pieces[1], preferred_element_type=jnp.float32)
    gate = gate.astype(jnp.bfloat16).astype(jnp.float32)
    value = value.astype(jnp.bfloat16).astype(jnp.float32)
    gate_conv = conv_positions(gate, up_taps[0]) + up_bias[0]
    value_conv = conv_positions(value, up_taps[1]) + up_bias[1]
    hidden = (jax.nn.silu(gate_conv) * value_conv).astype(jnp.bfloat16)
    ffn_terms = jnp.dot(
        hidden, lax.all_gather(w_down, "fs", axis=1, tiled=True), preferred_element_type=jnp.float32
    )
    ffn_sum = lax.psum_scatter(
        ffn_terms.astype(jnp.bfloat16), "tp", scatter_dimension=1, tiled=True
    ).astype(jnp.float32)
    return (resid.astype(jnp.float32) + ffn_sum).astype(jnp.bfloat16)


MESH = pl.DeviceIdType.MESH
UP, DOWN = 0, 1
LANES = 128


def shifted(values, by, length):
    rolled = pltpu.roll(values, by, 0)
    position = lax.rem(lax.broadcasted_iota(jnp.int32, values.shape, 0), length)
    return jnp.where(position < by, 0.0, rolled)


def conv_rows(values, taps, length):
    return (
        shifted(values, 2, length) * taps[0]
        + shifted(values, 1, length) * taps[1]
        + values * taps[2]
    )


END, INNER = 0, 1


def tiles_of(n_tiles, role):
    at_end = 2 * n_tiles // 5
    return at_end if role == END else n_tiles - at_end


def layer_kernel(
    n_fs,
    n_tp,
    tokens,
    mix_gain_given,
    w_signal,
    w_outer_gate,
    w_inner_gate,
    mix_taps_given,
    w_mix_out,
    ffn_gain_given,
    w_gate,
    w_value,
    up_taps_given,
    up_bias_given,
    w_down,
    out,
    mix_gain,
    mix_taps,
    ffn_gain,
    up_taps,
    up_bias,
    mix_in,
    mix_out,
    ffn_in,
    ffn_out,
    tok,
    res,
    normed,
    hidden,
    part_mix,
    mix_core,
    mix_x_sum,
    mix_x_got,
    mix_z_sum,
    mix_z_got,
    part_ffn,
    got_core,
    sum_x,
    got_x,
    sum_z,
    got_z,
    done,
    z_send,
    z_recv,
    f_send,
    y_send,
    y_recv,
    load_sem,
    all_send,
    all_recv,
    mix_core_send,
    mix_core_recv,
    mix_x_send,
    mix_x_recv,
    core_send,
    core_recv,
    x_send,
    x_recv,
    pair_send,
    pair_recv,
):
    g, j, k = lax.axis_index("grp"), lax.axis_index("fs"), lax.axis_index("tp")
    rows, own_cols = tokens.shape
    length = rows // SEQS_DEV
    shard, chans = w_signal.shape
    half, unit_chans = shard // 2, chans // 2
    n_tiles, n_out = w_gate.shape[1] // LANES, shard // LANES
    tiles = {END: tiles_of(n_tiles, END), INNER: tiles_of(n_tiles, INNER)}
    base = {END: 0, INNER: tiles[END]}
    n_x = n_tp // 2
    x, c = k // 2, lax.rem(k, 2)
    core = k + 1 - 2 * c
    p = lax.rem(j, 2)
    pair = j + 1 - 2 * p
    inward = jnp.where(j < n_fs // 2, 1, n_fs - 1)
    at_end = (j == 0) | (j == n_fs - 1)

    MINE, THEIRS = 0, 1

    def held_rows(o, h=None):
        side = p if o == MINE else 1 - p
        if h is None:
            return pl.ds(pl.multiple_of(side * rows, rows), rows)
        return pl.ds(pl.multiple_of(side * rows + h * length, length), length)

    def in_half(h):
        return slice(h * length, (h + 1) * length)

    mix = ("mix", 0)
    n_in = tiles[INNER]
    ins = [("in", t) for t in range(n_in)]
    outs = [("out", u) for u in range(n_out)]

    def by_role(body):
        pl.when(at_end)(functools.partial(body, END))
        pl.when(jnp.logical_not(at_end))(functools.partial(body, INNER))


    def other(d):
        return lax.rem(j + inward * d, n_fs)

    def sources(stage, role, side):
        kind, i = stage
        at_rows = pl.ds(pl.multiple_of(side * half, half), half)
        if kind == "mix":
            lanes = pl.ds(role * unit_chans, unit_chans)
            tall = unit_chans // 2
            at = pl.ds(pl.multiple_of(role * unit_chans + side * tall, tall), tall)
            refs = [ref.at[at_rows, lanes] for ref in (w_signal, w_outer_gate, w_inner_gate)]
            return [*refs, w_mix_out.at[at, :]]
        if kind == "in":
            lanes = pl.ds((base[role] + i) * LANES, LANES)
            return [w_gate.at[at_rows, lanes], w_value.at[at_rows, lanes]]
        tall = tiles[role] * LANES // 2
        at = pl.ds(pl.multiple_of(base[role] * LANES + side * tall, LANES), tall)
        return [w_down.at[at, pl.ds(i * LANES, LANES)]]

    def places(stage, role, source, side, whole):
        kind, i = stage
        at_rows = pl.ds(pl.multiple_of((source * 2 + side) * half, half), half)
        if kind == "mix":
            tall = unit_chans // 2
            at = pl.ds(pl.multiple_of(side * tall, tall), tall)
            outs = mix_out.at[source, at, :]
            if whole:
                return [mix_in.at[at_rows, :], outs]
            lanes = [pl.ds(b * unit_chans, unit_chans) for b in range(3)]
            return [*(mix_in.at[at_rows, lane] for lane in lanes), outs]
        if kind == "in":
            if whole:
                return [ffn_in.at[i, at_rows, :]]
            return [ffn_in.at[i, at_rows, pl.ds(b * LANES, LANES)] for b in (0, 1)]
        tall = tiles[role] * LANES // 2
        at = pl.ds(pl.multiple_of(side * tall, LANES), tall)
        lanes = pl.ds(pl.multiple_of(source * LANES, LANES), LANES)
        return [ffn_out.at[i, at, lanes]]

    def slot(stage, i):
        kind, at = stage
        if kind == "mix":
            return i
        return 2 + at if kind == "in" else 2 + n_in + at

    def group(stage, i):
        kind, _ = stage
        return i if kind == "mix" else {"in": 2, "out": 3}[kind]

    def to_fs(src, dst, send_sem, recv_sem, to):
        return pltpu.make_async_remote_copy(
            src_ref=src,
            dst_ref=dst,
            send_sem=send_sem,
            recv_sem=recv_sem,
            device_id={"fs": to},
            device_id_type=MESH,
        )

    def role_of(role, d):
        return INNER if d < n_fs - 1 - role else END

    def z_sends(s, role, d):
        to = other(d)
        there = role_of(role, d)
        pairs = zip(sources(s, there, g), places(s, there, j, g, False))
        copies = []
        for i, (src, dst) in enumerate(pairs):
            wide = i // 3 if s[0] == "mix" else 0
            sems = z_send.at[group(s, wide), d - 1], z_sem(s, wide, j, to)
            copies.append(to_fs(src, dst, *sems, to))
        return copies

    def z_takes(s, role, d):
        source = other(d)
        return [
            to_fs(view, view, z_send.at[group(s, i), 0], z_sem(s, i, source, j), source)
            for i, view in enumerate(places(s, role, source, g, True))
        ]

    def z_forwards(s):
        source = other(last)
        to = other(1)
        return [
            to_fs(view, view, f_send.at[group(s, i)], z_sem(s, i, source, to), to)
            for i, view in enumerate(places(s, INNER, source, g, True))
        ]

    def z_sem(s, i, source, to):
        return z_recv.at[slot(s, i), lax.rem(source - to + n_fs, n_fs) - 1]

    def to_y(src, dst, send_sem, recv_sem):
        return pltpu.make_async_remote_copy(
            src_ref=src,
            dst_ref=dst,
            send_sem=send_sem,
            recv_sem=recv_sem,
            device_id={"grp": 1 - g},
            device_id_type=MESH,
        )

    def late_d(role):
        return 1 if role == INNER else 2

    def y_copies(s, role, d):
        after = n_out if s[0] == "out" and d == late_d(role) else 0
        return [
            to_y(view, view, y_send.at[group(s, i)], y_recv.at[slot(s, i) + after])
            for i, view in enumerate(places(s, role, other(d), g, True))
        ]

    n_from = n_fs - 1

    def sums(stage, role, count):
        kind, i = stage
        if kind == "mix":
            some = mix_out.at[pl.ds(0, count), pl.ds(0, unit_chans // 2), :]
            return [mix_in.at[pl.ds(0, count * half), :], some]
        if kind == "in":
            return [ffn_in.at[i, pl.ds(0, count * half), :]]
        return [ffn_out.at[i, pl.ds(0, tiles[role] * LANES // 2), pl.ds(0, count * LANES)]]

    def all_sums(role, count):
        return [
            *sums(mix, role, count),
            *sums(("in", pl.ds(0, tiles[role])), role, count),
            *sums(("out", pl.ds(0, n_out)), role, count),
        ]

    def start(copies):
        for copy in copies:
            copy.start()

    def wait_recv(copies):
        for copy in copies:
            copy.wait_recv()

    def wait_send(copies):
        for copy in copies:
            copy.wait_send()

    def send(s, role, ds):
        for d in ds:
            if s[0] != "in" or s[1] < tiles[role_of(role, d)]:
                start(z_sends(s, role, d))

    last = n_fs - 1

    def relay(s, role, d):
        wait_recv(z_takes(s, role, d))
        start(y_copies(s, role, d))

    def ahead(s):
        relay(s, INNER, last)
        start(z_forwards(s))

    def relay_all(s, role):
        if s[0] == "in" and s[1] >= tiles[role]:
            return
        for d in (1, 2, last) if role == END else (1, 2):
            relay(s, role, d)

    def relay_both(s):
        by_role(lambda role: relay_all(s, role))

    def arrived(s, role):
        for i, view in enumerate(sums(s, role, n_from)):
            to_y(view, view, y_send.at[group(s, i)], y_recv.at[slot(s, i)]).wait_recv()

    def arrived_out(u, role, late):
        s = outs[u]
        (view,) = sums(s, role, 1 if late else n_from - 1)
        at = slot(s, 0) + (n_out if late else 0)
        to_y(view, view, y_send.at[group(s, 0)], y_recv.at[at]).wait_recv()

    def to_tp(src, dst, send_sem, recv_sem, to):
        return pltpu.make_async_remote_copy(
            src_ref=src,
            dst_ref=dst,
            send_sem=send_sem,
            recv_sem=recv_sem,
            device_id={"tp": to},
            device_id_type=MESH,
        )

    def all_copies(buffer, i, at, kind):
        sent = all_send.at[0 if i <= SEQS_DEV else 1]
        copies = []
        for dx in range(n_x):
            there = lax.rem(x + dx, n_x)
            if kind == "over":
                if dx:
                    view = buffer.at[k, at]
                    copies.append(to_tp(view, view, sent, all_recv.at[i, dx - 1], there * 2 + c))
            else:
                back = lax.rem(x + n_x - dx, n_x) * 2
                seen = back + c if kind == "pass" else back + 1 - c
                view = buffer.at[seen, at]
                copies.append(to_tp(view, view, sent, all_recv.at[i, n_x - 1], core))
        return copies

    def all_begin(buffer, i, at):
        start(all_copies(buffer, i, at, "over"))
        all_copies(buffer, i, at, "pass")[0].start()

    def all_middle(buffer, i, at):
        passed = all_copies(buffer, i, at, "pass")
        for dx in range(1, n_x):
            view = buffer.at[lax.rem(x + n_x - dx, n_x) * 2 + c, at]
            sent = all_send.at[0 if i <= SEQS_DEV else 1]
            to_tp(view, view, sent, all_recv.at[i, dx - 1], core).wait_recv()
            passed[dx].start()

    def all_end(buffer, i, at):
        view = buffer.at[pl.ds(0, n_x), at]
        to_tp(view, view, all_send.at[0], all_recv.at[i, n_x - 1], core).wait_recv()

    def to_pair(i, src, dst):
        return pltpu.make_async_remote_copy(
            src_ref=src,
            dst_ref=dst,
            send_sem=pair_send.at[0],
            recv_sem=pair_recv.at[i],
            device_id={"fs": pair},
            device_id_type=MESH,
        )

    halves = range(SEQS_DEV)
    mine, theirs = held_rows(MINE), held_rows(THEIRS)

    def tok_swap(o, h):
        view = tok.at[k, held_rows(o, h)]
        return to_pair(h, view, view)

    def res_swap(o, h):
        view = res.at[k, held_rows(o, h)]
        return to_pair(SEQS_DEV + h, view, view)

    def mix_swap(h):
        return to_pair(2 * SEQS_DEV + h, mix_z_sum.at[h], mix_z_got.at[h])

    def back(u):
        return to_pair(3 * SEQS_DEV + u, sum_z.at[u], got_z.at[u])

    barrier = pltpu.get_barrier_semaphore()
    for d in range(1, n_fs):
        to = lax.rem(j + d, n_fs)
        pl.semaphore_signal(barrier, inc=1, device_id={"fs": to}, device_id_type=MESH)
    pl.semaphore_signal(barrier, inc=1, device_id={"grp": 1 - g}, device_id_type=MESH)
    for d in range(1, n_tp):
        to = lax.rem(k + d, n_tp)
        pl.semaphore_signal(barrier, inc=1, device_id={"tp": to}, device_id_type=MESH)
    for dx in range(1, n_x):
        far = {"tp": lax.rem(x + dx, n_x) * 2 + c, "fs": pair}
        pl.semaphore_signal(barrier, inc=1, device_id=far, device_id_type=MESH)

    first = pltpu.make_async_copy(tokens, tok.at[k, mine], load_sem.at[4])
    own_rows = pl.ds(pl.multiple_of(j * shard, shard), shard)
    own_lanes = pl.ds(pl.multiple_of(j * LANES, LANES), LANES)
    inner_role = jnp.where(at_end, END, INNER)
    at_chans = pl.ds(pl.multiple_of(inner_role * unit_chans, unit_chans), unit_chans)

    def load(i, src, dst):
        pltpu.make_async_copy(src, dst, load_sem.at[i]).start()

    first.start()
    small = [
        pltpu.make_async_copy(src, dst, load_sem.at[5 + i])
        for i, (src, dst) in enumerate(
            (
                (mix_gain_given, mix_gain),
                (mix_taps_given, mix_taps),
                (ffn_gain_given, ffn_gain),
                (up_taps_given, up_taps),
                (up_bias_given, up_bias),
            )
        )
    ]
    for copy in small:
        copy.start()
    for i, ref in enumerate((w_signal, w_outer_gate, w_inner_gate)):
        load(0, ref.at[:, at_chans], mix_in.at[own_rows, pl.ds(i * unit_chans, unit_chans)])
    load(1, w_mix_out.at[at_chans, :], mix_out.at[j])
    def load_ffn(role):
        for t in range(tiles[role]):
            for i, src in enumerate((w_gate, w_value)):
                lanes = pl.ds((base[role] + t) * LANES, LANES)
                load(2, src.at[:, lanes], ffn_in.at[t, own_rows, pl.ds(i * LANES, LANES)])
        tall = tiles[role] * LANES
        for u in range(n_out):
            src = w_down.at[pl.ds(base[role] * LANES, tall), pl.ds(u * LANES, LANES)]
            load(3, src, ffn_out.at[u, pl.ds(0, tall), own_lanes])

    def wait_loads(role):
        views = [
            mix_in.at[own_rows, :],
            mix_out.at[j],
            ffn_in.at[pl.ds(0, tiles[role]), own_rows, :],
            ffn_out.at[:, pl.ds(0, tiles[role] * LANES), own_lanes],
        ]
        for i, view in enumerate(views):
            pltpu.make_async_copy(view, view, load_sem.at[i]).wait()

    with jax.named_scope("barrier"):
        first.wait()
        pl.semaphore_wait(barrier, n_fs - 1 + 1 + n_tp - 1 + n_x - 1)

    def begin(role):
        send(mix, role, (1, last) if role == END else (last, 1))
        tok_swap(MINE, 0).start()
        all_begin(tok, 0, mine)
        if role == INNER:
            send(mix, role, (2,))
        for h in halves[1:]:
            tok_swap(MINE, h).start()
        if role == END:
            for s in ins:
                send(s, role, (1,))
            for s in ins[:2]:
                send(s, role, (last,))
        load_ffn(role)

    by_role(begin)
    with jax.named_scope("loads"):
        by_role(wait_loads)
        for copy in small:
            copy.wait()

    def norm(buffer, at, gain):
        count = at.size
        squares = jnp.zeros((count, 1), jnp.float32)
        for b in range(n_tp):
            values = buffer[b, at, :].astype(jnp.float32)
            squares = squares + jnp.sum(values * values, axis=-1, keepdims=True)
        scale = lax.rsqrt(squares / (n_tp * own_cols) + 1e-06)
        for b in range(n_tp):
            cut = slice(b * own_cols, (b + 1) * own_cols)
            values = buffer[b, at, :].astype(jnp.float32)
            normed[at, cut] = (values * scale * gain[:, cut]).astype(jnp.bfloat16)

    with jax.named_scope("tok_mid"):
        all_middle(tok, 0, mine)
    def take_tok(h):
        with jax.named_scope("tok_swap"):
            tok_swap(THEIRS, h).wait_recv()
            all_begin(tok, 1 + h, held_rows(THEIRS, h))

    def pass_tok(h):
        with jax.named_scope("tok_theirs"):
            all_middle(tok, 1 + h, held_rows(THEIRS, h))

    def early(role):
        if role == END:
            with jax.named_scope("relay_mix"):
                relay(mix, role, 1)
            take_tok(0)
            with jax.named_scope("norm_mine"):
                all_end(tok, 0, mine)
                norm(tok, mine, mix_gain)
            with jax.named_scope("relay_mix"):
                relay(mix, role, 2)
            pass_tok(0)
            for h in halves[1:]:
                take_tok(h)
            with jax.named_scope("relay_mix"):
                relay(mix, role, last)
            for h in halves[1:]:
                pass_tok(h)
            return
        with jax.named_scope("relay_mix"):
            relay(mix, role, 1)
        with jax.named_scope("relay_mix"):
            ahead(mix)
        send(ins[0], role, (1, 2))
        take_tok(0)
        with jax.named_scope("norm_mine"):
            all_end(tok, 0, mine)
            norm(tok, mine, mix_gain)
        for h in halves[1:]:
            take_tok(h)
        pass_tok(0)
        with jax.named_scope("relay_mix"):
            relay(mix, role, 2)
        for s in ins[:3]:
            send(s, role, (last,))
        with jax.named_scope("ahead0"):
            ahead(ins[0])
            send(ins[1], role, (1, 2))
        for h in halves[1:]:
            pass_tok(h)

    by_role(early)
    with jax.named_scope("norm_theirs"):
        for h in halves:
            all_end(tok, 1 + h, held_rows(THEIRS, h))
        norm(tok, theirs, mix_gain)
    with jax.named_scope("arrived_mix"):
        arrived(mix, INNER)

    taps = [mix_taps[i : i + 1, at_chans] for i in range(3)]

    def mix_core_copy(o, dx):
        there = lax.rem(x + dx, n_x)
        return to_tp(
            part_mix.at[o, there * 2 + 1 - c],
            mix_core.at[o, there],
            mix_core_send.at[0],
            mix_core_recv.at[o],
            core,
        )

    def mix_core_wait(o):
        view = part_mix.at[o, pl.ds(0, n_x)]
        to_tp(view, mix_core.at[o], mix_core_send.at[0], mix_core_recv.at[o], core).wait_recv()

    def mix_x_copy(o, h, dx):
        to = lax.rem(x + dx, n_x) * 2 + c
        return to_tp(
            mix_x_sum.at[o, h, dx - 1],
            mix_x_got.at[o, h, dx - 1],
            mix_x_send.at[0],
            mix_x_recv.at[o, h, dx - 1],
            to,
        )

    def mix_chip_sum(o, h, dx):
        there = lax.rem(x + dx, n_x)
        cut = in_half(h)
        near = part_mix[o, there * 2 + c, cut, :].astype(jnp.float32)
        return near + mix_core[o, there, cut, :].astype(jnp.float32)

    def mix_place_sum(o, h):
        value = mix_chip_sum(o, h, 0)
        for dx in range(1, n_x):
            value = value + mix_x_got[o, h, dx - 1].astype(jnp.float32)
        return value

    with jax.named_scope("mixer"):
        for o, at in ((THEIRS, theirs), (MINE, mine)):
            both = jnp.dot(normed[at, :], mix_in[...], preferred_element_type=jnp.float32)
            both = both.astype(jnp.bfloat16).astype(jnp.float32)
            gated = both[:, 2 * unit_chans :] * both[:, :unit_chans]
            conv = conv_rows(gated, taps, length)
            mixed = (both[:, unit_chans : 2 * unit_chans] * conv).astype(jnp.bfloat16)
            for b in range(n_fs):
                terms = jnp.dot(mixed, mix_out[b], preferred_element_type=jnp.float32)
                part_mix[o, b] = terms.astype(jnp.bfloat16)
            for dx in (*range(1, n_x), 0):
                mix_core_copy(o, dx).start()

    with jax.named_scope("mix_core"):
        for o in (THEIRS, MINE):
            mix_core_wait(o)
            for dx in range(1, n_x):
                for h in halves:
                    mix_x_sum[o, h, dx - 1] = mix_chip_sum(o, h, dx).astype(jnp.bfloat16)
                    mix_x_copy(o, h, dx).start()

    def between(role):
        if role == INNER:
            with jax.named_scope("ahead1"):
                for at in (1, 2):
                    ahead(ins[at])
                    send(ins[at + 1], role, (1, 2))
        with jax.named_scope("relay_in0"):
            relay_all(ins[0], role)

    by_role(between)

    with jax.named_scope("mix_x_theirs"):
        for h in halves:
            for dx in range(1, n_x):
                mix_x_copy(THEIRS, h, dx).wait_recv()
            mix_z_sum[h] = mix_place_sum(THEIRS, h).astype(jnp.bfloat16)
            mix_swap(h).start()

    def second(role):
        if role == END:
            send(ins[2], role, (last,))
            for s in outs[:2]:
                send(s, role, (1,))
        else:
            with jax.named_scope("ahead3"):
                for at in range(3, n_in):
                    ahead(ins[at])
                    if at + 1 < n_in:
                        send(ins[at + 1], role, (1, 2))
        with jax.named_scope("relay_in1"):
            relay_all(ins[1], role)

    by_role(second)
    with jax.named_scope("mix_mine"):
        for h in halves:
            for dx in range(1, n_x):
                mix_x_copy(MINE, h, dx).wait_recv()
            mix_swap(h).wait_recv()
            mixer = mix_place_sum(MINE, h) + mix_z_got[h].astype(jnp.float32)
            at = held_rows(MINE, h)
            res[k, at, :] = (tok[k, at, :].astype(jnp.float32) + mixer).astype(jnp.bfloat16)
            res_swap(MINE, h).start()
            all_begin(res, 1 + SEQS_DEV + h, at)

    def third(role):
        for s in ins[3:]:
            send(s, role, (last,))
        for s in outs[2:] if role == END else ():
            send(s, role, (1,))
        for s in outs if role == INNER else ():
            send(s, role, (1, 2, last))
        with jax.named_scope("relay_in2"):
            relay_all(ins[2], role)

    by_role(third)
    with jax.named_scope("res_mid"):
        for h in halves:
            all_middle(res, 1 + SEQS_DEV + h, held_rows(MINE, h))
    @pl.when(jnp.logical_not(at_end))
    def _():
        with jax.named_scope("relay_in3"):
            relay_all(ins[3], INNER)

    with jax.named_scope("res_swap"):
        for h in halves:
            res_swap(THEIRS, h).wait_recv()
            all_begin(res, 1 + 2 * SEQS_DEV + h, held_rows(THEIRS, h))
    @pl.when(at_end)
    def _():
        with jax.named_scope("relay_in3"):
            relay_all(ins[3], END)

    @pl.when(jnp.logical_not(at_end))
    def _():
        for s in outs[:2]:
            relay(s, INNER, last)

    with jax.named_scope("res_norm"):
        for h in halves:
            all_end(res, 1 + SEQS_DEV + h, held_rows(MINE, h))
            norm(res, held_rows(MINE, h), ffn_gain)
    def fourth(role):
        if role == INNER:
            with jax.named_scope("relay_in4"):
                relay_all(ins[4], INNER)

    by_role(fourth)
    with jax.named_scope("res_mid2"):
        for h in halves:
            all_middle(res, 1 + 2 * SEQS_DEV + h, held_rows(THEIRS, h))
    with jax.named_scope("res_norm2"):
        for h in halves:
            all_end(res, 1 + 2 * SEQS_DEV + h, held_rows(THEIRS, h))
            norm(res, held_rows(THEIRS, h), ffn_gain)

    first_tile = jnp.where(at_end, base[END], base[INNER])

    def feed(t):
        with jax.named_scope("in_wait"):
            arrived(("in", t), INNER)
        cut = pl.ds(pl.multiple_of((first_tile + t) * LANES, LANES), LANES)
        both = jnp.dot(normed[...], ffn_in[t], preferred_element_type=jnp.float32)
        both = both.astype(jnp.bfloat16).astype(jnp.float32)
        gate_taps, value_taps = ([up_taps[i, b : b + 1, cut] for i in range(3)] for b in (0, 1))
        gate = conv_rows(both[:, :LANES], gate_taps, length) + up_bias[0:1, cut]
        value = conv_rows(both[:, LANES:], value_taps, length) + up_bias[1:2, cut]
        unit = (gate / (1.0 + jnp.exp(-gate)) * value).astype(jnp.bfloat16)
        hidden[:, pl.ds(pl.multiple_of(t * LANES, LANES), LANES)] = unit

    paced = {0: outs[:1], 2: outs[1:2], 3: outs[2:]}
    beside = {
        (INNER, 2): [(ins[5], 1), (ins[5], 2)],
        (INNER, 4): [(outs[0], 2), (outs[2], last), (outs[3], last)],
        (INNER, 5): [(outs[1], 2)],
        (END, 1): [(stage, 1) for stage in outs],
        (END, 3): [(outs[0], last)],
    }
    ready = {
        INNER: [[], [(outs[2], 2)], [(outs[3], 2)]],
        END: [[(stage, last)] for stage in outs[1:]],
    }

    @pl.loop(0, jnp.where(at_end, tiles[END], tiles[INNER]))
    def _(t):
        for at, stages in paced.items():

            @pl.when(at_end & (t == at))
            def _():
                for stage in stages:
                    send(stage, END, (2, last))

        for (role, at), relays in beside.items():
            here = at_end if role == END else jnp.logical_not(at_end)

            @pl.when(here & (t == at))
            def _():
                for stage, d in relays:
                    with jax.named_scope("relay_beside"):
                        relay(stage, role, d)

        feed(t)

    middle = n_fs // 2
    left = j < middle
    late_block = jnp.where(left, middle, middle - 1)

    def when_block(block, late):
        return pl.when(block == late_block if late else block != late_block)

    def core_copy(u, o, dx):
        there = lax.rem(x + dx, n_x)
        return to_tp(
            part_ffn.at[u, o, there * 2 + 1 - c],
            got_core.at[u, o, there],
            core_send.at[0],
            core_recv.at[u, o, dx],
            core,
        )

    def x_copy(u, o, dx):
        to = lax.rem(x + dx, n_x) * 2 + c
        straight = u == n_out - 1 and o == THEIRS
        return pltpu.make_async_remote_copy(
            src_ref=sum_x.at[u, o, dx - 1],
            dst_ref=got_x.at[u, o, dx - 1],
            send_sem=x_send.at[0],
            recv_sem=x_recv.at[u, o, dx - 1],
            device_id={"tp": to, "fs": pair} if straight else {"tp": to},
            device_id_type=MESH,
        )

    def chip_sum(u, o, dx):
        there = lax.rem(x + dx, n_x)
        mine_there = part_ffn[u, o, there * 2 + c].astype(jnp.float32)
        return mine_there + got_core[u, o, there].astype(jnp.float32)

    def place_sum(u, o):
        value = chip_sum(u, o, 0)
        for dx in range(1, n_x):
            value = value + got_x[u, o, dx - 1].astype(jnp.float32)
        return value

    def product(u, o, deep, first, count):
        at = theirs if o == THEIRS else mine
        lanes = pl.ds(pl.multiple_of(first * LANES, LANES), count * LANES)
        left_side, right_side = hidden[at, deep], ffn_out[u, deep, lanes]
        terms = jnp.dot(left_side, right_side, preferred_element_type=jnp.float32)
        for b in range(count):
            part_ffn[u, o, first + b] = terms[:, b * LANES : (b + 1) * LANES].astype(jnp.bfloat16)

    def down(u, late):
        def body(role):
            arrived_out(u, role, late)
            deep = pl.ds(0, tiles[role] * LANES)
            for o in (THEIRS, MINE):
                if late:
                    product(u, o, deep, late_block, 1)
                else:
                    product(u, o, deep, jnp.where(left, 0, middle), middle)
                    product(u, o, deep, jnp.where(left, n_fs - 1, 0), 1)

        with jax.named_scope("down_late" if late else "down"):
            by_role(body)
        for o in (THEIRS, MINE):
            for dx in (*range(1, n_x), 0):
                block = lax.rem(x + dx, n_x) * 2 + 1 - c

                @when_block(block, late)
                def _():
                    core_copy(u, o, dx).start()

    def over_x(u, late):
        for dx in range(1, n_x):

            @when_block(lax.rem(x + dx, n_x) * 2 + c, late)
            def _():
                with jax.named_scope("over_x"):
                    for o in (THEIRS, MINE):
                        core_copy(u, o, dx).wait_recv()
                        sum_x[u, o, dx - 1] = chip_sum(u, o, dx).astype(jnp.bfloat16)
                        x_copy(u, o, dx).start()

    def over_z(u, late):
        @when_block(k, late)
        def _():
            with jax.named_scope("over_z"):
                core_copy(u, THEIRS, 0).wait_recv()
                if u == n_out - 1:
                    value = chip_sum(u, THEIRS, 0)
                else:
                    for dx in range(1, n_x):
                        x_copy(u, THEIRS, dx).wait_recv()
                    value = place_sum(u, THEIRS)
                sum_z[u] = value.astype(jnp.bfloat16)
                back(u).start()

    def relay_late(u):
        with jax.named_scope("relay_late"):
            by_role(lambda role: relay(outs[u], role, late_d(role)))

    def relay_ready(i):
        def body(role):
            for stage, d in ready[role][i]:
                with jax.named_scope("relay_ready"):
                    relay(stage, role, d)

        by_role(body)

    early, late = False, True
    relay_ready(0)
    down(0, early)
    relay_ready(1)
    over_x(0, early)
    down(1, early)
    relay_ready(2)
    relay_late(0)
    over_x(1, early)
    down(2, early)
    over_x(2, early)
    down(3, early)
    relay_late(1)
    over_x(3, early)
    over_z(3, early)
    down(0, late)
    relay_late(2)
    over_x(0, late)
    over_z(0, early)
    down(1, late)
    relay_late(3)
    over_x(1, late)
    over_z(1, early)
    down(2, late)
    over_x(2, late)
    over_z(0, late)
    down(3, late)
    over_x(3, late)
    over_z(3, late)
    over_z(2, early)
    over_z(1, late)
    over_z(2, late)

    def result(u):
        cut = pl.ds(u * LANES, LANES)
        return pltpu.make_async_copy(done.at[u], out.at[:, cut], load_sem.at[u])

    with jax.named_scope("final"):
        for u in range(n_out):
            cut = slice(u * LANES, (u + 1) * LANES)
            core_copy(u, MINE, 0).wait_recv()
            for dx in range(1, n_x):
                x_copy(u, MINE, dx).wait_recv()
            value = res[k, mine, cut].astype(jnp.float32) + place_sum(u, MINE)
            back(u).wait_recv()
            value = value + got_z[u].astype(jnp.float32)
            for dx in range(1, n_x) if u == n_out - 1 else ():
                x_copy(u, THEIRS, dx).wait_recv()
                value = value + got_x[u, THEIRS, dx - 1].astype(jnp.float32)
            done[u] = value.astype(jnp.bfloat16)
            result(u).start()

    with jax.named_scope("drain"):
        for u in range(n_out):
            result(u).wait()
        def drain(role):
            for i, view in enumerate(all_sums(role, n_from)):
                to_y(view, view, y_send.at[i], y_recv.at[0]).wait_send()
            for d in range(1, n_fs):
                for i, view in enumerate(all_sums(role_of(role, d), 1)):
                    if (role, d) != (END, 2) or i == 3:
                        to_fs(view, view, z_send.at[i, d - 1], z_recv.at[0, 0], pair).wait_send()
            if role == INNER:
                for i, view in enumerate(all_sums(role, 1)[:3]):
                    to_fs(view, view, f_send.at[i], z_recv.at[0, 0], pair).wait_send()

        by_role(drain)
        for i, buffer in enumerate((tok, res)):
            view = buffer.at[pl.ds(0, n_tp - 1)]
            to_tp(view, view, all_send.at[i], all_recv.at[0, 0], core).wait_send()
        view = part_mix.at[:, pl.ds(0, n_x)]
        to_tp(view, view, mix_core_send.at[0], all_recv.at[0, 0], core).wait_send()
        to_tp(mix_x_sum, mix_x_sum, mix_x_send.at[0], all_recv.at[0, 0], core).wait_send()
        view = part_ffn.at[:, :, pl.ds(0, n_x)]
        to_tp(view, view, core_send.at[0], all_recv.at[0, 0], core).wait_send()
        to_tp(sum_x, sum_x, x_send.at[0], all_recv.at[0, 0], core).wait_send()
        view = tok.at[pl.ds(0, 2)]
        to_pair(0, view, view).wait_send()


def fused(n_fs, n_tp, *args):
    tokens, w_signal, w_gate = args[0], args[2], args[8]
    rows, cols = tokens.shape
    shard, chans = w_signal.shape
    n_in, n_out = tiles_of(w_gate.shape[1] // LANES, INNER), shard // LANES
    units = n_in * LANES
    width = n_fs * shard
    args = list(args)
    args[1], args[7] = args[1].reshape(1, -1), args[7].reshape(1, -1)
    args[10] = args[10].transpose(1, 0, 2)
    small = [pltpu.VMEM(args[i].shape, jnp.float32) for i in (1, 5, 7, 10, 11)]
    n_x = n_tp // 2
    length = rows // SEQS_DEV
    dma = pltpu.SemaphoreType.DMA

    def held(*shape):
        return pltpu.VMEM(shape, jnp.bfloat16)

    return pl.pallas_call(
        functools.partial(layer_kernel, n_fs, n_tp),
        out_shape=jax.ShapeDtypeStruct((rows, cols), jnp.bfloat16),
        in_specs=[pl.BlockSpec(memory_space=pl.ANY)] * len(args),
        out_specs=pl.BlockSpec(memory_space=pl.ANY),
        scratch_shapes=[
            *small,
            held(width, 3 * (chans // 2)),
            held(n_fs, chans // 2, shard),
            held(n_in, width, 2 * LANES),
            held(n_out, units, n_fs * LANES),
            held(n_tp, 2 * rows, cols),
            held(n_tp, 2 * rows, cols),
            held(2 * rows, width),
            held(2 * rows, units),
            held(2, n_tp, rows, cols),
            held(2, n_x, rows, cols),
            held(2, SEQS_DEV, n_x - 1, length, cols),
            held(2, SEQS_DEV, n_x - 1, length, cols),
            held(SEQS_DEV, length, cols),
            held(SEQS_DEV, length, cols),
            held(n_out, 2, n_tp, rows, LANES),
            held(n_out, 2, n_x, rows, LANES),
            held(n_out, 2, n_x - 1, rows, LANES),
            held(n_out, 2, n_x - 1, rows, LANES),
            held(n_out, rows, LANES),
            held(n_out, rows, LANES),
            held(n_out, rows, LANES),
            dma((4, n_fs - 1)),
            dma((2 + n_in + n_out, n_fs - 1)),
            dma((4,)),
            dma((4,)),
            dma((2 + n_in + 2 * n_out,)),
            dma((10,)),
            dma((2,)),
            dma((1 + 3 * SEQS_DEV, n_x)),
            dma((1,)),
            dma((2,)),
            dma((1,)),
            dma((2, SEQS_DEV, n_x - 1)),
            dma((1,)),
            dma((n_out, 2, n_x)),
            dma((1,)),
            dma((n_out, 2, n_x - 1)),
            dma((1,)),
            dma((3 * SEQS_DEV + n_out,)),
        ],
        compiler_params=pltpu.CompilerParams(
            collective_id=0, has_side_effects=True, vmem_limit_bytes=62 * 1024 * 1024
        ),
    )(*args)


def solution(mesh):
    n_fs, n_tp = mesh.shape["fs"], mesh.shape["tp"]
    body = functools.partial(fused, n_fs, n_tp)
    if n_fs != 4 or n_tp != 4 or mesh.shape["grp"] != 2:
        body = on_device
    placed = (
        P(("grp", "fs"), "tp"),
        P(),
        P("fs", "tp"),
        P("fs", "tp"),
        P("fs", "tp"),
        P(None, "tp"),
        P("tp", "fs"),
        P(),
        P("fs", "tp"),
        P("fs", "tp"),
        P(None, None, "tp"),
        P(None, "tp"),
        P("tp", "fs"),
    )
    return jax.shard_map(
        body, mesh=mesh, in_specs=placed, out_specs=P(("grp", "fs"), "tp"), check_vma=False
    )
```

```python
import functools

import jax
import jax.numpy as jnp
from jax import lax
from jax.experimental import pallas as pl
from jax.experimental.pallas import tpu as pltpu
from jax.sharding import PartitionSpec as P

SEQS_DEV = 2


def conv_positions(values, taps):
    width = values.shape[1]
    blocks = values.reshape(SEQS_DEV, -1, width)
    length = blocks.shape[1]
    padded = jnp.pad(blocks, ((0, 0), (2, 0), (0, 0)))
    result = (
        padded[:, 0:length] * taps[0]
        + padded[:, 1 : length + 1] * taps[1]
        + padded[:, 2 : length + 2] * taps[2]
    )
    return result.reshape(-1, width)


def rms_norm(stream, gain):
    values = stream.astype(jnp.float32)
    scale = lax.rsqrt(jnp.mean(values * values, axis=-1, keepdims=True) + 1e-06)
    return (values * scale * gain).astype(jnp.bfloat16)


def on_device(
    tokens,
    mix_gain,
    w_signal,
    w_outer_gate,
    w_inner_gate,
    mix_taps,
    w_mix_out,
    ffn_gain,
    w_gate,
    w_value,
    up_taps,
    up_bias,
    w_down,
):
    whole = lax.all_gather(tokens, "tp", axis=1, tiled=True)
    normed = rms_norm(whole, mix_gain)
    pieces = (
        lax.all_gather(w_signal, "fs", axis=0, tiled=True),
        lax.all_gather(w_outer_gate, "fs", axis=0, tiled=True),
        lax.all_gather(w_inner_gate, "fs", axis=0, tiled=True),
    )
    columns = normed
    signal, outer, inner = tuple(
        (jnp.dot(columns, piece, preferred_element_type=jnp.float32) for piece in pieces)
    )
    signal = signal.astype(jnp.bfloat16).astype(jnp.float32)
    outer = outer.astype(jnp.bfloat16).astype(jnp.float32)
    inner = inner.astype(jnp.bfloat16).astype(jnp.float32)
    mixed = (outer * conv_positions(inner * signal, mix_taps)).astype(jnp.bfloat16)
    mix_terms = jnp.dot(
        mixed,
        lax.all_gather(w_mix_out, "fs", axis=1, tiled=True),
        preferred_element_type=jnp.float32,
    )
    mix_sum = lax.psum_scatter(
        mix_terms.astype(jnp.bfloat16), "tp", scatter_dimension=1, tiled=True
    ).astype(jnp.float32)
    resid = (tokens.astype(jnp.float32) + mix_sum).astype(jnp.bfloat16)
    whole_ffn = lax.all_gather(resid, "tp", axis=1, tiled=True)
    normed_ffn = rms_norm(whole_ffn, ffn_gain)
    pieces = (
        lax.all_gather(w_gate, "fs", axis=0, tiled=True),
        lax.all_gather(w_value, "fs", axis=0, tiled=True),
    )
    columns = normed_ffn
    gate = jnp.dot(columns, pieces[0], preferred_element_type=jnp.float32)
    value = jnp.dot(columns, pieces[1], preferred_element_type=jnp.float32)
    gate = gate.astype(jnp.bfloat16).astype(jnp.float32)
    value = value.astype(jnp.bfloat16).astype(jnp.float32)
    gate_conv = conv_positions(gate, up_taps[0]) + up_bias[0]
    value_conv = conv_positions(value, up_taps[1]) + up_bias[1]
    hidden = (jax.nn.silu(gate_conv) * value_conv).astype(jnp.bfloat16)
    ffn_terms = jnp.dot(
        hidden, lax.all_gather(w_down, "fs", axis=1, tiled=True), preferred_element_type=jnp.float32
    )
    ffn_sum = lax.psum_scatter(
        ffn_terms.astype(jnp.bfloat16), "tp", scatter_dimension=1, tiled=True
    ).astype(jnp.float32)
    return (resid.astype(jnp.float32) + ffn_sum).astype(jnp.bfloat16)


MESH = pl.DeviceIdType.MESH
UP, DOWN = 0, 1
LANES = 128


def shifted(values, by, length):
    rolled = pltpu.roll(values, by, 0)
    position = lax.rem(lax.broadcasted_iota(jnp.int32, values.shape, 0), length)
    return jnp.where(position < by, 0.0, rolled)


def conv_rows(values, taps, length):
    return (
        shifted(values, 2, length) * taps[0]
        + shifted(values, 1, length) * taps[1]
        + values * taps[2]
    )


END, INNER = 0, 1


def tiles_of(n_tiles, role):
    at_end = 2 * n_tiles // 5
    return at_end if role == END else n_tiles - at_end


def layer_kernel(
    n_fs,
    n_tp,
    tokens,
    mix_gain_given,
    w_signal,
    w_outer_gate,
    w_inner_gate,
    mix_taps_given,
    w_mix_out,
    ffn_gain_given,
    w_gate,
    w_value,
    up_taps_given,
    up_bias_given,
    w_down,
    out,
    mix_gain,
    mix_taps,
    ffn_gain,
    up_taps,
    up_bias,
    mix_in,
    mix_out,
    ffn_in,
    ffn_out,
    tok,
    res,
    normed,
    hidden,
    part_mix,
    mix_core,
    mix_x_sum,
    mix_x_got,
    mix_z_sum,
    mix_z_got,
    part_ffn,
    got_core,
    sum_x,
    got_x,
    sum_z,
    got_z,
    done,
    z_send,
    z_recv,
    f_send,
    y_send,
    y_recv,
    load_sem,
    all_send,
    all_recv,
    mix_core_send,
    mix_core_recv,
    mix_x_send,
    mix_x_recv,
    core_send,
    core_recv,
    x_send,
    x_recv,
    pair_send,
    pair_recv,
):
    g, j, k = lax.axis_index("grp"), lax.axis_index("fs"), lax.axis_index("tp")
    rows, own_cols = tokens.shape
    length = rows // SEQS_DEV
    shard, chans = w_signal.shape
    half, unit_chans = shard // 2, chans // 2
    n_tiles, n_out = w_gate.shape[1] // LANES, shard // LANES
    tiles = {END: tiles_of(n_tiles, END), INNER: tiles_of(n_tiles, INNER)}
    base = {END: 0, INNER: tiles[END]}
    n_x = n_tp // 2
    x, c = k // 2, lax.rem(k, 2)
    core = k + 1 - 2 * c
    p = lax.rem(j, 2)
    pair = j + 1 - 2 * p
    inward = jnp.where(j < n_fs // 2, 1, n_fs - 1)
    at_end = (j == 0) | (j == n_fs - 1)

    MINE, THEIRS = 0, 1

    def held_rows(o, h=None):
        side = p if o == MINE else 1 - p
        if h is None:
            return pl.ds(pl.multiple_of(side * rows, rows), rows)
        return pl.ds(pl.multiple_of(side * rows + h * length, length), length)

    def in_half(h):
        return slice(h * length, (h + 1) * length)

    mix = ("mix", 0)
    n_in = tiles[INNER]
    ins = [("in", t) for t in range(n_in)]
    outs = [("out", u) for u in range(n_out)]

    def by_role(body):
        pl.when(at_end)(functools.partial(body, END))
        pl.when(jnp.logical_not(at_end))(functools.partial(body, INNER))


    def other(d):
        return lax.rem(j + inward * d, n_fs)

    def sources(stage, role, side):
        kind, i = stage
        at_rows = pl.ds(pl.multiple_of(side * half, half), half)
        if kind == "mix":
            lanes = pl.ds(role * unit_chans, unit_chans)
            tall = unit_chans // 2
            at = pl.ds(pl.multiple_of(role * unit_chans + side * tall, tall), tall)
            refs = [ref.at[at_rows, lanes] for ref in (w_signal, w_outer_gate, w_inner_gate)]
            return [*refs, w_mix_out.at[at, :]]
        if kind == "in":
            lanes = pl.ds((base[role] + i) * LANES, LANES)
            return [w_gate.at[at_rows, lanes], w_value.at[at_rows, lanes]]
        tall = tiles[role] * LANES // 2
        at = pl.ds(pl.multiple_of(base[role] * LANES + side * tall, LANES), tall)
        return [w_down.at[at, pl.ds(i * LANES, LANES)]]

    def places(stage, role, source, side, whole):
        kind, i = stage
        at_rows = pl.ds(pl.multiple_of((source * 2 + side) * half, half), half)
        if kind == "mix":
            tall = unit_chans // 2
            at = pl.ds(pl.multiple_of(side * tall, tall), tall)
            outs = mix_out.at[source, at, :]
            if whole:
                return [mix_in.at[at_rows, :], outs]
            lanes = [pl.ds(b * unit_chans, unit_chans) for b in range(3)]
            return [*(mix_in.at[at_rows, lane] for lane in lanes), outs]
        if kind == "in":
            if whole:
                return [ffn_in.at[i, at_rows, :]]
            return [ffn_in.at[i, at_rows, pl.ds(b * LANES, LANES)] for b in (0, 1)]
        tall = tiles[role] * LANES // 2
        at = pl.ds(pl.multiple_of(side * tall, LANES), tall)
        lanes = pl.ds(pl.multiple_of(source * LANES, LANES), LANES)
        return [ffn_out.at[i, at, lanes]]

    def slot(stage, i):
        kind, at = stage
        if kind == "mix":
            return i
        return 2 + at if kind == "in" else 2 + n_in + at

    def group(stage, i):
        kind, _ = stage
        return i if kind == "mix" else {"in": 2, "out": 3}[kind]

    def to_fs(src, dst, send_sem, recv_sem, to):
        return pltpu.make_async_remote_copy(
            src_ref=src,
            dst_ref=dst,
            send_sem=send_sem,
            recv_sem=recv_sem,
            device_id={"fs": to},
            device_id_type=MESH,
        )

    def role_of(role, d):
        return INNER if d < n_fs - 1 - role else END

    def z_sends(s, role, d):
        to = other(d)
        there = role_of(role, d)
        pairs = zip(sources(s, there, g), places(s, there, j, g, False))
        copies = []
        for i, (src, dst) in enumerate(pairs):
            wide = i // 3 if s[0] == "mix" else 0
            sems = z_send.at[group(s, wide), d - 1], z_sem(s, wide, j, to)
            copies.append(to_fs(src, dst, *sems, to))
        return copies

    def z_takes(s, role, d):
        source = other(d)
        return [
            to_fs(view, view, z_send.at[group(s, i), 0], z_sem(s, i, source, j), source)
            for i, view in enumerate(places(s, role, source, g, True))
        ]

    def z_forwards(s):
        source = other(last)
        to = other(1)
        return [
            to_fs(view, view, f_send.at[group(s, i)], z_sem(s, i, source, to), to)
            for i, view in enumerate(places(s, INNER, source, g, True))
        ]

    def z_sem(s, i, source, to):
        return z_recv.at[slot(s, i), lax.rem(source - to + n_fs, n_fs) - 1]

    def to_y(src, dst, send_sem, recv_sem):
        return pltpu.make_async_remote_copy(
            src_ref=src,
            dst_ref=dst,
            send_sem=send_sem,
            recv_sem=recv_sem,
            device_id={"grp": 1 - g},
            device_id_type=MESH,
        )

    def late_d(role):
        return 1 if role == INNER else 2

    def y_copies(s, role, d):
        after = n_out if s[0] == "out" and d == late_d(role) else 0
        return [
            to_y(view, view, y_send.at[group(s, i)], y_recv.at[slot(s, i) + after])
            for i, view in enumerate(places(s, role, other(d), g, True))
        ]

    n_from = n_fs - 1

    def sums(stage, role, count):
        kind, i = stage
        if kind == "mix":
            some = mix_out.at[pl.ds(0, count), pl.ds(0, unit_chans // 2), :]
            return [mix_in.at[pl.ds(0, count * half), :], some]
        if kind == "in":
            return [ffn_in.at[i, pl.ds(0, count * half), :]]
        return [ffn_out.at[i, pl.ds(0, tiles[role] * LANES // 2), pl.ds(0, count * LANES)]]

    def all_sums(role, count):
        return [
            *sums(mix, role, count),
            *sums(("in", pl.ds(0, tiles[role])), role, count),
            *sums(("out", pl.ds(0, n_out)), role, count),
        ]

    def start(copies):
        for copy in copies:
            copy.start()

    def wait_recv(copies):
        for copy in copies:
            copy.wait_recv()

    def wait_send(copies):
        for copy in copies:
            copy.wait_send()

    def send(s, role, ds):
        for d in ds:
            if s[0] != "in" or s[1] < tiles[role_of(role, d)]:
                start(z_sends(s, role, d))

    last = n_fs - 1

    def relay(s, role, d):
        wait_recv(z_takes(s, role, d))
        start(y_copies(s, role, d))

    def ahead(s):
        relay(s, INNER, last)
        start(z_forwards(s))

    def relay_all(s, role):
        if s[0] == "in" and s[1] >= tiles[role]:
            return
        for d in (1, 2, last) if role == END else (1, 2):
            relay(s, role, d)

    def relay_both(s):
        by_role(lambda role: relay_all(s, role))

    def arrived(s, role):
        for i, view in enumerate(sums(s, role, n_from)):
            to_y(view, view, y_send.at[group(s, i)], y_recv.at[slot(s, i)]).wait_recv()

    def arrived_out(u, role, late):
        s = outs[u]
        (view,) = sums(s, role, 1 if late else n_from - 1)
        at = slot(s, 0) + (n_out if late else 0)
        to_y(view, view, y_send.at[group(s, 0)], y_recv.at[at]).wait_recv()

    def to_tp(src, dst, send_sem, recv_sem, to):
        return pltpu.make_async_remote_copy(
            src_ref=src,
            dst_ref=dst,
            send_sem=send_sem,
            recv_sem=recv_sem,
            device_id={"tp": to},
            device_id_type=MESH,
        )

    def all_copies(buffer, i, at, kind):
        sent = all_send.at[0 if i <= SEQS_DEV else 1]
        copies = []
        for dx in range(n_x):
            there = lax.rem(x + dx, n_x)
            if kind == "over":
                if dx:
                    view = buffer.at[k, at]
                    copies.append(to_tp(view, view, sent, all_recv.at[i, dx - 1], there * 2 + c))
            else:
                back = lax.rem(x + n_x - dx, n_x) * 2
                seen = back + c if kind == "pass" else back + 1 - c
                view = buffer.at[seen, at]
                copies.append(to_tp(view, view, sent, all_recv.at[i, n_x - 1], core))
        return copies

    def all_begin(buffer, i, at):
        start(all_copies(buffer, i, at, "over"))
        all_copies(buffer, i, at, "pass")[0].start()

    def all_middle(buffer, i, at):
        passed = all_copies(buffer, i, at, "pass")
        for dx in range(1, n_x):
            view = buffer.at[lax.rem(x + n_x - dx, n_x) * 2 + c, at]
            sent = all_send.at[0 if i <= SEQS_DEV else 1]
            to_tp(view, view, sent, all_recv.at[i, dx - 1], core).wait_recv()
            passed[dx].start()

    def all_end(buffer, i, at):
        view = buffer.at[pl.ds(0, n_x), at]
        to_tp(view, view, all_send.at[0], all_recv.at[i, n_x - 1], core).wait_recv()

    def to_pair(i, src, dst):
        return pltpu.make_async_remote_copy(
            src_ref=src,
            dst_ref=dst,
            send_sem=pair_send.at[0],
            recv_sem=pair_recv.at[i],
            device_id={"fs": pair},
            device_id_type=MESH,
        )

    halves = range(SEQS_DEV)
    mine, theirs = held_rows(MINE), held_rows(THEIRS)

    def tok_swap(o, h):
        view = tok.at[k, held_rows(o, h)]
        return to_pair(h, view, view)

    def res_swap(o, h):
        view = res.at[k, held_rows(o, h)]
        return to_pair(SEQS_DEV + h, view, view)

    def mix_swap(h):
        return to_pair(2 * SEQS_DEV + h, mix_z_sum.at[h], mix_z_got.at[h])

    def back(u):
        return to_pair(3 * SEQS_DEV + u, sum_z.at[u], got_z.at[u])

    barrier = pltpu.get_barrier_semaphore()
    for d in range(1, n_fs):
        to = lax.rem(j + d, n_fs)
        pl.semaphore_signal(barrier, inc=1, device_id={"fs": to}, device_id_type=MESH)
    pl.semaphore_signal(barrier, inc=1, device_id={"grp": 1 - g}, device_id_type=MESH)
    for d in range(1, n_tp):
        to = lax.rem(k + d, n_tp)
        pl.semaphore_signal(barrier, inc=1, device_id={"tp": to}, device_id_type=MESH)
    for dx in range(1, n_x):
        far = {"tp": lax.rem(x + dx, n_x) * 2 + c, "fs": pair}
        pl.semaphore_signal(barrier, inc=1, device_id=far, device_id_type=MESH)

    first = pltpu.make_async_copy(tokens, tok.at[k, mine], load_sem.at[4])
    own_rows = pl.ds(pl.multiple_of(j * shard, shard), shard)
    own_lanes = pl.ds(pl.multiple_of(j * LANES, LANES), LANES)
    inner_role = jnp.where(at_end, END, INNER)
    at_chans = pl.ds(pl.multiple_of(inner_role * unit_chans, unit_chans), unit_chans)

    def load(i, src, dst):
        pltpu.make_async_copy(src, dst, load_sem.at[i]).start()

    first.start()
    small = [
        pltpu.make_async_copy(src, dst, load_sem.at[5 + i])
        for i, (src, dst) in enumerate(
            (
                (mix_gain_given, mix_gain),
                (mix_taps_given, mix_taps),
                (ffn_gain_given, ffn_gain),
                (up_taps_given, up_taps),
                (up_bias_given, up_bias),
            )
        )
    ]
    for copy in small:
        copy.start()
    for i, ref in enumerate((w_signal, w_outer_gate, w_inner_gate)):
        load(0, ref.at[:, at_chans], mix_in.at[own_rows, pl.ds(i * unit_chans, unit_chans)])
    load(1, w_mix_out.at[at_chans, :], mix_out.at[j])
    def load_ffn(role):
        for t in range(tiles[role]):
            for i, src in enumerate((w_gate, w_value)):
                lanes = pl.ds((base[role] + t) * LANES, LANES)
                load(2, src.at[:, lanes], ffn_in.at[t, own_rows, pl.ds(i * LANES, LANES)])
        tall = tiles[role] * LANES
        for u in range(n_out):
            src = w_down.at[pl.ds(base[role] * LANES, tall), pl.ds(u * LANES, LANES)]
            load(3, src, ffn_out.at[u, pl.ds(0, tall), own_lanes])

    def wait_loads(role):
        views = [
            mix_in.at[own_rows, :],
            mix_out.at[j],
            ffn_in.at[pl.ds(0, tiles[role]), own_rows, :],
            ffn_out.at[:, pl.ds(0, tiles[role] * LANES), own_lanes],
        ]
        for i, view in enumerate(views):
            pltpu.make_async_copy(view, view, load_sem.at[i]).wait()

    with jax.named_scope("barrier"):
        first.wait()
        pl.semaphore_wait(barrier, n_fs - 1 + 1 + n_tp - 1 + n_x - 1)

    def begin(role):
        send(mix, role, (1, last) if role == END else (last, 1))
        tok_swap(MINE, 0).start()
        all_begin(tok, 0, mine)
        if role == INNER:
            send(mix, role, (2,))
        for h in halves[1:]:
            tok_swap(MINE, h).start()
        if role == END:
            for s in ins:
                send(s, role, (1,))
            for s in ins[:2]:
                send(s, role, (last,))
        load_ffn(role)

    by_role(begin)
    with jax.named_scope("loads"):
        by_role(wait_loads)
        for copy in small:
            copy.wait()

    def norm(buffer, at, gain):
        count = at.size
        squares = jnp.zeros((count, 1), jnp.float32)
        for b in range(n_tp):
            values = buffer[b, at, :].astype(jnp.float32)
            squares = squares + jnp.sum(values * values, axis=-1, keepdims=True)
        scale = lax.rsqrt(squares / (n_tp * own_cols) + 1e-06)
        for b in range(n_tp):
            cut = slice(b * own_cols, (b + 1) * own_cols)
            values = buffer[b, at, :].astype(jnp.float32)
            normed[at, cut] = (values * scale * gain[:, cut]).astype(jnp.bfloat16)

    with jax.named_scope("tok_mid"):
        all_middle(tok, 0, mine)
    def take_tok(h):
        with jax.named_scope("tok_swap"):
            tok_swap(THEIRS, h).wait_recv()
            all_begin(tok, 1 + h, held_rows(THEIRS, h))

    def pass_tok(h):
        with jax.named_scope("tok_theirs"):
            all_middle(tok, 1 + h, held_rows(THEIRS, h))

    def early(role):
        if role == END:
            with jax.named_scope("relay_mix"):
                relay(mix, role, 1)
            take_tok(0)
            with jax.named_scope("norm_mine"):
                all_end(tok, 0, mine)
                norm(tok, mine, mix_gain)
            with jax.named_scope("relay_mix"):
                relay(mix, role, 2)
            pass_tok(0)
            for h in halves[1:]:
                take_tok(h)
            with jax.named_scope("relay_mix"):
                relay(mix, role, last)
            for h in halves[1:]:
                pass_tok(h)
            return
        with jax.named_scope("relay_mix"):
            relay(mix, role, 1)
        with jax.named_scope("relay_mix"):
            ahead(mix)
        send(ins[0], role, (1, 2))
        take_tok(0)
        with jax.named_scope("norm_mine"):
            all_end(tok, 0, mine)
            norm(tok, mine, mix_gain)
        for h in halves[1:]:
            take_tok(h)
        pass_tok(0)
        with jax.named_scope("relay_mix"):
            relay(mix, role, 2)
        for s in ins[:3]:
            send(s, role, (last,))
        with jax.named_scope("ahead0"):
            ahead(ins[0])
            send(ins[1], role, (1, 2))
        for h in halves[1:]:
            pass_tok(h)

    by_role(early)
    with jax.named_scope("norm_theirs"):
        for h in halves:
            all_end(tok, 1 + h, held_rows(THEIRS, h))
        norm(tok, theirs, mix_gain)
    with jax.named_scope("arrived_mix"):
        arrived(mix, INNER)

    taps = [mix_taps[i : i + 1, at_chans] for i in range(3)]

    def mix_core_copy(o, dx):
        there = lax.rem(x + dx, n_x)
        return to_tp(
            part_mix.at[o, there * 2 + 1 - c],
            mix_core.at[o, there],
            mix_core_send.at[0],
            mix_core_recv.at[o],
            core,
        )

    def mix_core_wait(o):
        view = part_mix.at[o, pl.ds(0, n_x)]
        to_tp(view, mix_core.at[o], mix_core_send.at[0], mix_core_recv.at[o], core).wait_recv()

    def mix_x_copy(o, h, dx):
        to = lax.rem(x + dx, n_x) * 2 + c
        return to_tp(
            mix_x_sum.at[o, h, dx - 1],
            mix_x_got.at[o, h, dx - 1],
            mix_x_send.at[0],
            mix_x_recv.at[o, h, dx - 1],
            to,
        )

    def mix_chip_sum(o, h, dx):
        there = lax.rem(x + dx, n_x)
        cut = in_half(h)
        near = part_mix[o, there * 2 + c, cut, :].astype(jnp.float32)
        return near + mix_core[o, there, cut, :].astype(jnp.float32)

    def mix_place_sum(o, h):
        value = mix_chip_sum(o, h, 0)
        for dx in range(1, n_x):
            value = value + mix_x_got[o, h, dx - 1].astype(jnp.float32)
        return value

    with jax.named_scope("mixer"):
        for o, at in ((THEIRS, theirs), (MINE, mine)):
            both = jnp.dot(normed[at, :], mix_in[...], preferred_element_type=jnp.float32)
            both = both.astype(jnp.bfloat16).astype(jnp.float32)
            gated = both[:, 2 * unit_chans :] * both[:, :unit_chans]
            conv = conv_rows(gated, taps, length)
            mixed = (both[:, unit_chans : 2 * unit_chans] * conv).astype(jnp.bfloat16)
            for b in range(n_fs):
                terms = jnp.dot(mixed, mix_out[b], preferred_element_type=jnp.float32)
                part_mix[o, b] = terms.astype(jnp.bfloat16)
            for dx in (*range(1, n_x), 0):
                mix_core_copy(o, dx).start()

    with jax.named_scope("mix_core"):
        for o in (THEIRS, MINE):
            mix_core_wait(o)
            for dx in range(1, n_x):
                for h in halves:
                    mix_x_sum[o, h, dx - 1] = mix_chip_sum(o, h, dx).astype(jnp.bfloat16)
                    mix_x_copy(o, h, dx).start()

    def between(role):
        if role == INNER:
            with jax.named_scope("ahead1"):
                for at in (1, 2):
                    ahead(ins[at])
                    send(ins[at + 1], role, (1, 2))
        with jax.named_scope("relay_in0"):
            relay_all(ins[0], role)

    by_role(between)

    with jax.named_scope("mix_x_theirs"):
        for h in halves:
            for dx in range(1, n_x):
                mix_x_copy(THEIRS, h, dx).wait_recv()
            mix_z_sum[h] = mix_place_sum(THEIRS, h).astype(jnp.bfloat16)
            mix_swap(h).start()

    def second(role):
        if role == END:
            send(ins[2], role, (last,))
            for s in outs[:2]:
                send(s, role, (1,))
        else:
            with jax.named_scope("ahead3"):
                for at in range(3, n_in):
                    ahead(ins[at])
                    if at + 1 < n_in:
                        send(ins[at + 1], role, (1, 2))
        with jax.named_scope("relay_in1"):
            relay_all(ins[1], role)

    by_role(second)
    with jax.named_scope("mix_mine"):
        for h in halves:
            for dx in range(1, n_x):
                mix_x_copy(MINE, h, dx).wait_recv()
            mix_swap(h).wait_recv()
            mixer = mix_place_sum(MINE, h) + mix_z_got[h].astype(jnp.float32)
            at = held_rows(MINE, h)
            res[k, at, :] = (tok[k, at, :].astype(jnp.float32) + mixer).astype(jnp.bfloat16)
            res_swap(MINE, h).start()
            all_begin(res, 1 + SEQS_DEV + h, at)

    def third(role):
        for s in ins[3:]:
            send(s, role, (last,))
        for s in outs[2:] if role == END else ():
            send(s, role, (1,))
        for s in outs if role == INNER else ():
            send(s, role, (1, 2, last))
        with jax.named_scope("relay_in2"):
            relay_all(ins[2], role)

    by_role(third)
    with jax.named_scope("res_mid"):
        for h in halves:
            all_middle(res, 1 + SEQS_DEV + h, held_rows(MINE, h))
    @pl.when(jnp.logical_not(at_end))
    def _():
        with jax.named_scope("relay_in3"):
            relay_all(ins[3], INNER)

    with jax.named_scope("res_swap"):
        for h in halves:
            res_swap(THEIRS, h).wait_recv()
            all_begin(res, 1 + 2 * SEQS_DEV + h, held_rows(THEIRS, h))
    @pl.when(at_end)
    def _():
        with jax.named_scope("relay_in3"):
            relay_all(ins[3], END)

    @pl.when(jnp.logical_not(at_end))
    def _():
        for s in outs[:2]:
            relay(s, INNER, last)

    with jax.named_scope("res_norm"):
        for h in halves:
            all_end(res, 1 + SEQS_DEV + h, held_rows(MINE, h))
            norm(res, held_rows(MINE, h), ffn_gain)
    def fourth(role):
        if role == INNER:
            with jax.named_scope("relay_in4"):
                relay_all(ins[4], INNER)

    by_role(fourth)
    with jax.named_scope("res_mid2"):
        for h in halves:
            all_middle(res, 1 + 2 * SEQS_DEV + h, held_rows(THEIRS, h))
    with jax.named_scope("res_norm2"):
        for h in halves:
            all_end(res, 1 + 2 * SEQS_DEV + h, held_rows(THEIRS, h))
            norm(res, held_rows(THEIRS, h), ffn_gain)

    first_tile = jnp.where(at_end, base[END], base[INNER])

    def feed(t):
        with jax.named_scope("in_wait"):
            arrived(("in", t), INNER)
        cut = pl.ds(pl.multiple_of((first_tile + t) * LANES, LANES), LANES)
        both = jnp.dot(normed[...], ffn_in[t], preferred_element_type=jnp.float32)
        both = both.astype(jnp.bfloat16).astype(jnp.float32)
        gate_taps, value_taps = ([up_taps[i, b : b + 1, cut] for i in range(3)] for b in (0, 1))
        gate = conv_rows(both[:, :LANES], gate_taps, length) + up_bias[0:1, cut]
        value = conv_rows(both[:, LANES:], value_taps, length) + up_bias[1:2, cut]
        unit = (gate / (1.0 + jnp.exp(-gate)) * value).astype(jnp.bfloat16)
        hidden[:, pl.ds(pl.multiple_of(t * LANES, LANES), LANES)] = unit

    paced = {0: outs[:1], 2: outs[1:2], 3: outs[2:]}
    beside = {
        (INNER, 2): [(ins[5], 1), (ins[5], 2)],
        (INNER, 4): [(outs[0], 2)],
        (INNER, 5): [(outs[1], 2)],
        (END, 1): [(stage, 1) for stage in outs],
        (END, 3): [(outs[0], last)],
    }
    ready = {
        INNER: [[(outs[2], last)], [(outs[2], 2)], [(outs[3], last), (outs[3], 2)]],
        END: [[(stage, last)] for stage in outs[1:]],
    }

    @pl.loop(0, jnp.where(at_end, tiles[END], tiles[INNER]))
    def _(t):
        for at, stages in paced.items():

            @pl.when(at_end & (t == at))
            def _():
                for stage in stages:
                    send(stage, END, (2, last))

        for (role, at), relays in beside.items():
            here = at_end if role == END else jnp.logical_not(at_end)

            @pl.when(here & (t == at))
            def _():
                for stage, d in relays:
                    with jax.named_scope("relay_beside"):
                        relay(stage, role, d)

        feed(t)

    middle = n_fs // 2
    left = j < middle
    late_block = jnp.where(left, middle, middle - 1)

    def when_block(block, late):
        return pl.when(block == late_block if late else block != late_block)

    def core_copy(u, o, dx):
        there = lax.rem(x + dx, n_x)
        return to_tp(
            part_ffn.at[u, o, there * 2 + 1 - c],
            got_core.at[u, o, there],
            core_send.at[0],
            core_recv.at[u, o, dx],
            core,
        )

    def x_copy(u, o, dx):
        to = lax.rem(x + dx, n_x) * 2 + c
        straight = u == n_out - 1 and o == THEIRS
        return pltpu.make_async_remote_copy(
            src_ref=sum_x.at[u, o, dx - 1],
            dst_ref=got_x.at[u, o, dx - 1],
            send_sem=x_send.at[0],
            recv_sem=x_recv.at[u, o, dx - 1],
            device_id={"tp": to, "fs": pair} if straight else {"tp": to},
            device_id_type=MESH,
        )

    def chip_sum(u, o, dx):
        there = lax.rem(x + dx, n_x)
        mine_there = part_ffn[u, o, there * 2 + c].astype(jnp.float32)
        return mine_there + got_core[u, o, there].astype(jnp.float32)

    def place_sum(u, o):
        value = chip_sum(u, o, 0)
        for dx in range(1, n_x):
            value = value + got_x[u, o, dx - 1].astype(jnp.float32)
        return value

    def product(u, o, deep, first, count):
        at = theirs if o == THEIRS else mine
        lanes = pl.ds(pl.multiple_of(first * LANES, LANES), count * LANES)
        left_side, right_side = hidden[at, deep], ffn_out[u, deep, lanes]
        terms = jnp.dot(left_side, right_side, preferred_element_type=jnp.float32)
        for b in range(count):
            part_ffn[u, o, first + b] = terms[:, b * LANES : (b + 1) * LANES].astype(jnp.bfloat16)

    def down(u, late):
        def body(role):
            arrived_out(u, role, late)
            deep = pl.ds(0, tiles[role] * LANES)
            for o in (THEIRS, MINE):
                if late:
                    product(u, o, deep, late_block, 1)
                else:
                    product(u, o, deep, jnp.where(left, 0, middle), middle)
                    product(u, o, deep, jnp.where(left, n_fs - 1, 0), 1)

        with jax.named_scope("down_late" if late else "down"):
            by_role(body)
        for o in (THEIRS, MINE):
            for dx in (*range(1, n_x), 0):
                block = lax.rem(x + dx, n_x) * 2 + 1 - c

                @when_block(block, late)
                def _():
                    core_copy(u, o, dx).start()

    def over_x(u, late):
        for dx in range(1, n_x):

            @when_block(lax.rem(x + dx, n_x) * 2 + c, late)
            def _():
                with jax.named_scope("over_x"):
                    for o in (THEIRS, MINE):
                        core_copy(u, o, dx).wait_recv()
                        sum_x[u, o, dx - 1] = chip_sum(u, o, dx).astype(jnp.bfloat16)
                        x_copy(u, o, dx).start()

    def over_z(u, late):
        @when_block(k, late)
        def _():
            with jax.named_scope("over_z"):
                core_copy(u, THEIRS, 0).wait_recv()
                if u == n_out - 1:
                    value = chip_sum(u, THEIRS, 0)
                else:
                    for dx in range(1, n_x):
                        x_copy(u, THEIRS, dx).wait_recv()
                    value = place_sum(u, THEIRS)
                sum_z[u] = value.astype(jnp.bfloat16)
                back(u).start()

    def relay_late(u):
        with jax.named_scope("relay_late"):
            by_role(lambda role: relay(outs[u], role, late_d(role)))

    def relay_ready(i):
        def body(role):
            for stage, d in ready[role][i]:
                with jax.named_scope("relay_ready"):
                    relay(stage, role, d)

        by_role(body)

    early, late = False, True
    relay_ready(0)
    down(0, early)
    relay_ready(1)
    over_x(0, early)
    down(1, early)
    relay_ready(2)
    relay_late(0)
    over_x(1, early)
    down(2, early)
    relay_late(1)
    over_x(2, early)
    down(3, early)
    over_x(3, early)
    over_z(3, early)
    relay_late(2)
    down(0, late)
    over_x(0, late)
    over_z(0, early)
    down(1, late)
    over_x(1, late)
    relay_late(3)
    over_z(1, early)
    down(2, late)
    over_x(2, late)
    over_z(0, late)
    over_z(2, early)
    down(3, late)
    over_x(3, late)
    over_z(3, late)
    over_z(1, late)
    over_z(2, late)

    def result(u):
        cut = pl.ds(u * LANES, LANES)
        return pltpu.make_async_copy(done.at[u], out.at[:, cut], load_sem.at[u])

    with jax.named_scope("final"):
        for u in range(n_out):
            cut = slice(u * LANES, (u + 1) * LANES)
            core_copy(u, MINE, 0).wait_recv()
            for dx in range(1, n_x):
                x_copy(u, MINE, dx).wait_recv()
            value = res[k, mine, cut].astype(jnp.float32) + place_sum(u, MINE)
            back(u).wait_recv()
            value = value + got_z[u].astype(jnp.float32)
            for dx in range(1, n_x) if u == n_out - 1 else ():
                x_copy(u, THEIRS, dx).wait_recv()
                value = value + got_x[u, THEIRS, dx - 1].astype(jnp.float32)
            done[u] = value.astype(jnp.bfloat16)
            result(u).start()

    with jax.named_scope("drain"):
        for u in range(n_out):
            result(u).wait()
        def drain(role):
            for i, view in enumerate(all_sums(role, n_from)):
                to_y(view, view, y_send.at[i], y_recv.at[0]).wait_send()
            for d in range(1, n_fs):
                for i, view in enumerate(all_sums(role_of(role, d), 1)):
                    if (role, d) != (END, 2) or i == 3:
                        to_fs(view, view, z_send.at[i, d - 1], z_recv.at[0, 0], pair).wait_send()
            if role == INNER:
                for i, view in enumerate(all_sums(role, 1)[:3]):
                    to_fs(view, view, f_send.at[i], z_recv.at[0, 0], pair).wait_send()

        by_role(drain)
        for i, buffer in enumerate((tok, res)):
            view = buffer.at[pl.ds(0, n_tp - 1)]
            to_tp(view, view, all_send.at[i], all_recv.at[0, 0], core).wait_send()
        view = part_mix.at[:, pl.ds(0, n_x)]
        to_tp(view, view, mix_core_send.at[0], all_recv.at[0, 0], core).wait_send()
        to_tp(mix_x_sum, mix_x_sum, mix_x_send.at[0], all_recv.at[0, 0], core).wait_send()
        view = part_ffn.at[:, :, pl.ds(0, n_x)]
        to_tp(view, view, core_send.at[0], all_recv.at[0, 0], core).wait_send()
        to_tp(sum_x, sum_x, x_send.at[0], all_recv.at[0, 0], core).wait_send()
        view = tok.at[pl.ds(0, 2)]
        to_pair(0, view, view).wait_send()


def fused(n_fs, n_tp, *args):
    tokens, w_signal, w_gate = args[0], args[2], args[8]
    rows, cols = tokens.shape
    shard, chans = w_signal.shape
    n_in, n_out = tiles_of(w_gate.shape[1] // LANES, INNER), shard // LANES
    units = n_in * LANES
    width = n_fs * shard
    args = list(args)
    args[1], args[7] = args[1].reshape(1, -1), args[7].reshape(1, -1)
    args[10] = args[10].transpose(1, 0, 2)
    small = [pltpu.VMEM(args[i].shape, jnp.float32) for i in (1, 5, 7, 10, 11)]
    n_x = n_tp // 2
    length = rows // SEQS_DEV
    dma = pltpu.SemaphoreType.DMA

    def held(*shape):
        return pltpu.VMEM(shape, jnp.bfloat16)

    return pl.pallas_call(
        functools.partial(layer_kernel, n_fs, n_tp),
        out_shape=jax.ShapeDtypeStruct((rows, cols), jnp.bfloat16),
        in_specs=[pl.BlockSpec(memory_space=pl.ANY)] * len(args),
        out_specs=pl.BlockSpec(memory_space=pl.ANY),
        scratch_shapes=[
            *small,
            held(width, 3 * (chans // 2)),
            held(n_fs, chans // 2, shard),
            held(n_in, width, 2 * LANES),
            held(n_out, units, n_fs * LANES),
            held(n_tp, 2 * rows, cols),
            held(n_tp, 2 * rows, cols),
            held(2 * rows, width),
            held(2 * rows, units),
            held(2, n_tp, rows, cols),
            held(2, n_x, rows, cols),
            held(2, SEQS_DEV, n_x - 1, length, cols),
            held(2, SEQS_DEV, n_x - 1, length, cols),
            held(SEQS_DEV, length, cols),
            held(SEQS_DEV, length, cols),
            held(n_out, 2, n_tp, rows, LANES),
            held(n_out, 2, n_x, rows, LANES),
            held(n_out, 2, n_x - 1, rows, LANES),
            held(n_out, 2, n_x - 1, rows, LANES),
            held(n_out, rows, LANES),
            held(n_out, rows, LANES),
            held(n_out, rows, LANES),
            dma((4, n_fs - 1)),
            dma((2 + n_in + n_out, n_fs - 1)),
            dma((4,)),
            dma((4,)),
            dma((2 + n_in + 2 * n_out,)),
            dma((10,)),
            dma((2,)),
            dma((1 + 3 * SEQS_DEV, n_x)),
            dma((1,)),
            dma((2,)),
            dma((1,)),
            dma((2, SEQS_DEV, n_x - 1)),
            dma((1,)),
            dma((n_out, 2, n_x)),
            dma((1,)),
            dma((n_out, 2, n_x - 1)),
            dma((1,)),
            dma((3 * SEQS_DEV + n_out,)),
        ],
        compiler_params=pltpu.CompilerParams(
            collective_id=0, has_side_effects=True, vmem_limit_bytes=62 * 1024 * 1024
        ),
    )(*args)


def solution(mesh):
    n_fs, n_tp = mesh.shape["fs"], mesh.shape["tp"]
    body = functools.partial(fused, n_fs, n_tp)
    if n_fs != 4 or n_tp != 4 or mesh.shape["grp"] != 2:
        body = on_device
    placed = (
        P(("grp", "fs"), "tp"),
        P(),
        P("fs", "tp"),
        P("fs", "tp"),
        P("fs", "tp"),
        P(None, "tp"),
        P("tp", "fs"),
        P(),
        P("fs", "tp"),
        P("fs", "tp"),
        P(None, None, "tp"),
        P(None, "tp"),
        P("tp", "fs"),
    )
    return jax.shard_map(
        body, mesh=mesh, in_specs=placed, out_specs=P(("grp", "fs"), "tp"), check_vma=False
    )
```

```python
import functools

import jax
import jax.numpy as jnp
from jax import lax
from jax.experimental import pallas as pl
from jax.experimental.pallas import tpu as pltpu
from jax.sharding import PartitionSpec as P

SEQS_DEV = 2


def conv_positions(values, taps):
    width = values.shape[1]
    blocks = values.reshape(SEQS_DEV, -1, width)
    length = blocks.shape[1]
    padded = jnp.pad(blocks, ((0, 0), (2, 0), (0, 0)))
    result = (
        padded[:, 0:length] * taps[0]
        + padded[:, 1 : length + 1] * taps[1]
        + padded[:, 2 : length + 2] * taps[2]
    )
    return result.reshape(-1, width)


def rms_norm(stream, gain):
    values = stream.astype(jnp.float32)
    scale = lax.rsqrt(jnp.mean(values * values, axis=-1, keepdims=True) + 1e-06)
    return (values * scale * gain).astype(jnp.bfloat16)


def on_device(
    tokens,
    mix_gain,
    w_signal,
    w_outer_gate,
    w_inner_gate,
    mix_taps,
    w_mix_out,
    ffn_gain,
    w_gate,
    w_value,
    up_taps,
    up_bias,
    w_down,
):
    whole = lax.all_gather(tokens, "tp", axis=1, tiled=True)
    normed = rms_norm(whole, mix_gain)
    pieces = (
        lax.all_gather(w_signal, "fs", axis=0, tiled=True),
        lax.all_gather(w_outer_gate, "fs", axis=0, tiled=True),
        lax.all_gather(w_inner_gate, "fs", axis=0, tiled=True),
    )
    columns = normed
    signal, outer, inner = tuple(
        (jnp.dot(columns, piece, preferred_element_type=jnp.float32) for piece in pieces)
    )
    signal = signal.astype(jnp.bfloat16).astype(jnp.float32)
    outer = outer.astype(jnp.bfloat16).astype(jnp.float32)
    inner = inner.astype(jnp.bfloat16).astype(jnp.float32)
    mixed = (outer * conv_positions(inner * signal, mix_taps)).astype(jnp.bfloat16)
    mix_terms = jnp.dot(
        mixed,
        lax.all_gather(w_mix_out, "fs", axis=1, tiled=True),
        preferred_element_type=jnp.float32,
    )
    mix_sum = lax.psum_scatter(
        mix_terms.astype(jnp.bfloat16), "tp", scatter_dimension=1, tiled=True
    ).astype(jnp.float32)
    resid = (tokens.astype(jnp.float32) + mix_sum).astype(jnp.bfloat16)
    whole_ffn = lax.all_gather(resid, "tp", axis=1, tiled=True)
    normed_ffn = rms_norm(whole_ffn, ffn_gain)
    pieces = (
        lax.all_gather(w_gate, "fs", axis=0, tiled=True),
        lax.all_gather(w_value, "fs", axis=0, tiled=True),
    )
    columns = normed_ffn
    gate = jnp.dot(columns, pieces[0], preferred_element_type=jnp.float32)
    value = jnp.dot(columns, pieces[1], preferred_element_type=jnp.float32)
    gate = gate.astype(jnp.bfloat16).astype(jnp.float32)
    value = value.astype(jnp.bfloat16).astype(jnp.float32)
    gate_conv = conv_positions(gate, up_taps[0]) + up_bias[0]
    value_conv = conv_positions(value, up_taps[1]) + up_bias[1]
    hidden = (jax.nn.silu(gate_conv) * value_conv).astype(jnp.bfloat16)
    ffn_terms = jnp.dot(
        hidden, lax.all_gather(w_down, "fs", axis=1, tiled=True), preferred_element_type=jnp.float32
    )
    ffn_sum = lax.psum_scatter(
        ffn_terms.astype(jnp.bfloat16), "tp", scatter_dimension=1, tiled=True
    ).astype(jnp.float32)
    return (resid.astype(jnp.float32) + ffn_sum).astype(jnp.bfloat16)


MESH = pl.DeviceIdType.MESH
UP, DOWN = 0, 1
LANES = 128


def shifted(values, by, length):
    rolled = pltpu.roll(values, by, 0)
    position = lax.rem(lax.broadcasted_iota(jnp.int32, values.shape, 0), length)
    return jnp.where(position < by, 0.0, rolled)


def conv_rows(values, taps, length):
    return (
        shifted(values, 2, length) * taps[0]
        + shifted(values, 1, length) * taps[1]
        + values * taps[2]
    )


END, INNER = 0, 1


def tiles_of(n_tiles, role):
    at_end = 2 * n_tiles // 5
    return at_end if role == END else n_tiles - at_end


def layer_kernel(
    n_fs,
    n_tp,
    tokens,
    mix_gain_given,
    w_signal,
    w_outer_gate,
    w_inner_gate,
    mix_taps_given,
    w_mix_out,
    ffn_gain_given,
    w_gate,
    w_value,
    up_taps_given,
    up_bias_given,
    w_down,
    out,
    mix_gain,
    mix_taps,
    ffn_gain,
    up_taps,
    up_bias,
    mix_in,
    mix_out,
    ffn_in,
    ffn_out,
    tok,
    res,
    normed,
    hidden,
    part_mix,
    mix_core,
    mix_x_sum,
    mix_x_got,
    mix_z_sum,
    mix_z_got,
    part_ffn,
    got_core,
    sum_x,
    got_x,
    sum_z,
    got_z,
    done,
    z_send,
    z_recv,
    f_send,
    y_send,
    y_recv,
    load_sem,
    all_send,
    all_recv,
    mix_core_send,
    mix_core_recv,
    mix_x_send,
    mix_x_recv,
    core_send,
    core_recv,
    x_send,
    x_recv,
    pair_send,
    pair_recv,
):
    g, j, k = lax.axis_index("grp"), lax.axis_index("fs"), lax.axis_index("tp")
    rows, own_cols = tokens.shape
    length = rows // SEQS_DEV
    shard, chans = w_signal.shape
    half, unit_chans = shard // 2, chans // 2
    n_tiles, n_out = w_gate.shape[1] // LANES, shard // LANES
    tiles = {END: tiles_of(n_tiles, END), INNER: tiles_of(n_tiles, INNER)}
    base = {END: 0, INNER: tiles[END]}
    n_x = n_tp // 2
    x, c = k // 2, lax.rem(k, 2)
    core = k + 1 - 2 * c
    p = lax.rem(j, 2)
    pair = j + 1 - 2 * p
    inward = jnp.where(j < n_fs // 2, 1, n_fs - 1)
    at_end = (j == 0) | (j == n_fs - 1)

    MINE, THEIRS = 0, 1

    def held_rows(o, h=None):
        side = p if o == MINE else 1 - p
        if h is None:
            return pl.ds(pl.multiple_of(side * rows, rows), rows)
        return pl.ds(pl.multiple_of(side * rows + h * length, length), length)

    def in_half(h):
        return slice(h * length, (h + 1) * length)

    mix = ("mix", 0)
    n_in = tiles[INNER]
    ins = [("in", t) for t in range(n_in)]
    outs = [("out", u) for u in range(n_out)]

    def by_role(body):
        pl.when(at_end)(functools.partial(body, END))
        pl.when(jnp.logical_not(at_end))(functools.partial(body, INNER))


    def other(d):
        return lax.rem(j + inward * d, n_fs)

    def sources(stage, role, side):
        kind, i = stage
        at_rows = pl.ds(pl.multiple_of(side * half, half), half)
        if kind == "mix":
            lanes = pl.ds(role * unit_chans, unit_chans)
            tall = unit_chans // 2
            at = pl.ds(pl.multiple_of(role * unit_chans + side * tall, tall), tall)
            refs = [ref.at[at_rows, lanes] for ref in (w_signal, w_outer_gate, w_inner_gate)]
            return [*refs, w_mix_out.at[at, :]]
        if kind == "in":
            lanes = pl.ds((base[role] + i) * LANES, LANES)
            return [w_gate.at[at_rows, lanes], w_value.at[at_rows, lanes]]
        tall = tiles[role] * LANES // 2
        at = pl.ds(pl.multiple_of(base[role] * LANES + side * tall, LANES), tall)
        return [w_down.at[at, pl.ds(i * LANES, LANES)]]

    def places(stage, role, source, side, whole):
        kind, i = stage
        at_rows = pl.ds(pl.multiple_of((source * 2 + side) * half, half), half)
        if kind == "mix":
            tall = unit_chans // 2
            at = pl.ds(pl.multiple_of(side * tall, tall), tall)
            outs = mix_out.at[source, at, :]
            if whole:
                return [mix_in.at[at_rows, :], outs]
            lanes = [pl.ds(b * unit_chans, unit_chans) for b in range(3)]
            return [*(mix_in.at[at_rows, lane] for lane in lanes), outs]
        if kind == "in":
            if whole:
                return [ffn_in.at[i, at_rows, :]]
            return [ffn_in.at[i, at_rows, pl.ds(b * LANES, LANES)] for b in (0, 1)]
        tall = tiles[role] * LANES // 2
        at = pl.ds(pl.multiple_of(side * tall, LANES), tall)
        lanes = pl.ds(pl.multiple_of(source * LANES, LANES), LANES)
        return [ffn_out.at[i, at, lanes]]

    def slot(stage, i):
        kind, at = stage
        if kind == "mix":
            return i
        return 2 + at if kind == "in" else 2 + n_in + at

    def group(stage, i):
        kind, _ = stage
        return i if kind == "mix" else {"in": 2, "out": 3}[kind]

    def to_fs(src, dst, send_sem, recv_sem, to):
        return pltpu.make_async_remote_copy(
            src_ref=src,
            dst_ref=dst,
            send_sem=send_sem,
            recv_sem=recv_sem,
            device_id={"fs": to},
            device_id_type=MESH,
        )

    def role_of(role, d):
        return INNER if d < n_fs - 1 - role else END

    def z_sends(s, role, d):
        to = other(d)
        there = role_of(role, d)
        pairs = zip(sources(s, there, g), places(s, there, j, g, False))
        copies = []
        for i, (src, dst) in enumerate(pairs):
            wide = i // 3 if s[0] == "mix" else 0
            sems = z_send.at[group(s, wide), d - 1], z_sem(s, wide, j, to)
            copies.append(to_fs(src, dst, *sems, to))
        return copies

    def z_takes(s, role, d):
        source = other(d)
        return [
            to_fs(view, view, z_send.at[group(s, i), 0], z_sem(s, i, source, j), source)
            for i, view in enumerate(places(s, role, source, g, True))
        ]

    def z_forwards(s):
        source = other(last)
        to = other(1)
        return [
            to_fs(view, view, f_send.at[group(s, i)], z_sem(s, i, source, to), to)
            for i, view in enumerate(places(s, INNER, source, g, True))
        ]

    def z_sem(s, i, source, to):
        return z_recv.at[slot(s, i), lax.rem(source - to + n_fs, n_fs) - 1]

    def to_y(src, dst, send_sem, recv_sem):
        return pltpu.make_async_remote_copy(
            src_ref=src,
            dst_ref=dst,
            send_sem=send_sem,
            recv_sem=recv_sem,
            device_id={"grp": 1 - g},
            device_id_type=MESH,
        )

    def late_d(role):
        return 1 if role == INNER else 2

    def y_copies(s, role, d):
        after = n_out if s[0] == "out" and d == late_d(role) else 0
        return [
            to_y(view, view, y_send.at[group(s, i)], y_recv.at[slot(s, i) + after])
            for i, view in enumerate(places(s, role, other(d), g, True))
        ]

    n_from = n_fs - 1

    def sums(stage, role, count):
        kind, i = stage
        if kind == "mix":
            some = mix_out.at[pl.ds(0, count), pl.ds(0, unit_chans // 2), :]
            return [mix_in.at[pl.ds(0, count * half), :], some]
        if kind == "in":
            return [ffn_in.at[i, pl.ds(0, count * half), :]]
        return [ffn_out.at[i, pl.ds(0, tiles[role] * LANES // 2), pl.ds(0, count * LANES)]]

    def all_sums(role, count):
        return [
            *sums(mix, role, count),
            *sums(("in", pl.ds(0, tiles[role])), role, count),
            *sums(("out", pl.ds(0, n_out)), role, count),
        ]

    def start(copies):
        for copy in copies:
            copy.start()

    def wait_recv(copies):
        for copy in copies:
            copy.wait_recv()

    def wait_send(copies):
        for copy in copies:
            copy.wait_send()

    def send(s, role, ds):
        for d in ds:
            if s[0] != "in" or s[1] < tiles[role_of(role, d)]:
                start(z_sends(s, role, d))

    last = n_fs - 1

    def relay(s, role, d):
        wait_recv(z_takes(s, role, d))
        start(y_copies(s, role, d))

    def ahead(s):
        relay(s, INNER, last)
        start(z_forwards(s))

    def relay_all(s, role):
        if s[0] == "in" and s[1] >= tiles[role]:
            return
        for d in (1, 2, last) if role == END else (1, 2):
            relay(s, role, d)

    def relay_both(s):
        by_role(lambda role: relay_all(s, role))

    def arrived(s, role):
        for i, view in enumerate(sums(s, role, n_from)):
            to_y(view, view, y_send.at[group(s, i)], y_recv.at[slot(s, i)]).wait_recv()

    def arrived_out(u, role, late):
        s = outs[u]
        (view,) = sums(s, role, 1 if late else n_from - 1)
        at = slot(s, 0) + (n_out if late else 0)
        to_y(view, view, y_send.at[group(s, 0)], y_recv.at[at]).wait_recv()

    def to_tp(src, dst, send_sem, recv_sem, to):
        return pltpu.make_async_remote_copy(
            src_ref=src,
            dst_ref=dst,
            send_sem=send_sem,
            recv_sem=recv_sem,
            device_id={"tp": to},
            device_id_type=MESH,
        )

    def all_copies(buffer, i, at, kind):
        sent = all_send.at[0 if i <= SEQS_DEV else 1]
        copies = []
        for dx in range(n_x):
            there = lax.rem(x + dx, n_x)
            if kind == "over":
                if dx:
                    view = buffer.at[k, at]
                    copies.append(to_tp(view, view, sent, all_recv.at[i, dx - 1], there * 2 + c))
            else:
                back = lax.rem(x + n_x - dx, n_x) * 2
                seen = back + c if kind == "pass" else back + 1 - c
                view = buffer.at[seen, at]
                copies.append(to_tp(view, view, sent, all_recv.at[i, n_x - 1], core))
        return copies

    def all_begin(buffer, i, at):
        start(all_copies(buffer, i, at, "over"))
        all_copies(buffer, i, at, "pass")[0].start()

    def all_middle(buffer, i, at):
        passed = all_copies(buffer, i, at, "pass")
        for dx in range(1, n_x):
            view = buffer.at[lax.rem(x + n_x - dx, n_x) * 2 + c, at]
            sent = all_send.at[0 if i <= SEQS_DEV else 1]
            to_tp(view, view, sent, all_recv.at[i, dx - 1], core).wait_recv()
            passed[dx].start()

    def all_end(buffer, i, at):
        view = buffer.at[pl.ds(0, n_x), at]
        to_tp(view, view, all_send.at[0], all_recv.at[i, n_x - 1], core).wait_recv()

    def to_pair(i, src, dst):
        return pltpu.make_async_remote_copy(
            src_ref=src,
            dst_ref=dst,
            send_sem=pair_send.at[0],
            recv_sem=pair_recv.at[i],
            device_id={"fs": pair},
            device_id_type=MESH,
        )

    halves = range(SEQS_DEV)
    mine, theirs = held_rows(MINE), held_rows(THEIRS)

    def tok_swap(o, h):
        view = tok.at[k, held_rows(o, h)]
        return to_pair(h, view, view)

    def res_swap(o, h):
        view = res.at[k, held_rows(o, h)]
        return to_pair(SEQS_DEV + h, view, view)

    def mix_swap(h):
        return to_pair(2 * SEQS_DEV + h, mix_z_sum.at[h], mix_z_got.at[h])

    def back(u):
        return to_pair(3 * SEQS_DEV + u, sum_z.at[u], got_z.at[u])

    barrier = pltpu.get_barrier_semaphore()
    for d in range(1, n_fs):
        to = lax.rem(j + d, n_fs)
        pl.semaphore_signal(barrier, inc=1, device_id={"fs": to}, device_id_type=MESH)
    pl.semaphore_signal(barrier, inc=1, device_id={"grp": 1 - g}, device_id_type=MESH)
    for d in range(1, n_tp):
        to = lax.rem(k + d, n_tp)
        pl.semaphore_signal(barrier, inc=1, device_id={"tp": to}, device_id_type=MESH)
    for dx in range(1, n_x):
        far = {"tp": lax.rem(x + dx, n_x) * 2 + c, "fs": pair}
        pl.semaphore_signal(barrier, inc=1, device_id=far, device_id_type=MESH)

    first = pltpu.make_async_copy(tokens, tok.at[k, mine], load_sem.at[4])
    own_rows = pl.ds(pl.multiple_of(j * shard, shard), shard)
    own_lanes = pl.ds(pl.multiple_of(j * LANES, LANES), LANES)
    inner_role = jnp.where(at_end, END, INNER)
    at_chans = pl.ds(pl.multiple_of(inner_role * unit_chans, unit_chans), unit_chans)

    def load(i, src, dst):
        pltpu.make_async_copy(src, dst, load_sem.at[i]).start()

    first.start()
    small = [
        pltpu.make_async_copy(src, dst, load_sem.at[5 + i])
        for i, (src, dst) in enumerate(
            (
                (mix_gain_given, mix_gain),
                (mix_taps_given, mix_taps),
                (ffn_gain_given, ffn_gain),
                (up_taps_given, up_taps),
                (up_bias_given, up_bias),
            )
        )
    ]
    for copy in small:
        copy.start()
    for i, ref in enumerate((w_signal, w_outer_gate, w_inner_gate)):
        load(0, ref.at[:, at_chans], mix_in.at[own_rows, pl.ds(i * unit_chans, unit_chans)])
    load(1, w_mix_out.at[at_chans, :], mix_out.at[j])
    def load_ffn(role):
        for t in range(tiles[role]):
            for i, src in enumerate((w_gate, w_value)):
                lanes = pl.ds((base[role] + t) * LANES, LANES)
                load(2, src.at[:, lanes], ffn_in.at[t, own_rows, pl.ds(i * LANES, LANES)])
        tall = tiles[role] * LANES
        for u in range(n_out):
            src = w_down.at[pl.ds(base[role] * LANES, tall), pl.ds(u * LANES, LANES)]
            load(3, src, ffn_out.at[u, pl.ds(0, tall), own_lanes])

    def wait_loads(role):
        views = [
            mix_in.at[own_rows, :],
            mix_out.at[j],
            ffn_in.at[pl.ds(0, tiles[role]), own_rows, :],
            ffn_out.at[:, pl.ds(0, tiles[role] * LANES), own_lanes],
        ]
        for i, view in enumerate(views):
            pltpu.make_async_copy(view, view, load_sem.at[i]).wait()

    with jax.named_scope("barrier"):
        first.wait()
        pl.semaphore_wait(barrier, n_fs - 1 + 1 + n_tp - 1 + n_x - 1)

    def begin(role):
        send(mix, role, (1, last) if role == END else (last, 1))
        tok_swap(MINE, 0).start()
        all_begin(tok, 0, mine)
        if role == INNER:
            send(mix, role, (2,))
        for h in halves[1:]:
            tok_swap(MINE, h).start()
        if role == END:
            for s in ins:
                send(s, role, (1,))
            for s in ins[:2]:
                send(s, role, (last,))
        load_ffn(role)

    by_role(begin)
    with jax.named_scope("loads"):
        by_role(wait_loads)
        for copy in small:
            copy.wait()

    def norm(buffer, at, gain):
        count = at.size
        squares = jnp.zeros((count, 1), jnp.float32)
        for b in range(n_tp):
            values = buffer[b, at, :].astype(jnp.float32)
            squares = squares + jnp.sum(values * values, axis=-1, keepdims=True)
        scale = lax.rsqrt(squares / (n_tp * own_cols) + 1e-06)
        for b in range(n_tp):
            cut = slice(b * own_cols, (b + 1) * own_cols)
            values = buffer[b, at, :].astype(jnp.float32)
            normed[at, cut] = (values * scale * gain[:, cut]).astype(jnp.bfloat16)

    with jax.named_scope("tok_mid"):
        all_middle(tok, 0, mine)
    def take_tok(h):
        with jax.named_scope("tok_swap"):
            tok_swap(THEIRS, h).wait_recv()
            all_begin(tok, 1 + h, held_rows(THEIRS, h))

    def pass_tok(h):
        with jax.named_scope("tok_theirs"):
            all_middle(tok, 1 + h, held_rows(THEIRS, h))

    def early(role):
        if role == END:
            with jax.named_scope("relay_mix"):
                relay(mix, role, 1)
            take_tok(0)
            with jax.named_scope("norm_mine"):
                all_end(tok, 0, mine)
                norm(tok, mine, mix_gain)
            with jax.named_scope("relay_mix"):
                relay(mix, role, 2)
            pass_tok(0)
            for h in halves[1:]:
                take_tok(h)
            with jax.named_scope("relay_mix"):
                relay(mix, role, last)
            for h in halves[1:]:
                pass_tok(h)
            return
        with jax.named_scope("relay_mix"):
            relay(mix, role, 1)
        with jax.named_scope("relay_mix"):
            ahead(mix)
        send(ins[0], role, (1, 2))
        take_tok(0)
        with jax.named_scope("norm_mine"):
            all_end(tok, 0, mine)
            norm(tok, mine, mix_gain)
        for h in halves[1:]:
            take_tok(h)
        pass_tok(0)
        with jax.named_scope("relay_mix"):
            relay(mix, role, 2)
        for s in ins[:3]:
            send(s, role, (last,))
        with jax.named_scope("ahead0"):
            ahead(ins[0])
            send(ins[1], role, (1, 2))
        for h in halves[1:]:
            pass_tok(h)

    by_role(early)
    with jax.named_scope("norm_theirs"):
        for h in halves:
            all_end(tok, 1 + h, held_rows(THEIRS, h))
        norm(tok, theirs, mix_gain)
    with jax.named_scope("arrived_mix"):
        arrived(mix, INNER)

    taps = [mix_taps[i : i + 1, at_chans] for i in range(3)]

    def mix_core_copy(o, dx):
        there = lax.rem(x + dx, n_x)
        return to_tp(
            part_mix.at[o, there * 2 + 1 - c],
            mix_core.at[o, there],
            mix_core_send.at[0],
            mix_core_recv.at[o],
            core,
        )

    def mix_core_wait(o):
        view = part_mix.at[o, pl.ds(0, n_x)]
        to_tp(view, mix_core.at[o], mix_core_send.at[0], mix_core_recv.at[o], core).wait_recv()

    def mix_x_copy(o, h, dx):
        to = lax.rem(x + dx, n_x) * 2 + c
        return to_tp(
            mix_x_sum.at[o, h, dx - 1],
            mix_x_got.at[o, h, dx - 1],
            mix_x_send.at[0],
            mix_x_recv.at[o, h, dx - 1],
            to,
        )

    def mix_chip_sum(o, h, dx):
        there = lax.rem(x + dx, n_x)
        cut = in_half(h)
        near = part_mix[o, there * 2 + c, cut, :].astype(jnp.float32)
        return near + mix_core[o, there, cut, :].astype(jnp.float32)

    def mix_place_sum(o, h):
        value = mix_chip_sum(o, h, 0)
        for dx in range(1, n_x):
            value = value + mix_x_got[o, h, dx - 1].astype(jnp.float32)
        return value

    with jax.named_scope("mixer"):
        for o, at in ((THEIRS, theirs), (MINE, mine)):
            both = jnp.dot(normed[at, :], mix_in[...], preferred_element_type=jnp.float32)
            both = both.astype(jnp.bfloat16).astype(jnp.float32)
            gated = both[:, 2 * unit_chans :] * both[:, :unit_chans]
            conv = conv_rows(gated, taps, length)
            mixed = (both[:, unit_chans : 2 * unit_chans] * conv).astype(jnp.bfloat16)
            for b in range(n_fs):
                terms = jnp.dot(mixed, mix_out[b], preferred_element_type=jnp.float32)
                part_mix[o, b] = terms.astype(jnp.bfloat16)
            for dx in (*range(1, n_x), 0):
                mix_core_copy(o, dx).start()

    with jax.named_scope("mix_core"):
        for o in (THEIRS, MINE):
            mix_core_wait(o)
            for dx in range(1, n_x):
                for h in halves:
                    mix_x_sum[o, h, dx - 1] = mix_chip_sum(o, h, dx).astype(jnp.bfloat16)
                    mix_x_copy(o, h, dx).start()

    def between(role):
        if role == INNER:
            with jax.named_scope("ahead1"):
                for at in (1, 2):
                    ahead(ins[at])
                    send(ins[at + 1], role, (1, 2))
        with jax.named_scope("relay_in0"):
            relay_all(ins[0], role)

    by_role(between)

    with jax.named_scope("mix_x_theirs"):
        for h in halves:
            for dx in range(1, n_x):
                mix_x_copy(THEIRS, h, dx).wait_recv()
            mix_z_sum[h] = mix_place_sum(THEIRS, h).astype(jnp.bfloat16)
            mix_swap(h).start()

    def second(role):
        if role == END:
            send(ins[2], role, (last,))
            for s in outs[:2]:
                send(s, role, (1,))
        else:
            with jax.named_scope("ahead3"):
                for at in range(3, n_in):
                    ahead(ins[at])
                    if at + 1 < n_in:
                        send(ins[at + 1], role, (1, 2))
        with jax.named_scope("relay_in1"):
            relay_all(ins[1], role)

    by_role(second)
    with jax.named_scope("mix_mine"):
        for h in halves:
            for dx in range(1, n_x):
                mix_x_copy(MINE, h, dx).wait_recv()
            mix_swap(h).wait_recv()
            mixer = mix_place_sum(MINE, h) + mix_z_got[h].astype(jnp.float32)
            at = held_rows(MINE, h)
            res[k, at, :] = (tok[k, at, :].astype(jnp.float32) + mixer).astype(jnp.bfloat16)
            res_swap(MINE, h).start()
            all_begin(res, 1 + SEQS_DEV + h, at)

    def third(role):
        for s in ins[3:]:
            send(s, role, (last,))
        for s in outs[2:] if role == END else ():
            send(s, role, (1,))
        for s in outs if role == INNER else ():
            send(s, role, (1, 2, last))
        with jax.named_scope("relay_in2"):
            relay_all(ins[2], role)

    by_role(third)
    with jax.named_scope("res_mid"):
        for h in halves:
            all_middle(res, 1 + SEQS_DEV + h, held_rows(MINE, h))
    @pl.when(jnp.logical_not(at_end))
    def _():
        with jax.named_scope("relay_in3"):
            relay_all(ins[3], INNER)

    with jax.named_scope("res_swap"):
        for h in halves:
            res_swap(THEIRS, h).wait_recv()
            all_begin(res, 1 + 2 * SEQS_DEV + h, held_rows(THEIRS, h))
    @pl.when(at_end)
    def _():
        with jax.named_scope("relay_in3"):
            relay_all(ins[3], END)

    @pl.when(jnp.logical_not(at_end))
    def _():
        for s in outs[:2]:
            relay(s, INNER, last)

    with jax.named_scope("res_norm"):
        for h in halves:
            all_end(res, 1 + SEQS_DEV + h, held_rows(MINE, h))
            norm(res, held_rows(MINE, h), ffn_gain)
    def fourth(role):
        if role == INNER:
            with jax.named_scope("relay_in4"):
                relay_all(ins[4], INNER)

    by_role(fourth)
    with jax.named_scope("res_mid2"):
        for h in halves:
            all_middle(res, 1 + 2 * SEQS_DEV + h, held_rows(THEIRS, h))
    with jax.named_scope("res_norm2"):
        for h in halves:
            all_end(res, 1 + 2 * SEQS_DEV + h, held_rows(THEIRS, h))
            norm(res, held_rows(THEIRS, h), ffn_gain)

    first_tile = jnp.where(at_end, base[END], base[INNER])

    def feed(t):
        with jax.named_scope("in_wait"):
            arrived(("in", t), INNER)
        cut = pl.ds(pl.multiple_of((first_tile + t) * LANES, LANES), LANES)
        both = jnp.dot(normed[...], ffn_in[t], preferred_element_type=jnp.float32)
        both = both.astype(jnp.bfloat16).astype(jnp.float32)
        gate_taps, value_taps = ([up_taps[i, b : b + 1, cut] for i in range(3)] for b in (0, 1))
        gate = conv_rows(both[:, :LANES], gate_taps, length) + up_bias[0:1, cut]
        value = conv_rows(both[:, LANES:], value_taps, length) + up_bias[1:2, cut]
        unit = (gate / (1.0 + jnp.exp(-gate)) * value).astype(jnp.bfloat16)
        hidden[:, pl.ds(pl.multiple_of(t * LANES, LANES), LANES)] = unit

    paced = {1: outs[:1], 2: outs[1:2], 3: outs[2:]}
    beside = {
        (INNER, 2): [(ins[5], 1), (ins[5], 2)],
        (INNER, 4): [(outs[0], 2)],
        (INNER, 5): [(outs[1], 2)],
        (END, 1): [(stage, 1) for stage in outs],
        (END, 3): [(outs[0], last)],
    }
    ready = {
        INNER: [[(outs[2], last)], [(outs[2], 2)], [(outs[3], last), (outs[3], 2)]],
        END: [[(stage, last)] for stage in outs[1:]],
    }

    @pl.loop(0, jnp.where(at_end, tiles[END], tiles[INNER]))
    def _(t):
        for at, stages in paced.items():

            @pl.when(at_end & (t == at))
            def _():
                for stage in stages:
                    send(stage, END, (2, last))

        for (role, at), relays in beside.items():
            here = at_end if role == END else jnp.logical_not(at_end)

            @pl.when(here & (t == at))
            def _():
                for stage, d in relays:
                    with jax.named_scope("relay_beside"):
                        relay(stage, role, d)

        feed(t)

    middle = n_fs // 2
    left = j < middle
    late_block = jnp.where(left, middle, middle - 1)

    def when_block(block, late):
        return pl.when(block == late_block if late else block != late_block)

    def core_copy(u, o, dx):
        there = lax.rem(x + dx, n_x)
        return to_tp(
            part_ffn.at[u, o, there * 2 + 1 - c],
            got_core.at[u, o, there],
            core_send.at[0],
            core_recv.at[u, o, dx],
            core,
        )

    def x_copy(u, o, dx):
        to = lax.rem(x + dx, n_x) * 2 + c
        straight = u == n_out - 1 and o == THEIRS
        return pltpu.make_async_remote_copy(
            src_ref=sum_x.at[u, o, dx - 1],
            dst_ref=got_x.at[u, o, dx - 1],
            send_sem=x_send.at[0],
            recv_sem=x_recv.at[u, o, dx - 1],
            device_id={"tp": to, "fs": pair} if straight else {"tp": to},
            device_id_type=MESH,
        )

    def chip_sum(u, o, dx):
        there = lax.rem(x + dx, n_x)
        mine_there = part_ffn[u, o, there * 2 + c].astype(jnp.float32)
        return mine_there + got_core[u, o, there].astype(jnp.float32)

    def place_sum(u, o):
        value = chip_sum(u, o, 0)
        for dx in range(1, n_x):
            value = value + got_x[u, o, dx - 1].astype(jnp.float32)
        return value

    def product(u, o, deep, first, count):
        at = theirs if o == THEIRS else mine
        lanes = pl.ds(pl.multiple_of(first * LANES, LANES), count * LANES)
        left_side, right_side = hidden[at, deep], ffn_out[u, deep, lanes]
        terms = jnp.dot(left_side, right_side, preferred_element_type=jnp.float32)
        for b in range(count):
            part_ffn[u, o, first + b] = terms[:, b * LANES : (b + 1) * LANES].astype(jnp.bfloat16)

    def down(u, late):
        def body(role):
            arrived_out(u, role, late)
            deep = pl.ds(0, tiles[role] * LANES)
            for o in (THEIRS, MINE):
                if late:
                    product(u, o, deep, late_block, 1)
                else:
                    product(u, o, deep, jnp.where(left, 0, middle), middle)
                    product(u, o, deep, jnp.where(left, n_fs - 1, 0), 1)

        with jax.named_scope("down_late" if late else "down"):
            by_role(body)
        for o in (THEIRS, MINE):
            for dx in (*range(1, n_x), 0):
                block = lax.rem(x + dx, n_x) * 2 + 1 - c

                @when_block(block, late)
                def _():
                    core_copy(u, o, dx).start()

    def over_x(u, late):
        for dx in range(1, n_x):

            @when_block(lax.rem(x + dx, n_x) * 2 + c, late)
            def _():
                with jax.named_scope("over_x"):
                    for o in (THEIRS, MINE):
                        core_copy(u, o, dx).wait_recv()
                        sum_x[u, o, dx - 1] = chip_sum(u, o, dx).astype(jnp.bfloat16)
                        x_copy(u, o, dx).start()

    def over_z(u, late):
        @when_block(k, late)
        def _():
            with jax.named_scope("over_z"):
                core_copy(u, THEIRS, 0).wait_recv()
                if u == n_out - 1:
                    value = chip_sum(u, THEIRS, 0)
                else:
                    for dx in range(1, n_x):
                        x_copy(u, THEIRS, dx).wait_recv()
                    value = place_sum(u, THEIRS)
                sum_z[u] = value.astype(jnp.bfloat16)
                back(u).start()

    def relay_late(u):
        with jax.named_scope("relay_late"):
            by_role(lambda role: relay(outs[u], role, late_d(role)))

    def relay_ready(i):
        def body(role):
            for stage, d in ready[role][i]:
                with jax.named_scope("relay_ready"):
                    relay(stage, role, d)

        by_role(body)

    early, late = False, True
    relay_ready(0)
    down(0, early)
    relay_ready(1)
    over_x(0, early)
    down(1, early)
    relay_ready(2)
    relay_late(0)
    over_x(1, early)
    down(2, early)
    relay_late(1)
    over_x(2, early)
    down(3, early)
    over_x(3, early)
    over_z(3, early)
    relay_late(2)
    down(0, late)
    over_x(0, late)
    over_z(0, early)
    down(1, late)
    over_x(1, late)
    relay_late(3)
    over_z(1, early)
    down(2, late)
    over_x(2, late)
    over_z(0, late)
    over_z(2, early)
    over_z(1, late)
    down(3, late)
    over_x(3, late)
    over_z(3, late)
    over_z(2, late)

    def result(u):
        cut = pl.ds(u * LANES, LANES)
        return pltpu.make_async_copy(done.at[u], out.at[:, cut], load_sem.at[u])

    with jax.named_scope("final"):
        for u in range(n_out):
            cut = slice(u * LANES, (u + 1) * LANES)
            core_copy(u, MINE, 0).wait_recv()
            for dx in range(1, n_x):
                x_copy(u, MINE, dx).wait_recv()
            value = res[k, mine, cut].astype(jnp.float32) + place_sum(u, MINE)
            back(u).wait_recv()
            value = value + got_z[u].astype(jnp.float32)
            for dx in range(1, n_x) if u == n_out - 1 else ():
                x_copy(u, THEIRS, dx).wait_recv()
                value = value + got_x[u, THEIRS, dx - 1].astype(jnp.float32)
            done[u] = value.astype(jnp.bfloat16)
            result(u).start()

    with jax.named_scope("drain"):
        for u in range(n_out):
            result(u).wait()
        def drain(role):
            for i, view in enumerate(all_sums(role, n_from)):
                to_y(view, view, y_send.at[i], y_recv.at[0]).wait_send()
            for d in range(1, n_fs):
                for i, view in enumerate(all_sums(role_of(role, d), 1)):
                    if (role, d) != (END, 2) or i == 3:
                        to_fs(view, view, z_send.at[i, d - 1], z_recv.at[0, 0], pair).wait_send()
            if role == INNER:
                for i, view in enumerate(all_sums(role, 1)[:3]):
                    to_fs(view, view, f_send.at[i], z_recv.at[0, 0], pair).wait_send()

        by_role(drain)
        for i, buffer in enumerate((tok, res)):
            view = buffer.at[pl.ds(0, n_tp - 1)]
            to_tp(view, view, all_send.at[i], all_recv.at[0, 0], core).wait_send()
        view = part_mix.at[:, pl.ds(0, n_x)]
        to_tp(view, view, mix_core_send.at[0], all_recv.at[0, 0], core).wait_send()
        to_tp(mix_x_sum, mix_x_sum, mix_x_send.at[0], all_recv.at[0, 0], core).wait_send()
        view = part_ffn.at[:, :, pl.ds(0, n_x)]
        to_tp(view, view, core_send.at[0], all_recv.at[0, 0], core).wait_send()
        to_tp(sum_x, sum_x, x_send.at[0], all_recv.at[0, 0], core).wait_send()
        view = tok.at[pl.ds(0, 2)]
        to_pair(0, view, view).wait_send()


def fused(n_fs, n_tp, *args):
    tokens, w_signal, w_gate = args[0], args[2], args[8]
    rows, cols = tokens.shape
    shard, chans = w_signal.shape
    n_in, n_out = tiles_of(w_gate.shape[1] // LANES, INNER), shard // LANES
    units = n_in * LANES
    width = n_fs * shard
    args = list(args)
    args[1], args[7] = args[1].reshape(1, -1), args[7].reshape(1, -1)
    args[10] = args[10].transpose(1, 0, 2)
    small = [pltpu.VMEM(args[i].shape, jnp.float32) for i in (1, 5, 7, 10, 11)]
    n_x = n_tp // 2
    length = rows // SEQS_DEV
    dma = pltpu.SemaphoreType.DMA

    def held(*shape):
        return pltpu.VMEM(shape, jnp.bfloat16)

    return pl.pallas_call(
        functools.partial(layer_kernel, n_fs, n_tp),
        out_shape=jax.ShapeDtypeStruct((rows, cols), jnp.bfloat16),
        in_specs=[pl.BlockSpec(memory_space=pl.ANY)] * len(args),
        out_specs=pl.BlockSpec(memory_space=pl.ANY),
        scratch_shapes=[
            *small,
            held(width, 3 * (chans // 2)),
            held(n_fs, chans // 2, shard),
            held(n_in, width, 2 * LANES),
            held(n_out, units, n_fs * LANES),
            held(n_tp, 2 * rows, cols),
            held(n_tp, 2 * rows, cols),
            held(2 * rows, width),
            held(2 * rows, units),
            held(2, n_tp, rows, cols),
            held(2, n_x, rows, cols),
            held(2, SEQS_DEV, n_x - 1, length, cols),
            held(2, SEQS_DEV, n_x - 1, length, cols),
            held(SEQS_DEV, length, cols),
            held(SEQS_DEV, length, cols),
            held(n_out, 2, n_tp, rows, LANES),
            held(n_out, 2, n_x, rows, LANES),
            held(n_out, 2, n_x - 1, rows, LANES),
            held(n_out, 2, n_x - 1, rows, LANES),
            held(n_out, rows, LANES),
            held(n_out, rows, LANES),
            held(n_out, rows, LANES),
            dma((4, n_fs - 1)),
            dma((2 + n_in + n_out, n_fs - 1)),
            dma((4,)),
            dma((4,)),
            dma((2 + n_in + 2 * n_out,)),
            dma((10,)),
            dma((2,)),
            dma((1 + 3 * SEQS_DEV, n_x)),
            dma((1,)),
            dma((2,)),
            dma((1,)),
            dma((2, SEQS_DEV, n_x - 1)),
            dma((1,)),
            dma((n_out, 2, n_x)),
            dma((1,)),
            dma((n_out, 2, n_x - 1)),
            dma((1,)),
            dma((3 * SEQS_DEV + n_out,)),
        ],
        compiler_params=pltpu.CompilerParams(
            collective_id=0, has_side_effects=True, vmem_limit_bytes=62 * 1024 * 1024
        ),
    )(*args)


def solution(mesh):
    n_fs, n_tp = mesh.shape["fs"], mesh.shape["tp"]
    body = functools.partial(fused, n_fs, n_tp)
    if n_fs != 4 or n_tp != 4 or mesh.shape["grp"] != 2:
        body = on_device
    placed = (
        P(("grp", "fs"), "tp"),
        P(),
        P("fs", "tp"),
        P("fs", "tp"),
        P("fs", "tp"),
        P(None, "tp"),
        P("tp", "fs"),
        P(),
        P("fs", "tp"),
        P("fs", "tp"),
        P(None, None, "tp"),
        P(None, "tp"),
        P("tp", "fs"),
    )
    return jax.shard_map(
        body, mesh=mesh, in_specs=placed, out_specs=P(("grp", "fs"), "tp"), check_vma=False
    )
```
